32 devices in a mesh: sp: 4 (over z), fs: 4 (over y, x), tp: 2 (over core).
Axes of the slice: x: 2, y: 2, z: 4, core: 2. Of those that a mesh axis runs over, the one named last changes fastest.
Arguments:
- activations: bfloat16 [4, 1024, 2048], P('fs', 'sp'), may hold values from -600 to 600
- norm_gain: float32 [2048], replicated, may hold values from 0.1 to 1.9
- w_conv_gate: bfloat16 [2048, 1024], P('sp', ('fs', 'tp')), may hold values from -0.125 to 0.125
- w_conv_mult: bfloat16 [2048, 1024], P('sp', ('fs', 'tp')), may hold values from -0.125 to 0.125
- w_conv_in: bfloat16 [2048, 1024], P('sp', ('fs', 'tp')), may hold values from -0.125 to 0.125
- conv_taps: float32 [3, 1024], replicated, may hold values from -3.5 to 3.5
- w_query: bfloat16 [2048, 1024], P('sp', ('fs', 'tp')), may hold values from -0.125 to 0.125
- w_key: bfloat16 [2048, 1024], P('sp', ('fs', 'tp')), may hold values from -0.125 to 0.125
- w_value: bfloat16 [2048, 1024], P('sp', ('fs', 'tp')), may hold values from -0.125 to 0.125
- w_input_gate: bfloat16 [2048, 8], replicated, may hold values from -0.125 to 0.125
- w_forget_gate: bfloat16 [2048, 8], replicated, may hold values from -0.125 to 0.125
- gate_bias: float32 [2, 8], replicated, may hold values from -1 to 120
- decay_shift: float32 [4, 1024, 8], P(None, 'sp'), may hold values from -2 to 0, as said below
- head_gain: float32 [1024], replicated, may hold values from 0.1 to 1.9
- w_out_conv: bfloat16 [1024, 2048], P(('fs', 'tp'), 'sp'), may hold values from -0.125 to 0.125
- w_out_mem: bfloat16 [1024, 2048], P(('fs', 'tp'), 'sp'), may hold values from -0.125 to 0.125
Outputs:
- output: bfloat16 [4, 1024, 2048], P('fs', ('sp', 'tp'))
The draws below stay inside these ranges and needn't reach their ends.
Inputs may be any that keep to these rules, and one draw needn't show every extreme that they name: `decay_shift`: never positive.
All inputs are finite; a program needn't handle non-finite values.
Results may differ from the reference program's by a relative error of at most 0.015.
Values may be sent and summed in bfloat16 or wider, within the bound.
A program may use at most 64 MiB of HBM per device.

```python
import math
import jax
import jax.numpy as jnp
from jax import lax

D = 2048
CONV_CH = 1024
MEMORY_HEADS = 8
HEAD_DIM = 128
BLOCK = 64
TAPS = 3
TOK_DEV = 256
SEQUENCE_COUNT = 4
SEQUENCE_LENGTH = 1024


def draw_activations(key, part):
    random_subkeys = jax.random.split(key, 3)
    row_scale = jnp.exp(jax.random.uniform(random_subkeys[0], (SEQUENCE_COUNT, SEQUENCE_LENGTH, 1), jnp.float32, 0.0, math.log(10.0)))
    col_scale = jnp.exp(jax.random.uniform(random_subkeys[1], (1, 1, D), jnp.float32, 0.0, math.log(10.0)))
    base_values = jnp.clip(jax.random.normal(random_subkeys[2], (SEQUENCE_COUNT, SEQUENCE_LENGTH, D), jnp.float32), -6.0, 6.0)
    return (base_values * row_scale * col_scale).astype(jnp.bfloat16)


def draw_gate_bias(key, part):
    random_subkeys = jax.random.split(key, 4)
    ranking = jax.random.permutation(random_subkeys[0], MEMORY_HEADS)
    slow_heads = ranking < MEMORY_HEADS // 2
    entry_bias = jax.random.uniform(random_subkeys[1], (MEMORY_HEADS,), jnp.float32, -1.0, 1.0)
    slow_bias = math.log(SEQUENCE_LENGTH) + 2.0 + jax.random.uniform(random_subkeys[2], (MEMORY_HEADS,), jnp.float32, -0.3, 0.3)
    fast_bias = jax.random.uniform(random_subkeys[3], (MEMORY_HEADS,), jnp.float32, 3.0, 4.5)
    forget = jnp.where(slow_heads, slow_bias, fast_bias)
    return jnp.stack([entry_bias, forget], axis=0)


def draw_decay_shift(key, part):
    random_subkeys = jax.random.split(key, 3)
    nblocks = SEQUENCE_LENGTH // TOK_DEV
    low_rate, high_rate = (0.2, 2.0)
    rates = jnp.exp(jax.random.uniform(random_subkeys[0], (SEQUENCE_COUNT, nblocks, 1, MEMORY_HEADS), jnp.float32, math.log(low_rate), math.log(high_rate)))
    stable_part = -jnp.broadcast_to(rates, (SEQUENCE_COUNT, nblocks, TOK_DEV, MEMORY_HEADS)).reshape(SEQUENCE_COUNT, SEQUENCE_LENGTH, MEMORY_HEADS) / SEQUENCE_LENGTH
    spike_positions = jax.random.randint(random_subkeys[1], (SEQUENCE_COUNT, 2, MEMORY_HEADS), 0, SEQUENCE_LENGTH)
    spike_penalty = jax.random.uniform(random_subkeys[2], (SEQUENCE_COUNT, 2, MEMORY_HEADS), jnp.float32, 0.2, 0.5)
    chosen_positions = jnp.arange(SEQUENCE_LENGTH)[None, :, None, None]
    match_count = (chosen_positions == spike_positions[:, None, :, :]).astype(jnp.float32)
    spike_events = jnp.sum(match_count * jnp.log(1.0 - spike_penalty)[:, None, :, :], axis=2)
    return stable_part + spike_events


def steps_of(stream_key, shape, cuts, least, largest):
    gain, own = 1.0, jax.random.fold_in(stream_key, 6)
    for axis_at, parts in cuts:
        steps = jnp.exp(jax.random.uniform(jax.random.fold_in(own, axis_at), (parts,), jnp.float32, least / len(cuts), largest / len(cuts)))
        gain = gain * jnp.repeat(steps, shape[axis_at] // parts).reshape([-1 if axis == axis_at else 1 for axis in range(len(shape))])
    return gain


def gaussian(rng, dims, deviation, bound, cuts=(), held_as=jnp.bfloat16):
    entries = jax.random.normal(rng, dims, jnp.float32) * deviation
    if len(cuts) > 0:
        entries = steps_of(rng, dims, cuts, -0.22, 0.18) * entries
    return jnp.clip(entries, min=-bound, max=bound).astype(held_as)


def setup_inputs(seed: int = 0) -> dict:
    splits = jax.random.split(jax.random.key(seed), 17)
    return {
        "activations": draw_activations(jax.random.fold_in(splits[16], 71), 0),
        "norm_gain": jnp.clip(1.0 + 0.18 * jax.random.normal(splits[1], (D,), jnp.float32), 0.1, 1.9),
        "w_conv_gate": gaussian(splits[2], (D, CONV_CH), D ** -0.5, 0.125, ((0, 4), (1, 8))),
        "w_conv_mult": gaussian(splits[3], (D, CONV_CH), D ** -0.5, 0.125, ((0, 4), (1, 8))),
        "w_conv_in": gaussian(splits[4], (D, CONV_CH), D ** -0.5, 0.125, ((0, 4), (1, 8))),
        "conv_taps": gaussian(splits[5], (TAPS, CONV_CH), TAPS ** -0.5, 3.5, (), jnp.float32),
        "w_query": gaussian(splits[6], (D, MEMORY_HEADS * HEAD_DIM), D ** -0.5, 0.125, ((0, 4), (1, 8))),
        "w_key": gaussian(splits[7], (D, MEMORY_HEADS * HEAD_DIM), D ** -0.5, 0.125, ((0, 4), (1, 8))),
        "w_value": gaussian(splits[8], (D, MEMORY_HEADS * HEAD_DIM), D ** -0.5, 0.125, ((0, 4), (1, 8))),
        "w_input_gate": gaussian(splits[9], (D, MEMORY_HEADS), D ** -0.5, 0.125),
        "w_forget_gate": gaussian(splits[10], (D, MEMORY_HEADS), D ** -0.5, 0.125),
        "gate_bias": draw_gate_bias(jax.random.fold_in(splits[16], 71), 0),
        "decay_shift": draw_decay_shift(jax.random.fold_in(splits[16], 71), 0),
        "head_gain": jnp.clip(1.0 + 0.18 * jax.random.normal(splits[13], (MEMORY_HEADS * HEAD_DIM,), jnp.float32), 0.1, 1.9),
        "w_out_conv": gaussian(splits[14], (CONV_CH, D), (CONV_CH + MEMORY_HEADS * HEAD_DIM) ** -0.5, 0.125, ((0, 8), (1, 4))),
        "w_out_mem": gaussian(splits[15], (MEMORY_HEADS * HEAD_DIM, D), (CONV_CH + MEMORY_HEADS * HEAD_DIM) ** -0.5, 0.125, ((0, 8), (1, 4))),
    }


EPSILON = 1e-06
HIGHEST_PRECISION = lax.Precision.HIGHEST

def combine_states(earlier, later):
    total_one, peak_one, state_one = earlier
    total_two, peak_two, state_two = later
    peak_new = jnp.maximum(total_two + peak_one, peak_two)
    scale_old = jnp.exp(total_two + peak_one - peak_new)
    scale_new = jnp.exp(peak_two - peak_new)
    return (total_one + total_two, peak_new, scale_old[..., None, None] * state_one + scale_new[..., None, None] * state_two)

def head_memory(block_inputs):
    query_rows, key_rows, value_rows, entry_gate, log_forget = block_inputs
    members = query_rows.shape[0]
    tokens = query_rows.shape[1]
    head_width = query_rows.shape[2]
    nblocks = tokens // BLOCK
    block_shape = (members, nblocks, BLOCK, head_width)
    query_blocks = query_rows.astype(jnp.float32).reshape(block_shape)
    key_blocks = key_rows.astype(jnp.float32).reshape(block_shape) * head_width ** (-0.5)
    value_blocks = value_rows.astype(jnp.float32).reshape(block_shape)
    entry_blocks = entry_gate.reshape(members, nblocks, BLOCK)
    forget_sums = jnp.cumsum(log_forget.reshape(members, nblocks, BLOCK), axis=-1)
    block_total = forget_sums[..., -1]
    local_logs = block_total[..., None] - forget_sums + entry_blocks
    local_peak = lax.optimization_barrier(jnp.max(local_logs, axis=-1))
    local_weights = jnp.exp(local_logs - local_peak[..., None])
    local_state = jnp.einsum('bclv,bclk->bcvk', local_weights[..., None] * value_blocks, key_blocks, precision=HIGHEST_PRECISION)

    def advance(running, block_item):
        return (combine_states(running, block_item), running)
    anchor = (jnp.zeros((members,), jnp.float32), jnp.zeros((members,), jnp.float32), jnp.zeros((members, head_width, head_width), jnp.float32))
    block_items = (jnp.moveaxis(block_total, 1, 0), jnp.moveaxis(local_peak, 1, 0), jnp.moveaxis(local_state, 1, 0))
    _, prior_states = lax.scan(advance, anchor, block_items)
    prior_peak = jnp.moveaxis(prior_states[1], 0, 1)
    prior_state = jnp.moveaxis(prior_states[2], 0, 1)
    positions = jnp.arange(BLOCK)
    causal_mask = positions[:, None] >= positions[None, :]
    pair_logs = jnp.where(causal_mask, forget_sums[..., :, None] - forget_sums[..., None, :] + entry_blocks[..., None, :], -jnp.inf)
    carried_logs = forget_sums + prior_peak[..., None]
    row_peak = jnp.maximum(carried_logs, lax.optimization_barrier(jnp.max(pair_logs, axis=-1)))
    inner_weights = jnp.exp(pair_logs - row_peak[..., None])
    carried_weights = jnp.exp(carried_logs - row_peak)
    scores = inner_weights * jnp.einsum('bcld,bcsd->bcls', query_blocks, key_blocks, precision=HIGHEST_PRECISION)
    numerator = carried_weights[..., None] * jnp.einsum('bcvk,bclk->bclv', prior_state, query_blocks, precision=HIGHEST_PRECISION) + jnp.einsum('bcls,bcsv->bclv', scores, value_blocks, precision=HIGHEST_PRECISION)
    return numerator.reshape(members, tokens, head_width)

def reference(activations, norm_gain, w_conv_gate, w_conv_mult, w_conv_in, conv_taps, w_query, w_key, w_value, w_input_gate, w_forget_gate, gate_bias, decay_shift, head_gain, w_out_conv, w_out_mem):
    seq_count = activations.shape[0]
    length = activations.shape[1]
    model_width = activations.shape[2]
    flat_rows = activations.reshape(seq_count * length, model_width).astype(jnp.float32)
    normed = (flat_rows * lax.rsqrt(lax.optimization_barrier(jnp.mean(flat_rows * flat_rows, axis=-1, keepdims=True)) + EPSILON) * norm_gain).astype(jnp.bfloat16)

    def project(weight):
        return jnp.dot(normed, weight, preferred_element_type=jnp.float32).astype(jnp.bfloat16)
    conv_gate = project(w_conv_gate).reshape(seq_count, length, CONV_CH)
    conv_mult = project(w_conv_mult).reshape(seq_count, length, CONV_CH)
    conv_in = project(w_conv_in).reshape(seq_count, length, CONV_CH)
    product = (conv_mult.astype(jnp.float32) * conv_in.astype(jnp.float32)).astype(jnp.bfloat16)
    padded = jnp.pad(product, ((0, 0), (TAPS - 1, 0), (0, 0))).astype(jnp.float32)
    mixed_sum = jnp.zeros((seq_count, length, CONV_CH), jnp.float32)
    for tap_index in range(TAPS):
        mixed_sum = mixed_sum + conv_taps[tap_index] * padded[:, tap_index:tap_index + length, :]
    conv_out = (conv_gate.astype(jnp.float32) * mixed_sum).astype(jnp.bfloat16)

    def heads_first(values, inner):
        return jnp.moveaxis(values.reshape(seq_count, length, MEMORY_HEADS, inner), 2, 0)
    query_heads = heads_first(project(w_query), HEAD_DIM)
    key_heads = heads_first(project(w_key), HEAD_DIM)
    value_heads = heads_first(project(w_value), HEAD_DIM)
    entry = jnp.dot(normed, w_input_gate, preferred_element_type=jnp.float32) + gate_bias[0]
    log_forget = jax.nn.log_sigmoid(jnp.dot(normed, w_forget_gate, preferred_element_type=jnp.float32) + gate_bias[1]) + decay_shift.reshape(seq_count * length, MEMORY_HEADS)
    entry_heads = jnp.moveaxis(entry.reshape(seq_count, length, MEMORY_HEADS), 2, 0)
    forget_heads = jnp.moveaxis(log_forget.reshape(seq_count, length, MEMORY_HEADS), 2, 0)
    memory = lax.map(head_memory, (query_heads, key_heads, value_heads, entry_heads, forget_heads))
    memory = memory * lax.rsqrt(lax.optimization_barrier(jnp.mean(memory * memory, axis=-1, keepdims=True)) + EPSILON) * head_gain.reshape(MEMORY_HEADS, 1, 1, HEAD_DIM)
    mem_out = jnp.moveaxis(memory, 0, 2).reshape(seq_count * length, MEMORY_HEADS * HEAD_DIM).astype(jnp.bfloat16)
    output = jnp.dot(conv_out.reshape(seq_count * length, CONV_CH), w_out_conv, preferred_element_type=jnp.float32) + jnp.dot(mem_out, w_out_mem, preferred_element_type=jnp.float32)
    return output.astype(jnp.bfloat16).reshape(seq_count, length, model_width)
```

```python
import functools

import jax
import jax.numpy as jnp
from jax import lax
from jax.experimental import pallas as pl
from jax.experimental.pallas import tpu as pltpu
from jax.sharding import PartitionSpec as P

MEMORY_HEADS = 8
HEAD_DIM = 128
BLOCK = 64


EPSILON = 1e-06
FAR_BELOW = -1e30
HIGHEST_PRECISION = lax.Precision.HIGHEST


def prefix(value, axis, join, neutral):
    count, mine = (lax.axis_size(axis), lax.axis_index(axis))
    total, peak, state = value
    stats = jnp.stack([total, peak], axis=1)[..., None]
    stats = jnp.broadcast_to(stats, stats.shape[:2] + state.shape[-1:])
    packed = lax.all_gather(jnp.concatenate([state, stats], axis=1), axis)
    height = state.shape[1]
    pieces = (packed[:, :, height, 0], packed[:, :, height + 1, 0], packed[:, :, :height])
    subtotal = jax.tree.map(
        lambda part, zero: jnp.full_like(part, 0) + jnp.asarray(zero, part.dtype), value, neutral
    )

    def lap(position, subtotal):
        longer = join(subtotal, jax.tree.map(lambda part: part[position], pieces))
        return jax.tree.map(lambda new, old: jnp.where(position < mine, new, old), longer, subtotal)

    return lax.fori_loop(0, count - 1, lap, subtotal)


def from_behind(array, axis, by):
    peers = lax.axis_size(axis)
    pairs = [(i, i + by) for i in range(peers) if 0 <= i + by < peers]
    return lax.ppermute(array, axis, pairs)


def combine_states(earlier, later):
    total_one, peak_one, state_one = earlier
    total_two, peak_two, state_two = later
    peak_new = jnp.maximum(total_two + peak_one, peak_two)
    scale_old = jnp.exp(total_two + peak_one - peak_new)
    scale_new = jnp.exp(peak_two - peak_new)
    return (
        total_one + total_two,
        peak_new,
        scale_old[..., None, None] * state_one + scale_new[..., None, None] * state_two,
    )


def head_rows(values, seq_count, heads_here):
    tokens = values.shape[1]
    split_heads = values.reshape(seq_count, tokens, heads_here, HEAD_DIM).transpose(0, 2, 1, 3)
    return split_heads.reshape(seq_count * heads_here, tokens, HEAD_DIM).astype(jnp.float32)


def gate_rows(values, seq_count, heads_here):
    tokens = values.shape[1]
    return values.transpose(0, 2, 1).reshape(seq_count * heads_here, tokens)


def memory_cell(query_rows, key_rows, value_rows, entry_gate, log_forget):
    members = query_rows.shape[0]
    tokens = query_rows.shape[1]
    head_width = query_rows.shape[2]
    nblocks = tokens // BLOCK
    block_shape = (members, nblocks, BLOCK, head_width)
    query_blocks = query_rows.reshape(block_shape)
    key_blocks = key_rows.reshape(block_shape) * head_width ** (-0.5)
    value_blocks = value_rows.reshape(block_shape)
    entry_blocks = entry_gate.reshape(members, nblocks, BLOCK)
    forget_sums = jnp.cumsum(log_forget.reshape(members, nblocks, BLOCK), axis=-1)
    block_total = forget_sums[..., -1]
    local_logs = block_total[..., None] - forget_sums + entry_blocks
    local_peak = jnp.max(local_logs, axis=-1)
    local_weights = jnp.exp(local_logs - local_peak[..., None])
    local_state = jnp.einsum(
        "bclv,bclk->bcvk",
        local_weights[..., None] * value_blocks,
        key_blocks,
        precision=HIGHEST_PRECISION,
    )

    def advance(running, block_item):
        return (combine_states(running, block_item), running)

    zero_sums = jnp.zeros((members,), jnp.float32)
    low_peaks = jnp.full((members,), FAR_BELOW, jnp.float32)
    zero_states = jnp.zeros((members, head_width, head_width), jnp.float32)
    block_items = (
        jnp.moveaxis(block_total, 1, 0),
        jnp.moveaxis(local_peak, 1, 0),
        jnp.moveaxis(local_state, 1, 0),
    )
    device_total, inner_states = lax.scan(advance, (zero_sums, low_peaks, zero_states), block_items)
    inner_states = tuple((jnp.moveaxis(tensor, 0, 1) for tensor in inner_states))
    total_sum, total_peak, total_state = device_total
    before = prefix(
        (total_sum, total_peak, total_state),
        "sp",
        combine_states,
        (zero_sums, low_peaks, zero_states),
    )
    opening = combine_states((zero_sums, zero_sums, zero_states), before)
    opening = tuple((tensor[:, None] for tensor in opening))
    _, prior_peak, prior_state = combine_states(opening, inner_states)
    positions = jnp.arange(BLOCK)
    causal_mask = positions[:, None] >= positions[None, :]
    pair_logs = jnp.where(
        causal_mask,
        forget_sums[..., :, None] - forget_sums[..., None, :] + entry_blocks[..., None, :],
        -jnp.inf,
    )
    carried_logs = forget_sums + prior_peak[..., None]
    row_peak = jnp.maximum(carried_logs, jnp.max(pair_logs, axis=-1))
    inner_weights = jnp.exp(pair_logs - row_peak[..., None])
    carried_weights = jnp.exp(carried_logs - row_peak)
    scores = inner_weights * jnp.einsum(
        "bcld,bcsd->bcls", query_blocks, key_blocks, precision=HIGHEST_PRECISION
    )
    numerator = carried_weights[..., None] * jnp.einsum(
        "bcvk,bclk->bclv", prior_state, query_blocks, precision=HIGHEST_PRECISION
    ) + jnp.einsum("bcls,bcsv->bclv", scores, value_blocks, precision=HIGHEST_PRECISION)
    return numerator.reshape(members, tokens, head_width)


MESH = pl.DeviceIdType.MESH
F32 = jnp.float32
BF16 = jnp.bfloat16
TAPS = 3
RIM = 8
KV, QUERY, OUT, MIX, GATE = range(5)
SPANS = {KV: (0, 2), QUERY: (2, 1), MIX: (3, 2), GATE: (5, 1)}
PARTS = 5


def layer_kernel(
    ns,
    nf,
    act_ref,
    gain_ref,
    w0_ref,
    w1_ref,
    w2_ref,
    w3_ref,
    w4_ref,
    w5_ref,
    wi_ref,
    wf_ref,
    bias_ref,
    decay_ref,
    taps_ref,
    head_ref,
    wc_ref,
    wm_ref,
    out_ref,
    raw,
    gain,
    normed,
    wbuf,
    wi,
    wf,
    bias,
    decay,
    taps,
    head,
    wo,
    kv,
    query,
    logs,
    logs_t,
    local_state,
    local_stat,
    carry,
    carry_m,
    passed,
    passed_m,
    padded,
    mixed,
    gate_sum,
    mine,
    got,
    acc,
    other,
    load_sem,
    x_send,
    x_recv,
    d_send,
    d_recv,
    w_send,
    w_recv,
    p_send,
    p_recv,
    s_send,
    s_recv,
    r_send,
    r_recv,
    m_send,
    m_recv,
    e_send,
    e_recv,
):
    sp, fs, tp = (lax.axis_index("sp"), lax.axis_index("fs"), lax.axis_index("tp"))
    g = fs * 2 + tp
    depth, cols = w0_ref.shape
    half, model = raw.shape
    tokens = 2 * half
    ocols = wc_ref.shape[1]
    partner = (sp, fs, 1 - tp)
    has_up, has_down = (sp + 1 < ns, sp > 0)
    up, down = ((sp + 1, fs, tp), (sp - 1, fs, tp))
    fy, fx = (fs // 2, lax.rem(fs, 2))
    ny = nf // 2

    def ahead(k):
        return lax.rem(fy + k // 2, ny) * 2 + lax.rem(fx + k % 2, 2)

    def behind(k):
        return lax.rem(fy + ny - k // 2, ny) * 2 + lax.rem(fx + k % 2, 2)

    def block(index, size):
        return pl.ds(pl.multiple_of(index * size, size), size)

    def remote(src, dst, send, recv, to):
        return pltpu.make_async_remote_copy(
            src, dst, send, recv, device_id=to, device_id_type=MESH
        )

    loads = [pltpu.make_async_copy(act_ref.at[block(tp, half)], raw, load_sem.at[0])]
    loads.append(pltpu.make_async_copy(gain_ref, gain, load_sem.at[1]))
    for j, ref in enumerate((w0_ref, w1_ref, w2_ref, w3_ref, w4_ref, w5_ref)):
        loads.append(
            pltpu.make_async_copy(
                ref, wbuf.at[block(sp, depth), pl.ds(j * cols, cols)], load_sem.at[2 + j]
            )
        )
    for m, ref in enumerate((wc_ref, wm_ref)):
        loads.append(
            pltpu.make_async_copy(
                ref, wo.at[m, block(fs, cols), block(sp, ocols)], load_sem.at[8 + m]
            )
        )
    smalls = (
        (wi_ref, wi),
        (wf_ref, wf),
        (bias_ref, bias),
        (decay_ref, decay),
        (taps_ref, taps),
        (head_ref, head),
    )
    for j, (ref, held) in enumerate(smalls):
        loads.append(pltpu.make_async_copy(ref, held, load_sem.at[10 + j]))
    for j in (2, 3, 0, 1, 4, 8, 9, 5, 6, 7, 10, 11, 12, 13, 14, 15):
        loads[j].start()

    barrier = pltpu.get_barrier_semaphore()
    for k in range(1, nf):
        pl.semaphore_signal(barrier, inc=1, device_id=(sp, ahead(k), tp), device_id_type=MESH)
    pl.semaphore_signal(barrier, inc=1, device_id=partner, device_id_type=MESH)

    @pl.when(has_up)
    def _():
        pl.semaphore_signal(barrier, inc=1, device_id=up, device_id_type=MESH)

    @pl.when(has_down)
    def _():
        pl.semaphore_signal(barrier, inc=1, device_id=down, device_id_type=MESH)

    def place(part, owner):
        if part == OUT:
            return wo.at[:, block(fs, cols), block(owner, ocols)]
        first, count = SPANS[part]
        return wbuf.at[block(owner, depth), pl.ds(first * cols, count * cols)]

    def z_copy(part, side, d, owner):
        there = place(part, owner)
        return remote(
            there,
            there,
            w_send.at[side, d, part],
            w_recv.at[side, d, part],
            (up, down)[side],
        )

    def owner_of(side, d):
        return sp - d if side == 0 else sp + d

    def arrives(side, d):
        return (sp - d >= 0) if side == 0 else (sp + d < ns)

    def sends(side, d):
        return arrives(side, d) & (has_up if side == 0 else has_down)

    def z_send(part, side, d):
        @pl.when(sends(side, d))
        def _():
            z_copy(part, side, d, owner_of(side, d)).start()

    def own(part):
        for side in range(2):
            z_send(part, side, 0)

    def p_copy(owner, k, row):
        there = wo.at[:, block(row, cols), block(owner, ocols)]
        return remote(
            there, there, p_send.at[owner, k - 1], p_recv.at[owner, k - 1], (sp, ahead(k), tp)
        )

    def spread(owner):
        for k in range(1, nf):
            p_copy(owner, k, fs).start()

    def z_step(part, d, use=None):
        for side in range(2):

            @pl.when(arrives(side, d))
            def _():
                owner = owner_of(side, d)
                z_copy(part, side, d - 1, owner).wait_recv()
                if d < ns - 1:
                    z_send(part, side, d)
                if part == OUT:
                    spread(owner)
                if use is not None:
                    use(owner)

    def x_copy(k, seq):
        there = normed.at[pl.ds(pl.multiple_of(seq * tokens + tp * half, half), half)]
        return remote(there, there, x_send.at[k - 1], x_recv.at[k - 1], (sp, ahead(k), tp))

    def d_copy(k, seq, part):
        there = normed.at[pl.ds(pl.multiple_of(seq * tokens + part * half, half), half)]
        return remote(there, there, d_send.at[k], d_recv.at[k], partner)

    loads[2].wait()
    loads[3].wait()
    pl.semaphore_wait(barrier, nf + has_up.astype(jnp.int32) + has_down.astype(jnp.int32))
    own(KV)
    loads[0].wait()
    loads[1].wait()
    step = 32

    def norm_rows(i, carried):
        x = raw[pl.ds(pl.multiple_of(i * step, step), step), :].astype(F32)
        scale = lax.rsqrt(jnp.mean(x * x, axis=-1, keepdims=True) + EPSILON)
        rows = pl.ds(pl.multiple_of(fs * tokens + tp * half + i * step, step), step)
        normed[rows, :] = (x * scale * gain[...]).astype(BF16)
        return carried

    lax.fori_loop(0, half // step, norm_rows, 0)
    loads[4].wait()
    own(QUERY)
    for k in range(1, nf):
        x_copy(k, fs).start()
    d_copy(0, fs, tp).start()
    loads[8].wait()
    loads[9].wait()
    z_step(KV, 1)

    def relay(k):
        x_copy(k, behind(k)).wait_recv()
        d_copy(k, behind(k), tp).start()

    for k in range(1, nf - 1):
        relay(k)
    for d in range(2, ns - 1):
        z_step(KV, d)
    own(OUT)
    spread(sp)
    relay(nf - 1)
    for d in range(1, ns - 1):
        z_step(QUERY, d)
    for j in (5, 6, 7, 10, 11, 12, 13, 14, 15):
        loads[j].wait()
    own(MIX)
    z_step(KV, ns - 1)
    for k in range(nf):
        d_copy(k, behind(k), 1 - tp).wait_recv()

    def tile(i):
        return pl.ds(pl.multiple_of(i * tokens, tokens), tokens)

    def project(part, into):
        first, count = SPANS[part]

        def body(i, carried):
            into[tile(i), :] = jnp.dot(
                normed[tile(i), :],
                wbuf[:, first * cols : (first + count) * cols],
                preferred_element_type=F32,
            ).astype(BF16)
            return carried

        lax.fori_loop(0, nf, body, 0)

    lane8 = lax.broadcasted_iota(jnp.int32, (tokens, wi.shape[1]), 1)
    lane = lax.broadcasted_iota(jnp.int32, (tokens, 128), 1)
    row_at = lax.broadcasted_iota(jnp.int32, (tokens, tokens), 0)
    col_at = lax.broadcasted_iota(jnp.int32, (tokens, tokens), 1)
    packed = jnp.zeros((tokens, 128), F32)
    for s in range(nf):
        x = normed[s * tokens : (s + 1) * tokens, :]
        entry = jnp.dot(x, wi[...], preferred_element_type=F32) + bias[0:1, :]
        raw_forget = jnp.dot(x, wf[...], preferred_element_type=F32) + bias[1:2, :]
        forget = (
            jnp.minimum(raw_forget, 0.0) - jnp.log1p(jnp.exp(-jnp.abs(raw_forget))) + decay[s]
        )
        entry = jnp.sum(jnp.where(lane8 == g, entry, 0.0), axis=1, keepdims=True)
        forget = jnp.sum(jnp.where(lane8 == g, forget, 0.0), axis=1, keepdims=True)
        packed = jnp.where(lane == s, forget, packed)
        packed = jnp.where(lane == nf + s, entry, packed)
    ones = jnp.where(row_at >= col_at, 1.0, 0.0).astype(F32)
    sums = jnp.dot(ones, packed, precision=HIGHEST_PRECISION, preferred_element_type=F32)
    sums = jnp.where(lane < nf, sums, packed)
    logs[...] = sums
    logs_t[...] = sums.T
    project(KV, kv)
    for s in range(nf):
        rows = pl.ds(s * tokens, tokens)
        total = logs_t[s : s + 1, tokens - 1 : tokens]
        reach = total - logs[:, s : s + 1] + logs[:, nf + s : nf + s + 1]
        peak = jnp.max(reach, axis=0, keepdims=True)
        weighted = (kv[rows, cols:].astype(F32) * jnp.exp(reach - peak)).astype(BF16)
        local_state[s] = lax.dot_general(
            kv[rows, :cols], weighted, (((0,), (0,)), ((), ())), preferred_element_type=F32
        )
        local_stat[s : s + 1, :] = jnp.broadcast_to(total, (1, 128))
        local_stat[nf + s : nf + s + 1, :] = jnp.broadcast_to(peak, (1, 128))

    z_step(QUERY, ns - 1)
    z_step(OUT, 1)

    def state_copies():
        return (
            remote(passed_m, carry_m, s_send.at[0], s_recv.at[0], up),
            remote(passed, carry, s_send.at[1], s_recv.at[1], up),
        )

    @pl.when(jnp.logical_not(has_down))
    def _():
        carry[...] = jnp.zeros_like(carry)
        carry_m[...] = jnp.zeros_like(carry_m)

    @pl.when(has_down)
    def _():
        for copy in state_copies():
            copy.wait_recv()

    @pl.when(has_up)
    def _():
        for s in range(nf):
            before = local_stat[s : s + 1, :] + carry_m[s : s + 1, :]
            peak = local_stat[nf + s : nf + s + 1, :]
            top = jnp.maximum(before, peak)
            passed[s] = (
                jnp.exp(before - top) * carry[s].astype(F32) + jnp.exp(peak - top) * local_state[s]
            ).astype(BF16)
            passed_m[s : s + 1, :] = top
        for copy in state_copies():
            copy.start()

    for d in range(2, ns - 1):
        z_step(OUT, d)
    own(GATE)
    project(QUERY, query)

    def mix_copy(m, k, seq, source):
        return remote(
            mine.at[m, seq],
            got.at[m, :, block(source, cols)],
            m_send.at[m, k - 1],
            m_recv.at[m, k - 1],
            (sp, ahead(k), tp),
        )

    def hand_out(m):
        for k in range(1, nf):
            mix_copy(m, k, ahead(k), fs).start()
        got[m, :, block(fs, cols)] = mine[m, fs]

    scale = HEAD_DIM ** (-0.5)
    head_gain = head[:, block(g, cols)]
    causal = row_at >= col_at
    for s in range(nf):
        rows = pl.ds(s * tokens, tokens)
        scores = lax.dot_general(
            query[rows, :], kv[rows, :cols], (((1,), (1,)), ((), ())), preferred_element_type=F32
        )
        sums = logs[:, s : s + 1]
        pairs = jnp.where(
            causal,
            sums - logs_t[s : s + 1, :] + logs_t[nf + s : nf + s + 1, :],
            FAR_BELOW,
        )
        carried = sums + carry_m[s : s + 1, 0:1]
        top = jnp.maximum(carried, jnp.max(pairs, axis=1, keepdims=True))
        weights = (jnp.exp(pairs - top) * scores).astype(BF16)
        cell = jnp.dot(weights, kv[rows, cols:], preferred_element_type=F32)
        cell = cell + jnp.exp(carried - top) * jnp.dot(
            query[rows, :], carry[s], preferred_element_type=F32
        )
        cell = cell * scale
        cell = cell * lax.rsqrt(jnp.mean(cell * cell, axis=-1, keepdims=True) + EPSILON)
        mine[1, s] = (cell * head_gain).astype(BF16)

    for d in range(1, ns - 1):
        z_step(MIX, d)
    hand_out(1)
    z_step(OUT, ns - 1)
    z_step(MIX, ns - 1)

    def rim_copy():
        return remote(
            padded.at[:, pl.ds(tokens, RIM), :],
            padded.at[:, pl.ds(0, RIM), :],
            r_send,
            r_recv,
            up,
        )

    def product(i, carried):
        both = jnp.dot(
            normed[tile(i), :],
            wbuf[:, SPANS[MIX][0] * cols : SPANS[GATE][0] * cols],
            preferred_element_type=F32,
        ).astype(BF16)
        both = both.astype(F32)
        padded[i, RIM:, :] = (both[:, :cols] * both[:, cols:]).astype(BF16).astype(F32)
        return carried

    lax.fori_loop(0, nf, product, 0)

    @pl.when(jnp.logical_not(has_down))
    def _():
        padded[:, 0:RIM, :] = jnp.zeros((nf, RIM, cols), F32)

    @pl.when(has_up)
    def _():
        rim_copy().start()

    gate_first, gate_count = SPANS[GATE]

    def gate_part(owner, first=False):
        def body(i, carried):
            part = jnp.dot(
                normed[tile(i), block(owner, depth)],
                wbuf[block(owner, depth), gate_first * cols : (gate_first + gate_count) * cols],
                preferred_element_type=F32,
            )
            gate_sum[tile(i), :] = part if first else gate_sum[tile(i), :] + part
            return carried

        lax.fori_loop(0, nf, body, 0)

    gate_part(sp, True)
    for d in range(1, ns - 1):
        z_step(GATE, d, gate_part)

    @pl.when(has_down)
    def _():
        rim_copy().wait_recv()

    tap = taps[:, block(g, cols)]
    for s in range(nf):
        total = jnp.zeros((tokens, cols), F32)
        for j in range(TAPS):
            at = RIM - (TAPS - 1) + j
            total = total + tap[j : j + 1, :] * padded[s, at : at + tokens, :]
        mixed[s * tokens : (s + 1) * tokens, :] = total

    def arrived(owner, carried):
        for k in range(1, nf):
            p_copy(owner, k, behind(k)).wait_recv()
        return carried

    lax.fori_loop(0, ns, arrived, 0)
    for k in range(1, nf):
        mix_copy(1, k, ahead(k), behind(k)).wait_recv()

    def memory_share(i, carried):
        acc[:, block(i, ocols)] = jnp.dot(
            got[1], wo[1, :, block(i, ocols)], preferred_element_type=F32
        )
        return carried

    lax.fori_loop(0, ns, memory_share, 0)

    z_step(GATE, ns - 1, gate_part)
    for s in range(nf):
        rows = slice(s * tokens, (s + 1) * tokens)
        mine[0, s] = (gate_sum[rows, :].astype(BF16).astype(F32) * mixed[rows, :]).astype(BF16)
    hand_out(0)
    for k in range(1, nf):
        mix_copy(0, k, ahead(k), behind(k)).wait_recv()

    def e_copy(i):
        return remote(
            acc.at[block(1 - tp, half), block(i, ocols)],
            other.at[:, block(i, ocols)],
            e_send.at[i],
            e_recv.at[i],
            partner,
        )

    def finish(i, carried):
        acc[:, block(i, ocols)] = acc[:, block(i, ocols)] + jnp.dot(
            got[0], wo[0, :, block(i, ocols)], preferred_element_type=F32
        )
        e_copy(i).start()
        return carried

    lax.fori_loop(0, ns, finish, 0)

    def merge(i, carried):
        e_copy(i).wait_recv()
        out_ref[:, block(i, ocols)] = (
            acc[block(tp, half), block(i, ocols)] + other[:, block(i, ocols)]
        ).astype(BF16)
        return carried

    lax.fori_loop(0, ns, merge, 0)

    def sent(i, carried):
        e_copy(i).wait_send()
        for k in range(1, nf):
            p_copy(i, k, fs).wait_send()
        return carried

    lax.fori_loop(0, ns, sent, 0)
    for k in range(1, nf):
        x_copy(k, fs).wait_send()
        d_copy(k, behind(k), tp).wait_send()
        for m in range(2):
            mix_copy(m, k, ahead(k), fs).wait_send()
    d_copy(0, fs, tp).wait_send()
    for side in range(2):
        for d in range(ns - 1):

            @pl.when(sends(side, d))
            def _():
                for part in range(PARTS):
                    z_copy(part, side, d, owner_of(side, d)).wait_send()

    @pl.when(has_up)
    def _():
        for copy in state_copies():
            copy.wait_send()
        rim_copy().wait_send()


def whole_layer(act, gain, weights, wi, wf, bias, decay, taps, head, w_out_conv, w_out_mem):
    ns, nf = (lax.axis_size("sp"), lax.axis_size("fs"))
    tokens, model = act.shape
    half = tokens // 2
    depth, cols = weights[0].shape
    ocols = w_out_conv.shape[1]
    count = nf * tokens
    anywhere = pl.BlockSpec(memory_space=pl.ANY)
    dma = pltpu.SemaphoreType.DMA
    vmem = pltpu.VMEM
    return pl.pallas_call(
        functools.partial(layer_kernel, ns, nf),
        out_shape=jax.ShapeDtypeStruct((half, ns * ocols), BF16),
        in_specs=[anywhere] * 16,
        out_specs=pl.BlockSpec(memory_space=pltpu.VMEM),
        scratch_shapes=[
            vmem((half, model), BF16),
            vmem(gain.shape, F32),
            vmem((count, model), BF16),
            vmem((ns * depth, 6 * cols), BF16),
            vmem(wi.shape, BF16),
            vmem(wf.shape, BF16),
            vmem(bias.shape, F32),
            vmem(decay.shape, F32),
            vmem(taps.shape, F32),
            vmem(head.shape, F32),
            vmem((2, nf * cols, ns * ocols), BF16),
            vmem((count, 2 * cols), BF16),
            vmem((count, cols), BF16),
            vmem((tokens, 128), F32),
            vmem((128, tokens), F32),
            vmem((nf, cols, cols), F32),
            vmem((2 * nf, 128), F32),
            vmem((nf, cols, cols), BF16),
            vmem((8, 128), F32),
            vmem((nf, cols, cols), BF16),
            vmem((8, 128), F32),
            vmem((nf, RIM + tokens, cols), F32),
            vmem((count, cols), F32),
            vmem((count, cols), F32),
            vmem((2, nf, tokens, cols), BF16),
            vmem((2, tokens, nf * cols), BF16),
            vmem((tokens, ns * ocols), F32),
            vmem((half, ns * ocols), F32),
            dma((16,)),
            dma((nf - 1,)),
            dma((nf - 1,)),
            dma((nf,)),
            dma((nf,)),
            dma((2, ns - 1, PARTS)),
            dma((2, ns - 1, PARTS)),
            dma((ns, nf - 1)),
            dma((ns, nf - 1)),
            dma((2,)),
            dma((2,)),
            dma,
            dma,
            dma((2, nf - 1)),
            dma((2, nf - 1)),
            dma((ns,)),
            dma((ns,)),
        ],
        compiler_params=pltpu.CompilerParams(
            collective_id=0, has_side_effects=True, vmem_limit_bytes=63 * 1024 * 1024
        ),
    )(act, gain, *weights, wi, wf, bias, decay, taps, head, w_out_conv, w_out_mem)


def shards(
    activations,
    norm_gain,
    w_conv_gate,
    w_conv_mult,
    w_conv_in,
    conv_taps,
    w_query,
    w_key,
    w_value,
    w_input_gate,
    w_forget_gate,
    gate_bias,
    decay_shift,
    head_gain,
    w_out_conv,
    w_out_mem,
):
    group_index = lax.axis_index(("fs", "tp"))
    heads_here = MEMORY_HEADS // (lax.axis_size("fs") * lax.axis_size("tp"))
    channels = w_conv_gate.shape[1]
    ns, nf, nt = (lax.axis_size("sp"), lax.axis_size("fs"), lax.axis_size("tp"))
    if 2 <= ns <= 8 and nf % 2 == 0 and nt == 2 and heads_here == 1 and channels == HEAD_DIM:
        return whole_layer(
            activations[0],
            norm_gain[None, :],
            (w_key, w_value, w_query, w_conv_mult, w_conv_in, w_conv_gate),
            w_input_gate,
            w_forget_gate,
            gate_bias,
            decay_shift,
            conv_taps,
            head_gain[None, :],
            w_out_conv,
            w_out_mem,
        )[None]
    sequences = lax.all_gather(activations, "fs", axis=0, tiled=True)
    seq_count = sequences.shape[0]
    tokens = sequences.shape[1]
    model_width = sequences.shape[2]
    row_count = seq_count * tokens
    flat_rows = sequences.reshape(row_count, model_width).astype(jnp.float32)
    normed = (
        flat_rows
        * lax.rsqrt(jnp.mean(flat_rows * flat_rows, axis=-1, keepdims=True) + EPSILON)
        * norm_gain
    ).astype(jnp.bfloat16)
    pieces = (
        lax.all_gather(w_conv_gate, "sp", axis=0, tiled=True),
        lax.all_gather(w_conv_mult, "sp", axis=0, tiled=True),
        lax.all_gather(w_conv_in, "sp", axis=0, tiled=True),
        lax.all_gather(w_query, "sp", axis=0, tiled=True),
        lax.all_gather(w_key, "sp", axis=0, tiled=True),
        lax.all_gather(w_value, "sp", axis=0, tiled=True),
    )
    projected = tuple(
        (jnp.dot(normed, shard_piece, preferred_element_type=jnp.float32) for shard_piece in pieces)
    )
    conv_gate, conv_mult, conv_in, query, keys_proj, value = [
        tensor.astype(jnp.bfloat16).reshape(seq_count, tokens, -1) for tensor in projected
    ]
    entry_cols = lax.dynamic_slice_in_dim(w_input_gate, group_index * heads_here, heads_here, 1)
    forget_cols = lax.dynamic_slice_in_dim(w_forget_gate, group_index * heads_here, heads_here, 1)
    gate_values = jnp.dot(
        normed,
        jnp.concatenate([entry_cols, forget_cols], axis=1),
        preferred_element_type=jnp.float32,
    ).reshape(seq_count, tokens, 2 * heads_here)
    product = (conv_mult.astype(jnp.float32) * conv_in.astype(jnp.float32)).astype(jnp.bfloat16)
    ntaps = conv_taps.shape[0]
    rim_rows = from_behind(product[:, tokens - (ntaps - 1) :, :], "sp", 1)
    padded = jnp.concatenate([rim_rows, product], axis=1).astype(jnp.float32)
    tap_weights = lax.dynamic_slice_in_dim(conv_taps, group_index * channels, channels, 1)
    mixed_sum = jnp.zeros((seq_count, tokens, channels), jnp.float32)
    for tap_index in range(ntaps):
        mixed_sum = (
            mixed_sum + tap_weights[tap_index] * padded[:, tap_index : tap_index + tokens, :]
        )
    conv_out = (conv_gate.astype(jnp.float32) * mixed_sum).astype(jnp.bfloat16)
    bias_rows = lax.dynamic_slice_in_dim(gate_bias, group_index * heads_here, heads_here, 1)
    decay_rows = lax.dynamic_slice_in_dim(decay_shift, group_index * heads_here, heads_here, 2)
    entry = gate_values[..., :heads_here] + bias_rows[0]
    log_forget = jax.nn.log_sigmoid(gate_values[..., heads_here:] + bias_rows[1]) + decay_rows
    cell = memory_cell(
        head_rows(query, seq_count, heads_here),
        head_rows(keys_proj, seq_count, heads_here),
        head_rows(value, seq_count, heads_here),
        gate_rows(entry, seq_count, heads_here),
        gate_rows(log_forget, seq_count, heads_here),
    )
    cell = cell * lax.rsqrt(jnp.mean(cell * cell, axis=-1, keepdims=True) + EPSILON)
    gain_rows = lax.dynamic_slice_in_dim(
        head_gain, group_index * heads_here * HEAD_DIM, heads_here * HEAD_DIM, 0
    ).reshape(1, heads_here, 1, HEAD_DIM)
    scaled = cell.reshape(seq_count, heads_here, tokens, HEAD_DIM) * gain_rows
    mem_out = (
        scaled.transpose(0, 2, 1, 3)
        .reshape(seq_count, tokens, heads_here * HEAD_DIM)
        .astype(jnp.bfloat16)
    )
    conv_seq, mem_seq = (
        lax.all_to_all(conv_out, "fs", split_axis=0, concat_axis=2, tiled=True),
        lax.all_to_all(mem_out, "fs", split_axis=0, concat_axis=2, tiled=True),
    )
    rows_conv, rows_mem = (
        lax.all_gather(w_out_conv, "fs", axis=0, tiled=True),
        lax.all_gather(w_out_mem, "fs", axis=0, tiled=True),
    )
    full_conv, full_mem = (
        lax.all_gather(rows_conv, "sp", axis=1, tiled=True),
        lax.all_gather(rows_mem, "sp", axis=1, tiled=True),
    )
    conv_flat = conv_seq[0]
    mem_flat = mem_seq[0]
    output = lax.psum_scatter(
        (
            jnp.dot(conv_flat, full_conv, preferred_element_type=jnp.float32)
            + jnp.dot(mem_flat, full_mem, preferred_element_type=jnp.float32)
        ).astype(jnp.bfloat16),
        "tp",
        scatter_dimension=0,
        tiled=True,
    ).astype(jnp.float32)
    return output.astype(jnp.bfloat16).reshape(1, output.shape[0], -1)


def solution(mesh):
    return jax.shard_map(
        shards,
        mesh=mesh,
        in_specs=(
            P("fs", "sp", None),
            P(),
            P("sp", ("fs", "tp")),
            P("sp", ("fs", "tp")),
            P("sp", ("fs", "tp")),
            P(),
            P("sp", ("fs", "tp")),
            P("sp", ("fs", "tp")),
            P("sp", ("fs", "tp")),
            P(),
            P(),
            P(),
            P(None, "sp", None),
            P(),
            P(("fs", "tp"), "sp"),
            P(("fs", "tp"), "sp"),
        ),
        out_specs=P("fs", ("sp", "tp"), None),
        check_vma=False,
    )
```

```python
import functools

import jax
import jax.numpy as jnp
from jax import lax
from jax.experimental import pallas as pl
from jax.experimental.pallas import tpu as pltpu
from jax.sharding import PartitionSpec as P

MEMORY_HEADS = 8
HEAD_DIM = 128
BLOCK = 64


EPSILON = 1e-06
FAR_BELOW = -1e30
HIGHEST_PRECISION = lax.Precision.HIGHEST


def prefix(value, axis, join, neutral):
    count, mine = (lax.axis_size(axis), lax.axis_index(axis))
    total, peak, state = value
    stats = jnp.stack([total, peak], axis=1)[..., None]
    stats = jnp.broadcast_to(stats, stats.shape[:2] + state.shape[-1:])
    packed = lax.all_gather(jnp.concatenate([state, stats], axis=1), axis)
    height = state.shape[1]
    pieces = (packed[:, :, height, 0], packed[:, :, height + 1, 0], packed[:, :, :height])
    subtotal = jax.tree.map(
        lambda part, zero: jnp.full_like(part, 0) + jnp.asarray(zero, part.dtype), value, neutral
    )

    def lap(position, subtotal):
        longer = join(subtotal, jax.tree.map(lambda part: part[position], pieces))
        return jax.tree.map(lambda new, old: jnp.where(position < mine, new, old), longer, subtotal)

    return lax.fori_loop(0, count - 1, lap, subtotal)


def from_behind(array, axis, by):
    peers = lax.axis_size(axis)
    pairs = [(i, i + by) for i in range(peers) if 0 <= i + by < peers]
    return lax.ppermute(array, axis, pairs)


def combine_states(earlier, later):
    total_one, peak_one, state_one = earlier
    total_two, peak_two, state_two = later
    peak_new = jnp.maximum(total_two + peak_one, peak_two)
    scale_old = jnp.exp(total_two + peak_one - peak_new)
    scale_new = jnp.exp(peak_two - peak_new)
    return (
        total_one + total_two,
        peak_new,
        scale_old[..., None, None] * state_one + scale_new[..., None, None] * state_two,
    )


def head_rows(values, seq_count, heads_here):
    tokens = values.shape[1]
    split_heads = values.reshape(seq_count, tokens, heads_here, HEAD_DIM).transpose(0, 2, 1, 3)
    return split_heads.reshape(seq_count * heads_here, tokens, HEAD_DIM).astype(jnp.float32)


def gate_rows(values, seq_count, heads_here):
    tokens = values.shape[1]
    return values.transpose(0, 2, 1).reshape(seq_count * heads_here, tokens)


def memory_cell(query_rows, key_rows, value_rows, entry_gate, log_forget):
    members = query_rows.shape[0]
    tokens = query_rows.shape[1]
    head_width = query_rows.shape[2]
    nblocks = tokens // BLOCK
    block_shape = (members, nblocks, BLOCK, head_width)
    query_blocks = query_rows.reshape(block_shape)
    key_blocks = key_rows.reshape(block_shape) * head_width ** (-0.5)
    value_blocks = value_rows.reshape(block_shape)
    entry_blocks = entry_gate.reshape(members, nblocks, BLOCK)
    forget_sums = jnp.cumsum(log_forget.reshape(members, nblocks, BLOCK), axis=-1)
    block_total = forget_sums[..., -1]
    local_logs = block_total[..., None] - forget_sums + entry_blocks
    local_peak = jnp.max(local_logs, axis=-1)
    local_weights = jnp.exp(local_logs - local_peak[..., None])
    local_state = jnp.einsum(
        "bclv,bclk->bcvk",
        local_weights[..., None] * value_blocks,
        key_blocks,
        precision=HIGHEST_PRECISION,
    )

    def advance(running, block_item):
        return (combine_states(running, block_item), running)

    zero_sums = jnp.zeros((members,), jnp.float32)
    low_peaks = jnp.full((members,), FAR_BELOW, jnp.float32)
    zero_states = jnp.zeros((members, head_width, head_width), jnp.float32)
    block_items = (
        jnp.moveaxis(block_total, 1, 0),
        jnp.moveaxis(local_peak, 1, 0),
        jnp.moveaxis(local_state, 1, 0),
    )
    device_total, inner_states = lax.scan(advance, (zero_sums, low_peaks, zero_states), block_items)
    inner_states = tuple((jnp.moveaxis(tensor, 0, 1) for tensor in inner_states))
    total_sum, total_peak, total_state = device_total
    before = prefix(
        (total_sum, total_peak, total_state),
        "sp",
        combine_states,
        (zero_sums, low_peaks, zero_states),
    )
    opening = combine_states((zero_sums, zero_sums, zero_states), before)
    opening = tuple((tensor[:, None] for tensor in opening))
    _, prior_peak, prior_state = combine_states(opening, inner_states)
    positions = jnp.arange(BLOCK)
    causal_mask = positions[:, None] >= positions[None, :]
    pair_logs = jnp.where(
        causal_mask,
        forget_sums[..., :, None] - forget_sums[..., None, :] + entry_blocks[..., None, :],
        -jnp.inf,
    )
    carried_logs = forget_sums + prior_peak[..., None]
    row_peak = jnp.maximum(carried_logs, jnp.max(pair_logs, axis=-1))
    inner_weights = jnp.exp(pair_logs - row_peak[..., None])
    carried_weights = jnp.exp(carried_logs - row_peak)
    scores = inner_weights * jnp.einsum(
        "bcld,bcsd->bcls", query_blocks, key_blocks, precision=HIGHEST_PRECISION
    )
    numerator = carried_weights[..., None] * jnp.einsum(
        "bcvk,bclk->bclv", prior_state, query_blocks, precision=HIGHEST_PRECISION
    ) + jnp.einsum("bcls,bcsv->bclv", scores, value_blocks, precision=HIGHEST_PRECISION)
    return numerator.reshape(members, tokens, head_width)


MESH = pl.DeviceIdType.MESH
F32 = jnp.float32
BF16 = jnp.bfloat16
TAPS = 3
RIM = 8
KV, QUERY, OUT, MIX, GATE = range(5)
SPANS = {KV: (0, 2), QUERY: (2, 1), MIX: (3, 2), GATE: (5, 1)}
PARTS = 5


def layer_kernel(
    ns,
    nf,
    act_ref,
    gain_ref,
    w0_ref,
    w1_ref,
    w2_ref,
    w3_ref,
    w4_ref,
    w5_ref,
    wi_ref,
    wf_ref,
    bias_ref,
    decay_ref,
    taps_ref,
    head_ref,
    wc_ref,
    wm_ref,
    out_ref,
    raw,
    gain,
    normed,
    wbuf,
    wi,
    wf,
    bias,
    decay,
    taps,
    head,
    wo,
    kv,
    query,
    logs,
    logs_t,
    local_state,
    local_stat,
    carry,
    carry_m,
    passed,
    passed_m,
    padded,
    mixed,
    gate_sum,
    mine,
    got,
    acc,
    other,
    load_sem,
    x_send,
    x_recv,
    d_send,
    d_recv,
    w_send,
    w_recv,
    p_send,
    p_recv,
    s_send,
    s_recv,
    r_send,
    r_recv,
    m_send,
    m_recv,
    e_send,
    e_recv,
):
    sp, fs, tp = (lax.axis_index("sp"), lax.axis_index("fs"), lax.axis_index("tp"))
    g = fs * 2 + tp
    depth, cols = w0_ref.shape
    half, model = raw.shape
    tokens = 2 * half
    ocols = wc_ref.shape[1]
    partner = (sp, fs, 1 - tp)
    has_up, has_down = (sp + 1 < ns, sp > 0)
    up, down = ((sp + 1, fs, tp), (sp - 1, fs, tp))
    fy, fx = (fs // 2, lax.rem(fs, 2))
    beside = (fy * 2 + 1 - fx, (1 - fy) * 2 + fx, (1 - fy) * 2 + 1 - fx)

    def block(index, size):
        return pl.ds(pl.multiple_of(index * size, size), size)

    def remote(src, dst, send, recv, to):
        return pltpu.make_async_remote_copy(
            src, dst, send, recv, device_id=to, device_id_type=MESH
        )

    loads = [pltpu.make_async_copy(act_ref.at[block(tp, half)], raw, load_sem.at[0])]
    loads.append(pltpu.make_async_copy(gain_ref, gain, load_sem.at[1]))
    for j, ref in enumerate((w0_ref, w1_ref, w2_ref, w3_ref, w4_ref, w5_ref)):
        loads.append(
            pltpu.make_async_copy(
                ref, wbuf.at[block(sp, depth), pl.ds(j * cols, cols)], load_sem.at[2 + j]
            )
        )
    for m, ref in enumerate((wc_ref, wm_ref)):
        loads.append(
            pltpu.make_async_copy(
                ref, wo.at[m, block(fs, cols), block(sp, ocols)], load_sem.at[8 + m]
            )
        )
    smalls = (
        (wi_ref, wi),
        (wf_ref, wf),
        (bias_ref, bias),
        (decay_ref, decay),
        (taps_ref, taps),
        (head_ref, head),
    )
    for j, (ref, held) in enumerate(smalls):
        loads.append(pltpu.make_async_copy(ref, held, load_sem.at[10 + j]))
    for j in (2, 3, 0, 1, 4, 8, 9, 5, 6, 7, 10, 11, 12, 13, 14, 15):
        loads[j].start()

    barrier = pltpu.get_barrier_semaphore()
    for peer in beside:
        pl.semaphore_signal(barrier, inc=1, device_id=(sp, peer, tp), device_id_type=MESH)
    pl.semaphore_signal(barrier, inc=1, device_id=partner, device_id_type=MESH)

    @pl.when(has_up)
    def _():
        pl.semaphore_signal(barrier, inc=1, device_id=up, device_id_type=MESH)

    @pl.when(has_down)
    def _():
        pl.semaphore_signal(barrier, inc=1, device_id=down, device_id_type=MESH)

    def place(part, owner):
        if part == OUT:
            return wo.at[:, block(fs, cols), block(owner, ocols)]
        first, count = SPANS[part]
        return wbuf.at[block(owner, depth), pl.ds(first * cols, count * cols)]

    def z_copy(part, side, d, owner):
        there = place(part, owner)
        return remote(
            there,
            there,
            w_send.at[side, d, part],
            w_recv.at[side, d, part],
            (up, down)[side],
        )

    def owner_of(side, d):
        return sp - d if side == 0 else sp + d

    def arrives(side, d):
        return (sp - d >= 0) if side == 0 else (sp + d < ns)

    def sends(side, d):
        return arrives(side, d) & (has_up if side == 0 else has_down)

    def z_send(part, side, d):
        @pl.when(sends(side, d))
        def _():
            z_copy(part, side, d, owner_of(side, d)).start()

    def own(part):
        for side in range(2):
            z_send(part, side, 0)

    def p_copy(owner, way, row):
        span = ((0, 2), (0, 2), (0, 1), (1, 1))[way]
        there = wo.at[pl.ds(*span), block(row, cols), block(owner, ocols)]
        return remote(
            there,
            there,
            p_send.at[owner, way],
            p_recv.at[owner, way],
            (sp, beside[(0, 1, 1, 0)[way]], tp),
        )

    def spread(owner):
        for way in range(2):
            p_copy(owner, way, fs).start()

    def pass_on(owner):
        for way in range(2):
            p_copy(owner, way, beside[way]).wait_recv()
            p_copy(owner, way + 2, beside[way]).start()

    def pass_step(d):
        for side in range(2):

            @pl.when(arrives(side, d))
            def _():
                pass_on(owner_of(side, d))

    def z_step(part, d, use=None):
        for side in range(2):

            @pl.when(arrives(side, d))
            def _():
                owner = owner_of(side, d)
                z_copy(part, side, d - 1, owner).wait_recv()
                if d < ns - 1:
                    z_send(part, side, d)
                if part == OUT:
                    spread(owner)
                if use is not None:
                    use(owner)

    def x_copy(way, seq):
        first, rows = ((0, half), (0, half), (0, half // 2), (half // 2, half // 2))[way]
        there = normed.at[pl.ds(pl.multiple_of(seq * tokens + tp * half + first, rows), rows)]
        return remote(
            there, there, x_send.at[way], x_recv.at[way], (sp, beside[(0, 1, 1, 0)[way]], tp)
        )

    def d_copy(k, seq, part):
        there = normed.at[pl.ds(pl.multiple_of(seq * tokens + part * half, half), half)]
        return remote(there, there, d_send.at[k], d_recv.at[k], partner)

    loads[2].wait()
    loads[3].wait()
    pl.semaphore_wait(barrier, nf + has_up.astype(jnp.int32) + has_down.astype(jnp.int32))
    own(KV)
    loads[0].wait()
    loads[1].wait()
    step = 32

    def norm_rows(i, carried):
        x = raw[pl.ds(pl.multiple_of(i * step, step), step), :].astype(F32)
        scale = lax.rsqrt(jnp.mean(x * x, axis=-1, keepdims=True) + EPSILON)
        rows = pl.ds(pl.multiple_of(fs * tokens + tp * half + i * step, step), step)
        normed[rows, :] = (x * scale * gain[...]).astype(BF16)
        return carried

    lax.fori_loop(0, half // step, norm_rows, 0)
    loads[4].wait()
    own(QUERY)
    for way in range(2):
        x_copy(way, fs).start()
    d_copy(0, fs, tp).start()
    loads[8].wait()
    loads[9].wait()
    z_step(KV, 1)
    z_step(QUERY, 1)
    for d in range(2, ns - 1):
        z_step(KV, d)
    for way in range(2):
        x_copy(way, beside[way]).wait_recv()
        x_copy(way + 2, beside[way]).start()
        d_copy(way + 1, beside[way], tp).start()
    own(OUT)
    spread(sp)
    for d in range(2, ns - 1):
        z_step(QUERY, d)
    for j in (5, 6, 7, 10, 11, 12, 13, 14, 15):
        loads[j].wait()
    own(MIX)
    for way in range(2, 4):
        x_copy(way, beside[2]).wait_recv()
    d_copy(3, beside[2], tp).start()
    own(GATE)
    z_step(KV, ns - 1)
    for k, seq in enumerate((fs,) + beside):
        d_copy(k, seq, 1 - tp).wait_recv()

    def tile(i):
        return pl.ds(pl.multiple_of(i * tokens, tokens), tokens)

    def project(part, into):
        first, count = SPANS[part]

        def body(i, carried):
            into[tile(i), :] = jnp.dot(
                normed[tile(i), :],
                wbuf[:, first * cols : (first + count) * cols],
                preferred_element_type=F32,
            ).astype(BF16)
            return carried

        lax.fori_loop(0, nf, body, 0)

    row_at = lax.broadcasted_iota(jnp.int32, (tokens, tokens), 0)
    col_at = lax.broadcasted_iota(jnp.int32, (tokens, tokens), 1)
    gates = jnp.concatenate([wi[...].astype(F32), wf[...].astype(F32)], axis=0).astype(BF16)
    heads = wi.shape[0]
    own_gate = lax.broadcasted_iota(jnp.int32, (2 * heads, tokens), 0)
    own_bias = lax.broadcasted_iota(jnp.int32, (1, heads), 1)
    bias_in = jnp.sum(jnp.where(own_bias == g, bias[0:1, :], 0.0), axis=1, keepdims=True)
    bias_out = jnp.sum(jnp.where(own_bias == g, bias[1:2, :], 0.0), axis=1, keepdims=True)
    line = lax.broadcasted_iota(jnp.int32, (128, tokens), 0)
    packed = jnp.zeros((128, tokens), F32)
    for s in range(nf):
        raw_gates = lax.dot_general(
            gates,
            normed[s * tokens : (s + 1) * tokens, :],
            (((1,), (1,)), ((), ())),
            preferred_element_type=F32,
        )
        entry = jnp.sum(jnp.where(own_gate == g, raw_gates, 0.0), axis=0, keepdims=True) + bias_in
        forget = (
            jnp.sum(jnp.where(own_gate == heads + g, raw_gates, 0.0), axis=0, keepdims=True)
            + bias_out
        )
        shift = jnp.sum(jnp.where(own_gate[:heads] == g, decay[s], 0.0), axis=0, keepdims=True)
        forget = jnp.minimum(forget, 0.0) - jnp.log1p(jnp.exp(-jnp.abs(forget))) + shift
        packed = jnp.where(line == s, forget, packed)
        packed = jnp.where(line == nf + s, entry, packed)
    ones = jnp.where(row_at <= col_at, 1.0, 0.0).astype(F32)
    sums = jnp.dot(packed, ones, precision=HIGHEST_PRECISION, preferred_element_type=F32)
    sums = jnp.where(line < nf, sums, packed)
    logs_t[...] = sums
    logs[...] = sums.T
    project(KV, kv)
    for s in range(nf):
        rows = pl.ds(s * tokens, tokens)
        total = logs_t[s : s + 1, tokens - 1 : tokens]
        reach = total - logs[:, s : s + 1] + logs[:, nf + s : nf + s + 1]
        peak = jnp.max(reach, axis=0, keepdims=True)
        weighted = (kv[rows, cols:].astype(F32) * jnp.exp(reach - peak)).astype(BF16)
        local_state[s] = lax.dot_general(
            kv[rows, :cols], weighted, (((0,), (0,)), ((), ())), preferred_element_type=F32
        )
        local_stat[s : s + 1, :] = jnp.broadcast_to(total, (1, 128))
        local_stat[nf + s : nf + s + 1, :] = jnp.broadcast_to(peak, (1, 128))

    pass_on(sp)
    z_step(OUT, 1)

    def state_copies():
        return (
            remote(passed_m, carry_m, s_send.at[0], s_recv.at[0], up),
            remote(passed, carry, s_send.at[1], s_recv.at[1], up),
        )

    @pl.when(jnp.logical_not(has_down))
    def _():
        carry[...] = jnp.zeros_like(carry)
        carry_m[...] = jnp.zeros_like(carry_m)

    @pl.when(has_down)
    def _():
        for copy in state_copies():
            copy.wait_recv()

    @pl.when(has_up)
    def _():
        for s in range(nf):
            before = local_stat[s : s + 1, :] + carry_m[s : s + 1, :]
            peak = local_stat[nf + s : nf + s + 1, :]
            top = jnp.maximum(before, peak)
            passed[s] = (
                jnp.exp(before - top) * carry[s].astype(F32) + jnp.exp(peak - top) * local_state[s]
            ).astype(BF16)
            passed_m[s : s + 1, :] = top
        for copy in state_copies():
            copy.start()

    z_step(QUERY, ns - 1)
    for d in range(2, ns - 1):
        z_step(OUT, d)
    pass_step(1)
    z_step(OUT, ns - 1)
    z_step(MIX, 1)
    for d in range(2, ns - 1):
        pass_step(d)
        z_step(MIX, d)
    project(QUERY, query)

    def mix_copy(m, k, seq, source):
        return remote(
            mine.at[m, seq],
            got.at[m, :, block(source, cols)],
            m_send.at[m, k],
            m_recv.at[m, k],
            (sp, beside[k], tp),
        )

    def hand_out(m):
        for k in (2, 0, 1):
            mix_copy(m, k, beside[k], fs).start()
        got[m, :, block(fs, cols)] = mine[m, fs]

    scale = HEAD_DIM ** (-0.5)
    head_gain = head[:, block(g, cols)]
    causal = row_at >= col_at
    for s in range(nf):
        rows = pl.ds(s * tokens, tokens)
        scores = lax.dot_general(
            query[rows, :], kv[rows, :cols], (((1,), (1,)), ((), ())), preferred_element_type=F32
        )
        sums = logs[:, s : s + 1]
        pairs = jnp.where(
            causal,
            sums - logs_t[s : s + 1, :] + logs_t[nf + s : nf + s + 1, :],
            FAR_BELOW,
        )
        carried = sums + carry_m[s : s + 1, 0:1]
        top = jnp.maximum(carried, jnp.max(pairs, axis=1, keepdims=True))
        weights = (jnp.exp(pairs - top) * scores).astype(BF16)
        cell = jnp.dot(weights, kv[rows, cols:], preferred_element_type=F32)
        cell = cell + jnp.exp(carried - top) * jnp.dot(
            query[rows, :], carry[s], preferred_element_type=F32
        )
        cell = cell * scale
        cell = cell * lax.rsqrt(jnp.mean(cell * cell, axis=-1, keepdims=True) + EPSILON)
        mine[1, s] = (cell * head_gain).astype(BF16)

    hand_out(1)
    gate_first, gate_count = SPANS[GATE]

    def gate_part(owner, first=False):
        def body(i, carried):
            part = jnp.dot(
                normed[tile(i), block(owner, depth)],
                wbuf[block(owner, depth), gate_first * cols : (gate_first + gate_count) * cols],
                preferred_element_type=F32,
            )
            gate_sum[tile(i), :] = part if first else gate_sum[tile(i), :] + part
            return carried

        lax.fori_loop(0, nf, body, 0)

    gate_part(sp, True)
    z_step(GATE, 1, gate_part)
    pass_step(ns - 1)
    z_step(MIX, ns - 1)
    for d in range(2, ns - 1):
        z_step(GATE, d, gate_part)

    def rim_copy():
        return remote(
            padded.at[:, pl.ds(tokens, RIM), :],
            padded.at[:, pl.ds(0, RIM), :],
            r_send,
            r_recv,
            up,
        )

    def product(i, carried):
        both = jnp.dot(
            normed[tile(i), :],
            wbuf[:, SPANS[MIX][0] * cols : SPANS[GATE][0] * cols],
            preferred_element_type=F32,
        ).astype(BF16)
        both = both.astype(F32)
        padded[i, RIM:, :] = (both[:, :cols] * both[:, cols:]).astype(BF16).astype(F32)
        return carried

    lax.fori_loop(0, nf, product, 0)

    @pl.when(jnp.logical_not(has_down))
    def _():
        padded[:, 0:RIM, :] = jnp.zeros((nf, RIM, cols), F32)

    @pl.when(has_up)
    def _():
        rim_copy().start()

    @pl.when(has_down)
    def _():
        rim_copy().wait_recv()

    tap = taps[:, block(g, cols)]
    for s in range(nf):
        total = jnp.zeros((tokens, cols), F32)
        for j in range(TAPS):
            at = RIM - (TAPS - 1) + j
            total = total + tap[j : j + 1, :] * padded[s, at : at + tokens, :]
        mixed[s * tokens : (s + 1) * tokens, :] = total

    def arrived(owner, carried):
        for way in range(2, 4):
            p_copy(owner, way, beside[2]).wait_recv()
        return carried

    lax.fori_loop(0, ns, arrived, 0)
    for k in range(nf - 1):
        mix_copy(1, k, beside[k], beside[k]).wait_recv()

    def memory_share(i, carried):
        acc[:, block(i, ocols)] = jnp.dot(
            got[1], wo[1, :, block(i, ocols)], preferred_element_type=F32
        )
        return carried

    lax.fori_loop(0, ns, memory_share, 0)

    z_step(GATE, ns - 1)
    at_end = jnp.logical_not(has_up & has_down)
    farthest = lax.rem(sp + ns - 1, 2 * (ns - 1))

    def convolve(seq):
        @pl.when(at_end)
        def _():
            gate_sum[tile(seq), :] = gate_sum[tile(seq), :] + jnp.dot(
                normed[tile(seq), block(farthest, depth)],
                wbuf[
                    block(farthest, depth), gate_first * cols : (gate_first + gate_count) * cols
                ],
                preferred_element_type=F32,
            )

        return (gate_sum[tile(seq), :].astype(BF16).astype(F32) * mixed[tile(seq), :]).astype(BF16)

    order = (2, 0, 1)
    for step, k in enumerate(order):
        mine[0, beside[k]] = convolve(beside[k])
        if step > 0:
            mix_copy(0, order[step - 1], beside[order[step - 1]], fs).start()
    got[0, :, block(fs, cols)] = convolve(fs)
    mix_copy(0, order[-1], beside[order[-1]], fs).start()

    def e_copy(i):
        return remote(
            acc.at[block(1 - tp, half), block(i, ocols)],
            other.at[:, block(i, ocols)],
            e_send.at[i],
            e_recv.at[i],
            partner,
        )

    def add_pair(i, pair):
        acc[:, block(i, ocols)] = acc[:, block(i, ocols)] + jnp.dot(
            got[0, :, block(pair, 2 * cols)],
            wo[0, block(pair, 2 * cols), block(i, ocols)],
            preferred_element_type=F32,
        )

    mix_copy(0, 0, beside[0], beside[0]).wait_recv()
    for i in range(ns):
        add_pair(i, fy)
    for k in (1, 2):
        mix_copy(0, k, beside[k], beside[k]).wait_recv()
    for i in range(ns):
        add_pair(i, 1 - fy)
        if i > 0:
            e_copy(i - 1).start()
    e_copy(ns - 1).start()

    def merge(i, carried):
        e_copy(i).wait_recv()
        out_ref[:, block(i, ocols)] = (
            acc[block(tp, half), block(i, ocols)] + other[:, block(i, ocols)]
        ).astype(BF16)
        return carried

    lax.fori_loop(0, ns, merge, 0)

    def sent(i, carried):
        e_copy(i).wait_send()
        for way in range(4):
            p_copy(i, way, (fs, fs, beside[0], beside[1])[way]).wait_send()
        return carried

    lax.fori_loop(0, ns, sent, 0)
    for way in range(4):
        x_copy(way, (fs, fs, beside[0], beside[1])[way]).wait_send()
    for k, seq in enumerate((fs,) + beside):
        d_copy(k, seq, tp).wait_send()
    for k in range(nf - 1):
        for m in range(2):
            mix_copy(m, k, beside[k], fs).wait_send()
    for side in range(2):
        for d in range(ns - 1):

            @pl.when(sends(side, d))
            def _():
                for part in range(PARTS):
                    z_copy(part, side, d, owner_of(side, d)).wait_send()

    @pl.when(has_up)
    def _():
        for copy in state_copies():
            copy.wait_send()
        rim_copy().wait_send()


def whole_layer(act, gain, weights, wi, wf, bias, decay, taps, head, w_out_conv, w_out_mem):
    ns, nf = (lax.axis_size("sp"), lax.axis_size("fs"))
    tokens, model = act.shape
    half = tokens // 2
    depth, cols = weights[0].shape
    ocols = w_out_conv.shape[1]
    count = nf * tokens
    anywhere = pl.BlockSpec(memory_space=pl.ANY)
    dma = pltpu.SemaphoreType.DMA
    vmem = pltpu.VMEM
    return pl.pallas_call(
        functools.partial(layer_kernel, ns, nf),
        out_shape=pltpu.VMEM((half, ns * ocols), BF16),
        in_specs=[anywhere] * 16,
        out_specs=pl.BlockSpec(memory_space=pltpu.VMEM),
        scratch_shapes=[
            vmem((half, model), BF16),
            vmem(gain.shape, F32),
            vmem((count, model), BF16),
            vmem((ns * depth, 6 * cols), BF16),
            vmem(wi.shape, BF16),
            vmem(wf.shape, BF16),
            vmem(bias.shape, F32),
            vmem(decay.shape, F32),
            vmem(taps.shape, F32),
            vmem(head.shape, F32),
            vmem((2, nf * cols, ns * ocols), BF16),
            vmem((count, 2 * cols), BF16),
            vmem((count, cols), BF16),
            vmem((tokens, 128), F32),
            vmem((128, tokens), F32),
            vmem((nf, cols, cols), F32),
            vmem((2 * nf, 128), F32),
            vmem((nf, cols, cols), BF16),
            vmem((8, 128), F32),
            vmem((nf, cols, cols), BF16),
            vmem((8, 128), F32),
            vmem((nf, RIM + tokens, cols), F32),
            vmem((count, cols), F32),
            vmem((count, cols), F32),
            vmem((2, nf, tokens, cols), BF16),
            vmem((2, tokens, nf * cols), BF16),
            vmem((tokens, ns * ocols), F32),
            vmem((half, ns * ocols), F32),
            dma((16,)),
            dma((4,)),
            dma((4,)),
            dma((nf,)),
            dma((nf,)),
            dma((2, ns - 1, PARTS)),
            dma((2, ns - 1, PARTS)),
            dma((ns, 4)),
            dma((ns, 4)),
            dma((2,)),
            dma((2,)),
            dma,
            dma,
            dma((2, nf - 1)),
            dma((2, nf - 1)),
            dma((ns,)),
            dma((ns,)),
        ],
        compiler_params=pltpu.CompilerParams(
            collective_id=0, has_side_effects=True, vmem_limit_bytes=54 * 1024 * 1024
        ),
    )(act, gain, *weights, wi, wf, bias, decay, taps, head, w_out_conv, w_out_mem)


def shards(
    activations,
    norm_gain,
    w_conv_gate,
    w_conv_mult,
    w_conv_in,
    conv_taps,
    w_query,
    w_key,
    w_value,
    w_input_gate,
    w_forget_gate,
    gate_bias,
    decay_shift,
    head_gain,
    w_out_conv,
    w_out_mem,
):
    group_index = lax.axis_index(("fs", "tp"))
    heads_here = MEMORY_HEADS // (lax.axis_size("fs") * lax.axis_size("tp"))
    channels = w_conv_gate.shape[1]
    ns, nf, nt = (lax.axis_size("sp"), lax.axis_size("fs"), lax.axis_size("tp"))
    if 2 <= ns <= 8 and nf == 4 and nt == 2 and heads_here == 1 and channels == HEAD_DIM:
        return whole_layer(
            activations[0],
            norm_gain[None, :],
            (w_key, w_value, w_query, w_conv_mult, w_conv_in, w_conv_gate),
            w_input_gate.T,
            w_forget_gate.T,
            gate_bias,
            decay_shift.transpose(0, 2, 1),
            conv_taps,
            head_gain[None, :],
            w_out_conv,
            w_out_mem,
        )[None]
    sequences = lax.all_gather(activations, "fs", axis=0, tiled=True)
    seq_count = sequences.shape[0]
    tokens = sequences.shape[1]
    model_width = sequences.shape[2]
    row_count = seq_count * tokens
    flat_rows = sequences.reshape(row_count, model_width).astype(jnp.float32)
    normed = (
        flat_rows
        * lax.rsqrt(jnp.mean(flat_rows * flat_rows, axis=-1, keepdims=True) + EPSILON)
        * norm_gain
    ).astype(jnp.bfloat16)
    pieces = (
        lax.all_gather(w_conv_gate, "sp", axis=0, tiled=True),
        lax.all_gather(w_conv_mult, "sp", axis=0, tiled=True),
        lax.all_gather(w_conv_in, "sp", axis=0, tiled=True),
        lax.all_gather(w_query, "sp", axis=0, tiled=True),
        lax.all_gather(w_key, "sp", axis=0, tiled=True),
        lax.all_gather(w_value, "sp", axis=0, tiled=True),
    )
    projected = tuple(
        (jnp.dot(normed, shard_piece, preferred_element_type=jnp.float32) for shard_piece in pieces)
    )
    conv_gate, conv_mult, conv_in, query, keys_proj, value = [
        tensor.astype(jnp.bfloat16).reshape(seq_count, tokens, -1) for tensor in projected
    ]
    entry_cols = lax.dynamic_slice_in_dim(w_input_gate, group_index * heads_here, heads_here, 1)
    forget_cols = lax.dynamic_slice_in_dim(w_forget_gate, group_index * heads_here, heads_here, 1)
    gate_values = jnp.dot(
        normed,
        jnp.concatenate([entry_cols, forget_cols], axis=1),
        preferred_element_type=jnp.float32,
    ).reshape(seq_count, tokens, 2 * heads_here)
    product = (conv_mult.astype(jnp.float32) * conv_in.astype(jnp.float32)).astype(jnp.bfloat16)
    ntaps = conv_taps.shape[0]
    rim_rows = from_behind(product[:, tokens - (ntaps - 1) :, :], "sp", 1)
    padded = jnp.concatenate([rim_rows, product], axis=1).astype(jnp.float32)
    tap_weights = lax.dynamic_slice_in_dim(conv_taps, group_index * channels, channels, 1)
    mixed_sum = jnp.zeros((seq_count, tokens, channels), jnp.float32)
    for tap_index in range(ntaps):
        mixed_sum = (
            mixed_sum + tap_weights[tap_index] * padded[:, tap_index : tap_index + tokens, :]
        )
    conv_out = (conv_gate.astype(jnp.float32) * mixed_sum).astype(jnp.bfloat16)
    bias_rows = lax.dynamic_slice_in_dim(gate_bias, group_index * heads_here, heads_here, 1)
    decay_rows = lax.dynamic_slice_in_dim(decay_shift, group_index * heads_here, heads_here, 2)
    entry = gate_values[..., :heads_here] + bias_rows[0]
    log_forget = jax.nn.log_sigmoid(gate_values[..., heads_here:] + bias_rows[1]) + decay_rows
    cell = memory_cell(
        head_rows(query, seq_count, heads_here),
        head_rows(keys_proj, seq_count, heads_here),
        head_rows(value, seq_count, heads_here),
        gate_rows(entry, seq_count, heads_here),
        gate_rows(log_forget, seq_count, heads_here),
    )
    cell = cell * lax.rsqrt(jnp.mean(cell * cell, axis=-1, keepdims=True) + EPSILON)
    gain_rows = lax.dynamic_slice_in_dim(
        head_gain, group_index * heads_here * HEAD_DIM, heads_here * HEAD_DIM, 0
    ).reshape(1, heads_here, 1, HEAD_DIM)
    scaled = cell.reshape(seq_count, heads_here, tokens, HEAD_DIM) * gain_rows
    mem_out = (
        scaled.transpose(0, 2, 1, 3)
        .reshape(seq_count, tokens, heads_here * HEAD_DIM)
        .astype(jnp.bfloat16)
    )
    conv_seq, mem_seq = (
        lax.all_to_all(conv_out, "fs", split_axis=0, concat_axis=2, tiled=True),
        lax.all_to_all(mem_out, "fs", split_axis=0, concat_axis=2, tiled=True),
    )
    rows_conv, rows_mem = (
        lax.all_gather(w_out_conv, "fs", axis=0, tiled=True),
        lax.all_gather(w_out_mem, "fs", axis=0, tiled=True),
    )
    full_conv, full_mem = (
        lax.all_gather(rows_conv, "sp", axis=1, tiled=True),
        lax.all_gather(rows_mem, "sp", axis=1, tiled=True),
    )
    conv_flat = conv_seq[0]
    mem_flat = mem_seq[0]
    output = lax.psum_scatter(
        (
            jnp.dot(conv_flat, full_conv, preferred_element_type=jnp.float32)
            + jnp.dot(mem_flat, full_mem, preferred_element_type=jnp.float32)
        ).astype(jnp.bfloat16),
        "tp",
        scatter_dimension=0,
        tiled=True,
    ).astype(jnp.float32)
    return output.astype(jnp.bfloat16).reshape(1, output.shape[0], -1)


def solution(mesh):
    return jax.shard_map(
        shards,
        mesh=mesh,
        in_specs=(
            P("fs", "sp", None),
            P(),
            P("sp", ("fs", "tp")),
            P("sp", ("fs", "tp")),
            P("sp", ("fs", "tp")),
            P(),
            P("sp", ("fs", "tp")),
            P("sp", ("fs", "tp")),
            P("sp", ("fs", "tp")),
            P(),
            P(),
            P(),
            P(None, "sp", None),
            P(),
            P(("fs", "tp"), "sp"),
            P(("fs", "tp"), "sp"),
        ),
        out_specs=P("fs", ("sp", "tp"), None),
        check_vma=False,
    )
```

```python
import functools

import jax
import jax.numpy as jnp
from jax import lax
from jax.experimental import pallas as pl
from jax.experimental.pallas import tpu as pltpu
from jax.sharding import PartitionSpec as P

MEMORY_HEADS = 8
HEAD_DIM = 128
BLOCK = 64


EPSILON = 1e-06
FAR_BELOW = -1e30
HIGHEST_PRECISION = lax.Precision.HIGHEST


def prefix(value, axis, join, neutral):
    count, mine = (lax.axis_size(axis), lax.axis_index(axis))
    total, peak, state = value
    stats = jnp.stack([total, peak], axis=1)[..., None]
    stats = jnp.broadcast_to(stats, stats.shape[:2] + state.shape[-1:])
    packed = lax.all_gather(jnp.concatenate([state, stats], axis=1), axis)
    height = state.shape[1]
    pieces = (packed[:, :, height, 0], packed[:, :, height + 1, 0], packed[:, :, :height])
    subtotal = jax.tree.map(
        lambda part, zero: jnp.full_like(part, 0) + jnp.asarray(zero, part.dtype), value, neutral
    )

    def lap(position, subtotal):
        longer = join(subtotal, jax.tree.map(lambda part: part[position], pieces))
        return jax.tree.map(lambda new, old: jnp.where(position < mine, new, old), longer, subtotal)

    return lax.fori_loop(0, count - 1, lap, subtotal)


def from_behind(array, axis, by):
    peers = lax.axis_size(axis)
    pairs = [(i, i + by) for i in range(peers) if 0 <= i + by < peers]
    return lax.ppermute(array, axis, pairs)


def combine_states(earlier, later):
    total_one, peak_one, state_one = earlier
    total_two, peak_two, state_two = later
    peak_new = jnp.maximum(total_two + peak_one, peak_two)
    scale_old = jnp.exp(total_two + peak_one - peak_new)
    scale_new = jnp.exp(peak_two - peak_new)
    return (
        total_one + total_two,
        peak_new,
        scale_old[..., None, None] * state_one + scale_new[..., None, None] * state_two,
    )


def head_rows(values, seq_count, heads_here):
    tokens = values.shape[1]
    split_heads = values.reshape(seq_count, tokens, heads_here, HEAD_DIM).transpose(0, 2, 1, 3)
    return split_heads.reshape(seq_count * heads_here, tokens, HEAD_DIM).astype(jnp.float32)


def gate_rows(values, seq_count, heads_here):
    tokens = values.shape[1]
    return values.transpose(0, 2, 1).reshape(seq_count * heads_here, tokens)


def memory_cell(query_rows, key_rows, value_rows, entry_gate, log_forget):
    members = query_rows.shape[0]
    tokens = query_rows.shape[1]
    head_width = query_rows.shape[2]
    nblocks = tokens // BLOCK
    block_shape = (members, nblocks, BLOCK, head_width)
    query_blocks = query_rows.reshape(block_shape)
    key_blocks = key_rows.reshape(block_shape) * head_width ** (-0.5)
    value_blocks = value_rows.reshape(block_shape)
    entry_blocks = entry_gate.reshape(members, nblocks, BLOCK)
    forget_sums = jnp.cumsum(log_forget.reshape(members, nblocks, BLOCK), axis=-1)
    block_total = forget_sums[..., -1]
    local_logs = block_total[..., None] - forget_sums + entry_blocks
    local_peak = jnp.max(local_logs, axis=-1)
    local_weights = jnp.exp(local_logs - local_peak[..., None])
    local_state = jnp.einsum(
        "bclv,bclk->bcvk",
        local_weights[..., None] * value_blocks,
        key_blocks,
        precision=HIGHEST_PRECISION,
    )

    def advance(running, block_item):
        return (combine_states(running, block_item), running)

    zero_sums = jnp.zeros((members,), jnp.float32)
    low_peaks = jnp.full((members,), FAR_BELOW, jnp.float32)
    zero_states = jnp.zeros((members, head_width, head_width), jnp.float32)
    block_items = (
        jnp.moveaxis(block_total, 1, 0),
        jnp.moveaxis(local_peak, 1, 0),
        jnp.moveaxis(local_state, 1, 0),
    )
    device_total, inner_states = lax.scan(advance, (zero_sums, low_peaks, zero_states), block_items)
    inner_states = tuple((jnp.moveaxis(tensor, 0, 1) for tensor in inner_states))
    total_sum, total_peak, total_state = device_total
    before = prefix(
        (total_sum, total_peak, total_state),
        "sp",
        combine_states,
        (zero_sums, low_peaks, zero_states),
    )
    opening = combine_states((zero_sums, zero_sums, zero_states), before)
    opening = tuple((tensor[:, None] for tensor in opening))
    _, prior_peak, prior_state = combine_states(opening, inner_states)
    positions = jnp.arange(BLOCK)
    causal_mask = positions[:, None] >= positions[None, :]
    pair_logs = jnp.where(
        causal_mask,
        forget_sums[..., :, None] - forget_sums[..., None, :] + entry_blocks[..., None, :],
        -jnp.inf,
    )
    carried_logs = forget_sums + prior_peak[..., None]
    row_peak = jnp.maximum(carried_logs, jnp.max(pair_logs, axis=-1))
    inner_weights = jnp.exp(pair_logs - row_peak[..., None])
    carried_weights = jnp.exp(carried_logs - row_peak)
    scores = inner_weights * jnp.einsum(
        "bcld,bcsd->bcls", query_blocks, key_blocks, precision=HIGHEST_PRECISION
    )
    numerator = carried_weights[..., None] * jnp.einsum(
        "bcvk,bclk->bclv", prior_state, query_blocks, precision=HIGHEST_PRECISION
    ) + jnp.einsum("bcls,bcsv->bclv", scores, value_blocks, precision=HIGHEST_PRECISION)
    return numerator.reshape(members, tokens, head_width)


MESH = pl.DeviceIdType.MESH
F32 = jnp.float32
BF16 = jnp.bfloat16
TAPS = 3
RIM = 8
KV, QUERY, OUT, MIX, GATE = range(5)
SPANS = {KV: (0, 2), QUERY: (2, 1), MIX: (3, 2), GATE: (5, 1)}
PARTS = 5


def layer_kernel(
    ns,
    nf,
    act_ref,
    gain_ref,
    w0_ref,
    w1_ref,
    w2_ref,
    w3_ref,
    w4_ref,
    w5_ref,
    wi_ref,
    wf_ref,
    bias_ref,
    decay_ref,
    taps_ref,
    head_ref,
    wc_ref,
    wm_ref,
    out_ref,
    raw,
    gain,
    normed,
    wbuf,
    wi,
    wf,
    bias,
    decay,
    taps,
    head,
    wo,
    kv,
    query,
    logs,
    logs_t,
    local_stat,
    passed,
    states,
    stats,
    carry,
    carry_m,
    padded,
    gated,
    mine,
    got,
    guest,
    guest_padded,
    guest_mine,
    acc,
    other,
    load_sem,
    x_send,
    x_recv,
    d_send,
    d_recv,
    w_send,
    w_recv,
    p_send,
    p_recv,
    s_send,
    s_recv,
    r_send,
    r_recv,
    m_send,
    m_recv,
    e_send,
    e_recv,
    t_send,
    t_recv,
    u_send,
    u_recv,
    v_send,
    v_recv,
    c_send,
    c_recv,
):
    sp, fs, tp = (lax.axis_index("sp"), lax.axis_index("fs"), lax.axis_index("tp"))
    g = fs * 2 + tp
    depth, cols = w0_ref.shape
    half, model = raw.shape
    tokens = 2 * half
    ocols = wc_ref.shape[1]
    partner = (sp, fs, 1 - tp)
    has_up, has_down = (sp + 1 < ns, sp > 0)
    up, down = ((sp + 1, fs, tp), (sp - 1, fs, tp))
    fy, fx = (fs // 2, lax.rem(fs, 2))
    beside = (fy * 2 + 1 - fx, (1 - fy) * 2 + fx, (1 - fy) * 2 + 1 - fx)

    pair = sp + 1 - 2 * lax.rem(sp, 2)
    hosts = has_up & has_down
    guests = jnp.logical_not(hosts)
    around = (fs,) + beside

    def block(index, size):
        return pl.ds(pl.multiple_of(index * size, size), size)

    def remote(src, dst, send, recv, to):
        return pltpu.make_async_remote_copy(
            src, dst, send, recv, device_id=to, device_id_type=MESH
        )

    loads = [pltpu.make_async_copy(act_ref.at[block(tp, half)], raw, load_sem.at[0])]
    loads.append(pltpu.make_async_copy(gain_ref, gain, load_sem.at[1]))
    for j, ref in enumerate((w0_ref, w1_ref, w2_ref, w3_ref, w4_ref, w5_ref)):
        loads.append(
            pltpu.make_async_copy(
                ref, wbuf.at[block(sp, depth), pl.ds(j * cols, cols)], load_sem.at[2 + j]
            )
        )
    for m, ref in enumerate((wc_ref, wm_ref)):
        loads.append(
            pltpu.make_async_copy(
                ref, wo.at[m, block(fs, cols), block(sp, ocols)], load_sem.at[8 + m]
            )
        )
    smalls = (
        (wi_ref, wi),
        (wf_ref, wf),
        (bias_ref, bias),
        (decay_ref, decay),
        (taps_ref, taps),
        (head_ref, head),
    )
    for j, (ref, held) in enumerate(smalls):
        loads.append(pltpu.make_async_copy(ref, held, load_sem.at[10 + j]))
    for j in (2, 3, 0, 1, 4, 8, 9, 5, 6, 7, 10, 11, 12, 13, 14, 15):
        loads[j].start()

    barrier = pltpu.get_barrier_semaphore()
    for peer in beside:
        pl.semaphore_signal(barrier, inc=1, device_id=(sp, peer, tp), device_id_type=MESH)
        pl.semaphore_signal(barrier, inc=1, device_id=(pair, peer, tp), device_id_type=MESH)
    for off in range(1, ns):
        there = (lax.rem(sp + off, ns), fs, tp)
        pl.semaphore_signal(barrier, inc=1, device_id=there, device_id_type=MESH)
    pl.semaphore_signal(barrier, inc=1, device_id=partner, device_id_type=MESH)

    def place(part, owner):
        if part == OUT:
            return wo.at[:, block(fs, cols), block(owner, ocols)]
        first, count = SPANS[part]
        return wbuf.at[block(owner, depth), pl.ds(first * cols, count * cols)]

    def z_copy(part, side, d, owner):
        there = place(part, owner)
        return remote(
            there,
            there,
            w_send.at[side, d, part],
            w_recv.at[side, d, part],
            (up, down)[side],
        )

    def owner_of(side, d):
        return sp - d if side == 0 else sp + d

    def arrives(part, side, d):
        there = (sp - d >= 0) if side == 0 else (sp + d < ns)
        return there & hosts if part in (MIX, GATE) else there

    def sends(part, side, d):
        there = (sp - d >= 0) if side == 0 else (sp + d < ns)
        if part in (MIX, GATE):
            return there & ((sp + 2 < ns) if side == 0 else (sp > 1))
        return there & (has_up if side == 0 else has_down)

    def z_send(part, side, d):
        @pl.when(sends(part, side, d))
        def _():
            z_copy(part, side, d, owner_of(side, d)).start()

    def own(part):
        for side in range(2):
            z_send(part, side, 0)

    def p_copy(owner, way, row):
        there = wo.at[:, block(row, cols), block(owner, ocols)]
        return remote(
            there,
            there,
            p_send.at[owner, way],
            p_recv.at[owner, way],
            (sp, beside[(0, 1, 0)[way]], tp),
        )

    def spread(owner):
        for way in range(2):
            p_copy(owner, way, fs).start()

    def pass_on(owner):
        p_copy(owner, 1, beside[1]).wait_recv()
        p_copy(owner, 2, beside[1]).start()

    def pass_step(d):
        for side in range(2):

            @pl.when(arrives(OUT, side, d))
            def _():
                pass_on(owner_of(side, d))

    def z_step(part, d):
        for side in range(2):

            @pl.when(arrives(part, side, d))
            def _():
                owner = owner_of(side, d)
                z_copy(part, side, d - 1, owner).wait_recv()
                if d < ns - 1:
                    z_send(part, side, d)
                if part == OUT:
                    spread(owner)

    def x_copy(way, seq):
        first, rows = ((0, half), (0, half), (0, half // 2), (half // 2, half // 2))[way]
        there = normed.at[pl.ds(pl.multiple_of(seq * tokens + tp * half + first, rows), rows)]
        return remote(
            there, there, x_send.at[way], x_recv.at[way], (sp, beside[(0, 1, 1, 0)[way]], tp)
        )

    def d_copy(k, seq, part):
        there = normed.at[pl.ds(pl.multiple_of(seq * tokens + part * half, half), half)]
        return remote(there, there, d_send.at[k], d_recv.at[k], partner)

    def guest_rows(ref, seq, part):
        return ref.at[pl.ds(pl.multiple_of(seq * tokens + part * half, half), half)]

    def t_copy(j):
        return remote(
            guest_rows(normed, around[j], tp),
            guest_rows(guest, around[j], tp),
            t_send.at[j],
            t_recv.at[j],
            (pair, fs, tp),
        )

    def u_copy(j, seq):
        there = guest_rows(guest, seq, tp)
        return remote(there, there, u_send.at[j], u_recv.at[j], (sp, beside[1], tp))

    def v_copy(k, part):
        there = guest_rows(guest, around[k], part)
        return remote(there, there, v_send.at[k], v_recv.at[k], partner)

    def guest_from_pair(j):
        @pl.when(hosts)
        def _():
            t_copy(j).wait_recv()
            u_copy(j, around[j]).start()
            v_copy(j, tp).start()

    def guest_from_beside(j):
        @pl.when(hosts)
        def _():
            u_copy(j, around[2 + j]).wait_recv()
            v_copy(2 + j, tp).start()

    def guest_to_pair(j):
        @pl.when(guests)
        def _():
            t_copy(j).start()

    def activations_in(way):
        x_copy(way, beside[way]).wait_recv()
        x_copy(way + 2, beside[way]).start()
        d_copy(way + 1, beside[way], tp).start()

    def tile(i):
        return pl.ds(pl.multiple_of(i * tokens, tokens), tokens)

    def project(part, into):
        first, count = SPANS[part]

        def body(i, carried):
            into[tile(i), :] = jnp.dot(
                normed[tile(i), :],
                wbuf[:, first * cols : (first + count) * cols],
                preferred_element_type=F32,
            ).astype(BF16)
            return carried

        lax.fori_loop(0, nf, body, 0)

    def mix_copy(m, k, seq, source):
        return remote(
            mine.at[m, seq],
            got.at[m, :, block(source, cols)],
            m_send.at[m, k],
            m_recv.at[m, k],
            (sp, beside[k], tp),
        )

    def hand_out(m):
        for k in (2, 0, 1):
            mix_copy(m, k, beside[k], fs).start()
        got[m, :, block(fs, cols)] = mine[m, fs]

    def state_copies(off, source):
        to = (lax.rem(sp + off, ns), fs, tp)
        return (
            remote(
                local_stat, stats.at[source], s_send.at[0, off - 1], s_recv.at[0, off - 1], to
            ),
            remote(passed, states.at[source], s_send.at[1, off - 1], s_recv.at[1, off - 1], to),
        )

    def states_out():
        for off in range(ns - 1, 0, -1):

            @pl.when(sp + off < ns)
            def _():
                for copy in state_copies(off, sp):
                    copy.start()

    def states_in():
        for off in range(1, ns):

            @pl.when(sp - off >= 0)
            def _():
                for copy in state_copies(off, sp - off):
                    copy.wait_recv()

        carry[...] = jnp.zeros_like(carry)
        carry_m[...] = jnp.zeros_like(carry_m)
        for source in range(ns - 1):

            @pl.when(source < sp)
            def _():
                for s in range(nf):
                    before = stats[source, s : s + 1, :] + carry_m[s : s + 1, :]
                    peak = stats[source, nf + s : nf + s + 1, :]
                    top = jnp.maximum(before, peak)
                    carry[s] = jnp.exp(before - top) * carry[s] + jnp.exp(peak - top) * states[
                        source, s
                    ].astype(F32)
                    carry_m[s : s + 1, :] = top

    def rim_copy():
        return remote(
            padded.at[:, pl.ds(tokens, RIM), :],
            padded.at[:, pl.ds(0, RIM), :],
            r_send,
            r_recv,
            up,
        )

    inner = hosts & (sp + 2 < ns)
    outer = hosts & (sp > 1)

    def products(source, seq, held):
        three = jnp.dot(
            source[tile(seq), :],
            wbuf[:, SPANS[MIX][0] * cols :],
            preferred_element_type=F32,
        ).astype(BF16)
        both = three[:, : 2 * cols].astype(F32)
        held[seq, RIM:, :] = (both[:, :cols] * both[:, cols:]).astype(BF16).astype(F32)
        return three[:, 2 * cols :]

    def convolve(held, seq, gate):
        tap = taps[:, block(g, cols)]
        total = jnp.zeros((tokens, cols), F32)
        for j in range(TAPS):
            at = RIM - (TAPS - 1) + j
            total = total + tap[j : j + 1, :] * held[seq, at : at + tokens, :]
        return (gate.astype(F32) * total).astype(BF16)

    def c_copy(k, seq, source):
        return remote(
            guest_mine.at[seq],
            got.at[0, :, block(source, cols)],
            c_send.at[k],
            c_recv.at[k],
            (pair, around[k], tp),
        )

    def own_products():
        @pl.when(hosts)
        def _():
            def body(i, carried):
                gated[tile(i), :] = products(normed, i, padded)
                return carried

            lax.fori_loop(0, nf, body, 0)

        @pl.when(inner)
        def _():
            rim_copy().start()

    def guest_part(k):
        seq = around[k]
        v_copy(k, 1 - tp).wait_recv()
        gate = products(guest, seq, guest_padded)
        guest_padded[seq, 0:RIM, :] = jnp.where(inner, 0.0, padded[seq, tokens : tokens + RIM, :])
        guest_mine[seq] = convolve(guest_padded, seq, gate)

    def own_part(seq):
        @pl.when(inner)
        def _():
            padded[seq, 0:RIM, :] = guest_padded[seq, tokens : tokens + RIM, :]

        return convolve(padded, seq, gated[tile(seq), :])

    loads[2].wait()
    loads[3].wait()
    pl.semaphore_wait(barrier, 2 * (nf - 1) + ns)
    own(KV)
    loads[8].wait()
    loads[9].wait()
    own(OUT)
    spread(sp)
    loads[0].wait()
    loads[1].wait()
    step = 32

    def norm_rows(i, carried):
        x = raw[pl.ds(pl.multiple_of(i * step, step), step), :].astype(F32)
        scale = lax.rsqrt(jnp.mean(x * x, axis=-1, keepdims=True) + EPSILON)
        rows = pl.ds(pl.multiple_of(fs * tokens + tp * half + i * step, step), step)
        normed[rows, :] = (x * scale * gain[...]).astype(BF16)
        return carried

    lax.fori_loop(0, half // step, norm_rows, 0)
    loads[4].wait()
    own(QUERY)
    for j in (5, 6, 7):
        loads[j].wait()
    own(GATE)
    for way in range(2):
        x_copy(way, fs).start()
    d_copy(0, fs, tp).start()
    z_step(OUT, 1)
    z_step(KV, 1)
    guest_to_pair(0)
    for way in range(2):
        activations_in(way)
    pass_on(sp)
    z_step(QUERY, 1)
    z_step(OUT, 2)
    own(MIX)
    z_step(KV, 2)
    z_step(QUERY, 2)
    guest_to_pair(1)
    pass_step(1)
    z_step(MIX, 1)
    for way in range(2, 4):
        x_copy(way, beside[2]).wait_recv()
    d_copy(3, beside[2], tp).start()
    z_step(OUT, 3)
    z_step(KV, 3)
    z_step(GATE, 1)
    guest_from_pair(0)
    for j in range(10, 16):
        loads[j].wait()
    for k, seq in enumerate(around):
        d_copy(k, seq, 1 - tp).wait_recv()

    row_at = lax.broadcasted_iota(jnp.int32, (tokens, tokens), 0)
    col_at = lax.broadcasted_iota(jnp.int32, (tokens, tokens), 1)
    gates = jnp.concatenate([wi[...].astype(F32), wf[...].astype(F32)], axis=0).astype(BF16)
    heads = wi.shape[0]
    own_gate = lax.broadcasted_iota(jnp.int32, (2 * heads, tokens), 0)
    own_bias = lax.broadcasted_iota(jnp.int32, (1, heads), 1)
    bias_in = jnp.sum(jnp.where(own_bias == g, bias[0:1, :], 0.0), axis=1, keepdims=True)
    bias_out = jnp.sum(jnp.where(own_bias == g, bias[1:2, :], 0.0), axis=1, keepdims=True)
    line = lax.broadcasted_iota(jnp.int32, (128, tokens), 0)
    packed = jnp.zeros((128, tokens), F32)
    for s in range(nf):
        raw_gates = lax.dot_general(
            gates,
            normed[s * tokens : (s + 1) * tokens, :],
            (((1,), (1,)), ((), ())),
            preferred_element_type=F32,
        )
        entry = jnp.sum(jnp.where(own_gate == g, raw_gates, 0.0), axis=0, keepdims=True) + bias_in
        forget = (
            jnp.sum(jnp.where(own_gate == heads + g, raw_gates, 0.0), axis=0, keepdims=True)
            + bias_out
        )
        shift = jnp.sum(jnp.where(own_gate[:heads] == g, decay[s], 0.0), axis=0, keepdims=True)
        forget = jnp.minimum(forget, 0.0) - jnp.log1p(jnp.exp(-jnp.abs(forget))) + shift
        packed = jnp.where(line == s, forget, packed)
        packed = jnp.where(line == nf + s, entry, packed)
    ones = jnp.where(row_at <= col_at, 1.0, 0.0).astype(F32)
    sums = jnp.dot(packed, ones, precision=HIGHEST_PRECISION, preferred_element_type=F32)
    sums = jnp.where(line < nf, sums, packed)
    logs_t[...] = sums
    logs[...] = sums.T
    project(KV, kv)
    for s in range(nf):
        rows = pl.ds(s * tokens, tokens)
        total = logs_t[s : s + 1, tokens - 1 : tokens]
        reach = total - logs[:, s : s + 1] + logs[:, nf + s : nf + s + 1]
        peak = jnp.max(reach, axis=0, keepdims=True)
        weighted = (kv[rows, cols:].astype(F32) * jnp.exp(reach - peak)).astype(BF16)
        passed[s] = lax.dot_general(
            kv[rows, :cols], weighted, (((0,), (0,)), ((), ())), preferred_element_type=F32
        ).astype(BF16)
        local_stat[s : s + 1, :] = jnp.broadcast_to(total, (1, 128))
        local_stat[nf + s : nf + s + 1, :] = jnp.broadcast_to(peak, (1, 128))

    z_step(QUERY, 3)
    z_step(GATE, 2)
    states_out()
    pass_step(2)
    guest_from_pair(1)
    pass_step(3)
    guest_from_beside(0)
    z_step(MIX, 2)
    own_products()

    @pl.when(hosts)
    def _():
        for k in range(nf - 1):
            guest_part(k)
            if k > 0:
                c_copy(k - 1, around[k - 1], fs).start()

    states_in()
    project(QUERY, query)

    scale = HEAD_DIM ** (-0.5)
    head_gain = head[:, block(g, cols)]
    causal = row_at >= col_at
    for s in range(nf):
        rows = pl.ds(s * tokens, tokens)
        scores = lax.dot_general(
            query[rows, :], kv[rows, :cols], (((1,), (1,)), ((), ())), preferred_element_type=F32
        )
        sums = logs[:, s : s + 1]
        pairs = jnp.where(
            causal,
            sums - logs_t[s : s + 1, :] + logs_t[nf + s : nf + s + 1, :],
            FAR_BELOW,
        )
        carried = sums + carry_m[s : s + 1, 0:1]
        top = jnp.maximum(carried, jnp.max(pairs, axis=1, keepdims=True))
        weights = (jnp.exp(pairs - top) * scores).astype(BF16)
        cell = jnp.dot(weights, kv[rows, cols:], preferred_element_type=F32)
        cell = cell + jnp.exp(carried - top) * jnp.dot(
            query[rows, :], carry[s].astype(BF16), preferred_element_type=F32
        )
        cell = cell * scale
        cell = cell * lax.rsqrt(jnp.mean(cell * cell, axis=-1, keepdims=True) + EPSILON)
        mine[1, s] = (cell * head_gain).astype(BF16)

    hand_out(1)

    @pl.when(outer)
    def _():
        rim_copy().wait_recv()

    @pl.when(hosts)
    def _():
        c_copy(nf - 2, around[nf - 2], fs).start()
        mine[0, beside[0]] = own_part(beside[0])
        mine[0, beside[1]] = own_part(beside[1])
        mix_copy(0, 0, beside[0], fs).start()
        got[0, :, block(fs, cols)] = own_part(fs)
        mix_copy(0, 1, beside[1], fs).start()

    guest_from_beside(1)

    @pl.when(hosts)
    def _():
        guest_part(nf - 1)
        mine[0, beside[2]] = own_part(beside[2])
        c_copy(nf - 1, around[nf - 1], fs).start()
        mix_copy(0, 2, beside[2], fs).start()

    def arrived(owner, carried):
        p_copy(owner, 0, beside[0]).wait_recv()
        p_copy(owner, 2, beside[2]).wait_recv()
        return carried

    lax.fori_loop(0, ns, arrived, 0)
    for k in range(nf - 1):
        mix_copy(1, k, beside[k], beside[k]).wait_recv()

    def memory_share(i, carried):
        acc[:, block(i, ocols)] = jnp.dot(
            got[1], wo[1, :, block(i, ocols)], preferred_element_type=F32
        )
        return carried

    lax.fori_loop(0, ns, memory_share, 0)

    def e_copy(i):
        return remote(
            acc.at[block(1 - tp, half), block(i, ocols)],
            other.at[:, block(i, ocols)],
            e_send.at[i],
            e_recv.at[i],
            partner,
        )

    def add_pair(i, pair):
        acc[:, block(i, ocols)] = acc[:, block(i, ocols)] + jnp.dot(
            got[0, :, block(pair, 2 * cols)],
            wo[0, block(pair, 2 * cols), block(i, ocols)],
            preferred_element_type=F32,
        )

    @pl.when(hosts)
    def _():
        mix_copy(0, 0, beside[0], beside[0]).wait_recv()

    @pl.when(guests)
    def _():
        for k in range(2):
            c_copy(k, around[k], around[k]).wait_recv()

    for i in range(ns):
        add_pair(i, fy)

    @pl.when(hosts)
    def _():
        for k in (1, 2):
            mix_copy(0, k, beside[k], beside[k]).wait_recv()

    @pl.when(guests)
    def _():
        for k in range(2, nf):
            c_copy(k, around[k], around[k]).wait_recv()

    for i in range(ns):
        add_pair(i, 1 - fy)
        if i > 0:
            e_copy(i - 1).start()
    e_copy(ns - 1).start()

    def merge(i, carried):
        e_copy(i).wait_recv()
        out_ref[:, block(i, ocols)] = (
            acc[block(tp, half), block(i, ocols)] + other[:, block(i, ocols)]
        ).astype(BF16)
        return carried

    lax.fori_loop(0, ns, merge, 0)

    def sent(i, carried):
        e_copy(i).wait_send()
        for way in range(3):
            p_copy(i, way, (fs, fs, beside[1])[way]).wait_send()
        return carried

    lax.fori_loop(0, ns, sent, 0)
    for way in range(4):
        x_copy(way, (fs, fs, beside[0], beside[1])[way]).wait_send()
    for k, seq in enumerate(around):
        d_copy(k, seq, tp).wait_send()
    for k in range(nf - 1):
        mix_copy(1, k, beside[k], fs).wait_send()

    @pl.when(hosts)
    def _():
        for k in range(nf - 1):
            mix_copy(0, k, beside[k], fs).wait_send()
        for k in range(nf):
            v_copy(k, tp).wait_send()
            c_copy(k, around[k], fs).wait_send()
        for j in range(2):
            u_copy(j, around[j]).wait_send()

    @pl.when(guests)
    def _():
        for j in range(2):
            t_copy(j).wait_send()

    @pl.when(inner)
    def _():
        rim_copy().wait_send()

    for side in range(2):
        for d in range(ns - 1):
            for parts in ((KV, QUERY, OUT), (MIX, GATE)):

                @pl.when(sends(parts[0], side, d))
                def _():
                    for part in parts:
                        z_copy(part, side, d, owner_of(side, d)).wait_send()

    for off in range(1, ns):

        @pl.when(sp + off < ns)
        def _():
            for copy in state_copies(off, sp):
                copy.wait_send()


def whole_layer(act, gain, weights, wi, wf, bias, decay, taps, head, w_out_conv, w_out_mem):
    ns, nf = (lax.axis_size("sp"), lax.axis_size("fs"))
    tokens, model = act.shape
    half = tokens // 2
    depth, cols = weights[0].shape
    ocols = w_out_conv.shape[1]
    count = nf * tokens
    anywhere = pl.BlockSpec(memory_space=pl.ANY)
    dma = pltpu.SemaphoreType.DMA
    vmem = pltpu.VMEM
    return pl.pallas_call(
        functools.partial(layer_kernel, ns, nf),
        out_shape=pltpu.VMEM((half, ns * ocols), BF16),
        in_specs=[anywhere] * 16,
        out_specs=pl.BlockSpec(memory_space=pltpu.VMEM),
        scratch_shapes=[
            vmem((half, model), BF16),
            vmem(gain.shape, F32),
            vmem((count, model), BF16),
            vmem((ns * depth, 6 * cols), BF16),
            vmem(wi.shape, BF16),
            vmem(wf.shape, BF16),
            vmem(bias.shape, F32),
            vmem(decay.shape, F32),
            vmem(taps.shape, F32),
            vmem(head.shape, F32),
            vmem((2, nf * cols, ns * ocols), BF16),
            vmem((count, 2 * cols), BF16),
            vmem((count, cols), BF16),
            vmem((tokens, 128), F32),
            vmem((128, tokens), F32),
            vmem((2 * nf, 128), F32),
            vmem((nf, cols, cols), BF16),
            vmem((ns - 1, nf, cols, cols), BF16),
            vmem((ns - 1, 2 * nf, 128), F32),
            vmem((nf, cols, cols), F32),
            vmem((nf, 128), F32),
            vmem((nf, RIM + tokens, cols), F32),
            vmem((count, cols), BF16),
            vmem((2, nf, tokens, cols), BF16),
            vmem((2, tokens, nf * cols), BF16),
            vmem((count, model), BF16),
            vmem((nf, RIM + tokens, cols), F32),
            vmem((nf, tokens, cols), BF16),
            vmem((tokens, ns * ocols), F32),
            vmem((half, ns * ocols), F32),
            dma((16,)),
            dma((4,)),
            dma((4,)),
            dma((nf,)),
            dma((nf,)),
            dma((2, ns - 1, PARTS)),
            dma((2, ns - 1, PARTS)),
            dma((ns, 3)),
            dma((ns, 3)),
            dma((2, ns - 1)),
            dma((2, ns - 1)),
            dma,
            dma,
            dma((2, nf - 1)),
            dma((2, nf - 1)),
            dma((ns,)),
            dma((ns,)),
            dma((2,)),
            dma((2,)),
            dma((2,)),
            dma((2,)),
            dma((nf,)),
            dma((nf,)),
            dma((nf,)),
            dma((nf,)),
        ],
        compiler_params=pltpu.CompilerParams(
            collective_id=0, has_side_effects=True, vmem_limit_bytes=54 * 1024 * 1024
        ),
    )(act, gain, *weights, wi, wf, bias, decay, taps, head, w_out_conv, w_out_mem)


def shards(
    activations,
    norm_gain,
    w_conv_gate,
    w_conv_mult,
    w_conv_in,
    conv_taps,
    w_query,
    w_key,
    w_value,
    w_input_gate,
    w_forget_gate,
    gate_bias,
    decay_shift,
    head_gain,
    w_out_conv,
    w_out_mem,
):
    group_index = lax.axis_index(("fs", "tp"))
    heads_here = MEMORY_HEADS // (lax.axis_size("fs") * lax.axis_size("tp"))
    channels = w_conv_gate.shape[1]
    ns, nf, nt = (lax.axis_size("sp"), lax.axis_size("fs"), lax.axis_size("tp"))
    if ns == 4 and nf == 4 and nt == 2 and heads_here == 1 and channels == HEAD_DIM:
        return whole_layer(
            activations[0],
            norm_gain[None, :],
            (w_key, w_value, w_query, w_conv_mult, w_conv_in, w_conv_gate),
            w_input_gate.T,
            w_forget_gate.T,
            gate_bias,
            decay_shift.transpose(0, 2, 1),
            conv_taps,
            head_gain[None, :],
            w_out_conv,
            w_out_mem,
        )[None]
    sequences = lax.all_gather(activations, "fs", axis=0, tiled=True)
    seq_count = sequences.shape[0]
    tokens = sequences.shape[1]
    model_width = sequences.shape[2]
    row_count = seq_count * tokens
    flat_rows = sequences.reshape(row_count, model_width).astype(jnp.float32)
    normed = (
        flat_rows
        * lax.rsqrt(jnp.mean(flat_rows * flat_rows, axis=-1, keepdims=True) + EPSILON)
        * norm_gain
    ).astype(jnp.bfloat16)
    pieces = (
        lax.all_gather(w_conv_gate, "sp", axis=0, tiled=True),
        lax.all_gather(w_conv_mult, "sp", axis=0, tiled=True),
        lax.all_gather(w_conv_in, "sp", axis=0, tiled=True),
        lax.all_gather(w_query, "sp", axis=0, tiled=True),
        lax.all_gather(w_key, "sp", axis=0, tiled=True),
        lax.all_gather(w_value, "sp", axis=0, tiled=True),
    )
    projected = tuple(
        (jnp.dot(normed, shard_piece, preferred_element_type=jnp.float32) for shard_piece in pieces)
    )
    conv_gate, conv_mult, conv_in, query, keys_proj, value = [
        tensor.astype(jnp.bfloat16).reshape(seq_count, tokens, -1) for tensor in projected
    ]
    entry_cols = lax.dynamic_slice_in_dim(w_input_gate, group_index * heads_here, heads_here, 1)
    forget_cols = lax.dynamic_slice_in_dim(w_forget_gate, group_index * heads_here, heads_here, 1)
    gate_values = jnp.dot(
        normed,
        jnp.concatenate([entry_cols, forget_cols], axis=1),
        preferred_element_type=jnp.float32,
    ).reshape(seq_count, tokens, 2 * heads_here)
    product = (conv_mult.astype(jnp.float32) * conv_in.astype(jnp.float32)).astype(jnp.bfloat16)
    ntaps = conv_taps.shape[0]
    rim_rows = from_behind(product[:, tokens - (ntaps - 1) :, :], "sp", 1)
    padded = jnp.concatenate([rim_rows, product], axis=1).astype(jnp.float32)
    tap_weights = lax.dynamic_slice_in_dim(conv_taps, group_index * channels, channels, 1)
    mixed_sum = jnp.zeros((seq_count, tokens, channels), jnp.float32)
    for tap_index in range(ntaps):
        mixed_sum = (
            mixed_sum + tap_weights[tap_index] * padded[:, tap_index : tap_index + tokens, :]
        )
    conv_out = (conv_gate.astype(jnp.float32) * mixed_sum).astype(jnp.bfloat16)
    bias_rows = lax.dynamic_slice_in_dim(gate_bias, group_index * heads_here, heads_here, 1)
    decay_rows = lax.dynamic_slice_in_dim(decay_shift, group_index * heads_here, heads_here, 2)
    entry = gate_values[..., :heads_here] + bias_rows[0]
    log_forget = jax.nn.log_sigmoid(gate_values[..., heads_here:] + bias_rows[1]) + decay_rows
    cell = memory_cell(
        head_rows(query, seq_count, heads_here),
        head_rows(keys_proj, seq_count, heads_here),
        head_rows(value, seq_count, heads_here),
        gate_rows(entry, seq_count, heads_here),
        gate_rows(log_forget, seq_count, heads_here),
    )
    cell = cell * lax.rsqrt(jnp.mean(cell * cell, axis=-1, keepdims=True) + EPSILON)
    gain_rows = lax.dynamic_slice_in_dim(
        head_gain, group_index * heads_here * HEAD_DIM, heads_here * HEAD_DIM, 0
    ).reshape(1, heads_here, 1, HEAD_DIM)
    scaled = cell.reshape(seq_count, heads_here, tokens, HEAD_DIM) * gain_rows
    mem_out = (
        scaled.transpose(0, 2, 1, 3)
        .reshape(seq_count, tokens, heads_here * HEAD_DIM)
        .astype(jnp.bfloat16)
    )
    conv_seq, mem_seq = (
        lax.all_to_all(conv_out, "fs", split_axis=0, concat_axis=2, tiled=True),
        lax.all_to_all(mem_out, "fs", split_axis=0, concat_axis=2, tiled=True),
    )
    rows_conv, rows_mem = (
        lax.all_gather(w_out_conv, "fs", axis=0, tiled=True),
        lax.all_gather(w_out_mem, "fs", axis=0, tiled=True),
    )
    full_conv, full_mem = (
        lax.all_gather(rows_conv, "sp", axis=1, tiled=True),
        lax.all_gather(rows_mem, "sp", axis=1, tiled=True),
    )
    conv_flat = conv_seq[0]
    mem_flat = mem_seq[0]
    output = lax.psum_scatter(
        (
            jnp.dot(conv_flat, full_conv, preferred_element_type=jnp.float32)
            + jnp.dot(mem_flat, full_mem, preferred_element_type=jnp.float32)
        ).astype(jnp.bfloat16),
        "tp",
        scatter_dimension=0,
        tiled=True,
    ).astype(jnp.float32)
    return output.astype(jnp.bfloat16).reshape(1, output.shape[0], -1)


def solution(mesh):
    return jax.shard_map(
        shards,
        mesh=mesh,
        in_specs=(
            P("fs", "sp", None),
            P(),
            P("sp", ("fs", "tp")),
            P("sp", ("fs", "tp")),
            P("sp", ("fs", "tp")),
            P(),
            P("sp", ("fs", "tp")),
            P("sp", ("fs", "tp")),
            P("sp", ("fs", "tp")),
            P(),
            P(),
            P(),
            P(None, "sp", None),
            P(),
            P(("fs", "tp"), "sp"),
            P(("fs", "tp"), "sp"),
        ),
        out_specs=P("fs", ("sp", "tp"), None),
        check_vma=False,
    )
```

```python
import functools

import jax
import jax.numpy as jnp
from jax import lax
from jax.experimental import pallas as pl
from jax.experimental.pallas import tpu as pltpu
from jax.sharding import PartitionSpec as P

MEMORY_HEADS = 8
HEAD_DIM = 128
BLOCK = 64


EPSILON = 1e-06
FAR_BELOW = -1e30
HIGHEST_PRECISION = lax.Precision.HIGHEST


def prefix(value, axis, join, neutral):
    count, mine = (lax.axis_size(axis), lax.axis_index(axis))
    total, peak, state = value
    stats = jnp.stack([total, peak], axis=1)[..., None]
    stats = jnp.broadcast_to(stats, stats.shape[:2] + state.shape[-1:])
    packed = lax.all_gather(jnp.concatenate([state, stats], axis=1), axis)
    height = state.shape[1]
    pieces = (packed[:, :, height, 0], packed[:, :, height + 1, 0], packed[:, :, :height])
    subtotal = jax.tree.map(
        lambda part, zero: jnp.full_like(part, 0) + jnp.asarray(zero, part.dtype), value, neutral
    )

    def lap(position, subtotal):
        longer = join(subtotal, jax.tree.map(lambda part: part[position], pieces))
        return jax.tree.map(lambda new, old: jnp.where(position < mine, new, old), longer, subtotal)

    return lax.fori_loop(0, count - 1, lap, subtotal)


def from_behind(array, axis, by):
    peers = lax.axis_size(axis)
    pairs = [(i, i + by) for i in range(peers) if 0 <= i + by < peers]
    return lax.ppermute(array, axis, pairs)


def combine_states(earlier, later):
    total_one, peak_one, state_one = earlier
    total_two, peak_two, state_two = later
    peak_new = jnp.maximum(total_two + peak_one, peak_two)
    scale_old = jnp.exp(total_two + peak_one - peak_new)
    scale_new = jnp.exp(peak_two - peak_new)
    return (
        total_one + total_two,
        peak_new,
        scale_old[..., None, None] * state_one + scale_new[..., None, None] * state_two,
    )


def head_rows(values, seq_count, heads_here):
    tokens = values.shape[1]
    split_heads = values.reshape(seq_count, tokens, heads_here, HEAD_DIM).transpose(0, 2, 1, 3)
    return split_heads.reshape(seq_count * heads_here, tokens, HEAD_DIM).astype(jnp.float32)


def gate_rows(values, seq_count, heads_here):
    tokens = values.shape[1]
    return values.transpose(0, 2, 1).reshape(seq_count * heads_here, tokens)


def memory_cell(query_rows, key_rows, value_rows, entry_gate, log_forget):
    members = query_rows.shape[0]
    tokens = query_rows.shape[1]
    head_width = query_rows.shape[2]
    nblocks = tokens // BLOCK
    block_shape = (members, nblocks, BLOCK, head_width)
    query_blocks = query_rows.reshape(block_shape)
    key_blocks = key_rows.reshape(block_shape) * head_width ** (-0.5)
    value_blocks = value_rows.reshape(block_shape)
    entry_blocks = entry_gate.reshape(members, nblocks, BLOCK)
    forget_sums = jnp.cumsum(log_forget.reshape(members, nblocks, BLOCK), axis=-1)
    block_total = forget_sums[..., -1]
    local_logs = block_total[..., None] - forget_sums + entry_blocks
    local_peak = jnp.max(local_logs, axis=-1)
    local_weights = jnp.exp(local_logs - local_peak[..., None])
    local_state = jnp.einsum(
        "bclv,bclk->bcvk",
        local_weights[..., None] * value_blocks,
        key_blocks,
        precision=HIGHEST_PRECISION,
    )

    def advance(running, block_item):
        return (combine_states(running, block_item), running)

    zero_sums = jnp.zeros((members,), jnp.float32)
    low_peaks = jnp.full((members,), FAR_BELOW, jnp.float32)
    zero_states = jnp.zeros((members, head_width, head_width), jnp.float32)
    block_items = (
        jnp.moveaxis(block_total, 1, 0),
        jnp.moveaxis(local_peak, 1, 0),
        jnp.moveaxis(local_state, 1, 0),
    )
    device_total, inner_states = lax.scan(advance, (zero_sums, low_peaks, zero_states), block_items)
    inner_states = tuple((jnp.moveaxis(tensor, 0, 1) for tensor in inner_states))
    total_sum, total_peak, total_state = device_total
    before = prefix(
        (total_sum, total_peak, total_state),
        "sp",
        combine_states,
        (zero_sums, low_peaks, zero_states),
    )
    opening = combine_states((zero_sums, zero_sums, zero_states), before)
    opening = tuple((tensor[:, None] for tensor in opening))
    _, prior_peak, prior_state = combine_states(opening, inner_states)
    positions = jnp.arange(BLOCK)
    causal_mask = positions[:, None] >= positions[None, :]
    pair_logs = jnp.where(
        causal_mask,
        forget_sums[..., :, None] - forget_sums[..., None, :] + entry_blocks[..., None, :],
        -jnp.inf,
    )
    carried_logs = forget_sums + prior_peak[..., None]
    row_peak = jnp.maximum(carried_logs, jnp.max(pair_logs, axis=-1))
    inner_weights = jnp.exp(pair_logs - row_peak[..., None])
    carried_weights = jnp.exp(carried_logs - row_peak)
    scores = inner_weights * jnp.einsum(
        "bcld,bcsd->bcls", query_blocks, key_blocks, precision=HIGHEST_PRECISION
    )
    numerator = carried_weights[..., None] * jnp.einsum(
        "bcvk,bclk->bclv", prior_state, query_blocks, precision=HIGHEST_PRECISION
    ) + jnp.einsum("bcls,bcsv->bclv", scores, value_blocks, precision=HIGHEST_PRECISION)
    return numerator.reshape(members, tokens, head_width)


MESH = pl.DeviceIdType.MESH
F32 = jnp.float32
BF16 = jnp.bfloat16
TAPS = 3
RIM = 8
KV, QUERY, OUT, MIX, GATE = range(5)
SPANS = {KV: (0, 2), QUERY: (2, 1), MIX: (3, 2), GATE: (5, 1)}
PARTS = 5


def layer_kernel(
    ns,
    nf,
    act_ref,
    gain_ref,
    w0_ref,
    w1_ref,
    w2_ref,
    w3_ref,
    w4_ref,
    w5_ref,
    wi_ref,
    wf_ref,
    bias_ref,
    decay_ref,
    taps_ref,
    head_ref,
    wc_ref,
    wm_ref,
    out_ref,
    raw,
    gain,
    normed,
    wbuf,
    wi,
    wf,
    bias,
    decay,
    taps,
    head,
    wo,
    kv,
    query,
    logs,
    logs_t,
    local_stat,
    passed,
    states,
    stats,
    carry,
    carry_m,
    padded,
    gated,
    mine,
    got,
    guest,
    guest_padded,
    guest_mine,
    acc,
    share,
    other,
    load_sem,
    x_send,
    x_recv,
    d_send,
    d_recv,
    w_send,
    w_recv,
    p_send,
    p_recv,
    s_send,
    s_recv,
    r_send,
    r_recv,
    m_send,
    m_recv,
    e_send,
    e_recv,
    t_send,
    t_recv,
    u_send,
    u_recv,
    v_send,
    v_recv,
    c_send,
    c_recv,
):
    sp, fs, tp = (lax.axis_index("sp"), lax.axis_index("fs"), lax.axis_index("tp"))
    g = fs * 2 + tp
    depth, cols = w0_ref.shape
    half, model = raw.shape
    tokens = 2 * half
    ocols = wc_ref.shape[1]
    partner = (sp, fs, 1 - tp)
    has_up, has_down = (sp + 1 < ns, sp > 0)
    up, down = ((sp + 1, fs, tp), (sp - 1, fs, tp))
    fy, fx = (fs // 2, lax.rem(fs, 2))
    beside = (fy * 2 + 1 - fx, (1 - fy) * 2 + fx, (1 - fy) * 2 + 1 - fx)

    pair = sp + 1 - 2 * lax.rem(sp, 2)
    hosts = has_up & has_down
    guests = jnp.logical_not(hosts)
    around = (fs,) + beside

    def block(index, size):
        return pl.ds(pl.multiple_of(index * size, size), size)

    def remote(src, dst, send, recv, to):
        return pltpu.make_async_remote_copy(
            src, dst, send, recv, device_id=to, device_id_type=MESH
        )

    loads = [pltpu.make_async_copy(act_ref.at[block(tp, half)], raw, load_sem.at[0])]
    loads.append(pltpu.make_async_copy(gain_ref, gain, load_sem.at[1]))
    for j, ref in enumerate((w0_ref, w1_ref, w2_ref, w3_ref, w4_ref, w5_ref)):
        loads.append(
            pltpu.make_async_copy(
                ref, wbuf.at[block(sp, depth), pl.ds(j * cols, cols)], load_sem.at[2 + j]
            )
        )
    for m, ref in enumerate((wc_ref, wm_ref)):
        loads.append(
            pltpu.make_async_copy(
                ref, wo.at[m, block(fs, cols), block(sp, ocols)], load_sem.at[8 + m]
            )
        )
    smalls = (
        (wi_ref, wi),
        (wf_ref, wf),
        (bias_ref, bias),
        (decay_ref, decay),
        (taps_ref, taps),
        (head_ref, head),
    )
    for j, (ref, held) in enumerate(smalls):
        loads.append(pltpu.make_async_copy(ref, held, load_sem.at[10 + j]))
    for j in (2, 3, 0, 1, 4, 8, 9, 5, 6, 7, 10, 11, 12, 13, 14, 15):
        loads[j].start()

    barrier = pltpu.get_barrier_semaphore()
    for peer in beside:
        pl.semaphore_signal(barrier, inc=1, device_id=(sp, peer, tp), device_id_type=MESH)
        pl.semaphore_signal(barrier, inc=1, device_id=(pair, peer, tp), device_id_type=MESH)
    pl.semaphore_signal(barrier, inc=1, device_id=partner, device_id_type=MESH)

    @pl.when(has_up)
    def _():
        pl.semaphore_signal(barrier, inc=1, device_id=up, device_id_type=MESH)

    @pl.when(has_down)
    def _():
        pl.semaphore_signal(barrier, inc=1, device_id=down, device_id_type=MESH)

    def place(part, owner):
        if part == OUT:
            return wo.at[:, block(fs, cols), block(owner, ocols)]
        first, count = SPANS[part]
        return wbuf.at[block(owner, depth), pl.ds(first * cols, count * cols)]

    def z_copy(part, side, d, owner):
        there = place(part, owner)
        return remote(
            there,
            there,
            w_send.at[side, d, part],
            w_recv.at[side, d, part],
            (up, down)[side],
        )

    def owner_of(side, d):
        return sp - d if side == 0 else sp + d

    def arrives(part, side, d):
        there = (sp - d >= 0) if side == 0 else (sp + d < ns)
        return there & hosts if part in (MIX, GATE) else there

    def sends(part, side, d):
        there = (sp - d >= 0) if side == 0 else (sp + d < ns)
        if part in (MIX, GATE):
            return there & ((sp + 2 < ns) if side == 0 else (sp > 1))
        return there & (has_up if side == 0 else has_down)

    def z_send(part, side, d):
        @pl.when(sends(part, side, d))
        def _():
            z_copy(part, side, d, owner_of(side, d)).start()

    def own(part):
        for side in range(2):
            z_send(part, side, 0)

    def p_copy(owner, way, row):
        there = wo.at[:, block(row, cols), block(owner, ocols)]
        return remote(
            there,
            there,
            p_send.at[owner, way],
            p_recv.at[owner, way],
            (sp, beside[(0, 1, 0, 1)[way]], tp),
        )

    def spread(owner):
        for way in range(2):
            p_copy(owner, way, fs).start()

    def side_of(d):
        return 1 if 0 < d < ns - 1 else 0

    def each_block(d, use):
        if d == 0:
            use(sp)
            return
        for side in range(2):

            @pl.when(arrives(OUT, side, d))
            def _():
                use(owner_of(side, d))

    def pass_step(d):
        side = side_of(d)

        def use(owner):
            p_copy(owner, side, beside[side]).wait_recv()
            p_copy(owner, 3 - side, beside[side]).start()

        each_block(d, use)

    def rest_step(d):
        side = side_of(d)

        def use(owner):
            p_copy(owner, 1 - side, beside[1 - side]).wait_recv()
            p_copy(owner, 3 - side, beside[2]).wait_recv()

        each_block(d, use)

    def drain_step(d):
        side = side_of(d)

        def use(owner):
            for way in range(2):
                p_copy(owner, way, fs).wait_send()
            p_copy(owner, 3 - side, beside[side]).wait_send()

        each_block(d, use)

    def z_step(part, d):
        for side in range(2):

            @pl.when(arrives(part, side, d))
            def _():
                owner = owner_of(side, d)
                z_copy(part, side, d - 1, owner).wait_recv()
                if d < ns - 1:
                    z_send(part, side, d)
                if part == OUT:
                    spread(owner)

    def x_copy(way, seq):
        first, rows = ((0, half), (0, half), (0, half // 2), (half // 2, half // 2))[way]
        there = normed.at[pl.ds(pl.multiple_of(seq * tokens + tp * half + first, rows), rows)]
        return remote(
            there, there, x_send.at[way], x_recv.at[way], (sp, beside[(0, 1, 1, 0)[way]], tp)
        )

    def d_copy(k, seq, part):
        there = normed.at[pl.ds(pl.multiple_of(seq * tokens + part * half, half), half)]
        return remote(there, there, d_send.at[k], d_recv.at[k], partner)

    def guest_rows(ref, seq, part):
        return ref.at[pl.ds(pl.multiple_of(seq * tokens + part * half, half), half)]

    def t_copy(j):
        return remote(
            guest_rows(normed, around[j], tp),
            guest_rows(guest, around[j], tp),
            t_send.at[j],
            t_recv.at[j],
            (pair, fs, tp),
        )

    def u_copy(seq):
        there = guest_rows(guest, seq, tp)
        return remote(there, there, u_send, u_recv, (sp, beside[1], tp))

    def v_copy(k, part):
        there = guest_rows(guest, around[k], part)
        return remote(there, there, v_send.at[k], v_recv.at[k], partner)

    def guest_from_pair(j):
        @pl.when(hosts)
        def _():
            t_copy(j).wait_recv()
            if j == 1:
                u_copy(around[1]).start()
            v_copy(j, tp).start()

    def guest_from_beside():
        @pl.when(hosts)
        def _():
            u_copy(around[3]).wait_recv()
            v_copy(3, tp).start()

    def guest_to_pair(j):
        @pl.when(guests)
        def _():
            t_copy(j).start()

    def activations_in(way):
        x_copy(way, beside[way]).wait_recv()
        x_copy(way + 2, beside[way]).start()
        d_copy(way + 1, beside[way], tp).start()

    def tile(i):
        return pl.ds(pl.multiple_of(i * tokens, tokens), tokens)

    def project(part, into):
        first, count = SPANS[part]

        def body(i, carried):
            into[tile(i), :] = jnp.dot(
                normed[tile(i), :],
                wbuf[:, first * cols : (first + count) * cols],
                preferred_element_type=F32,
            ).astype(BF16)
            return carried

        lax.fori_loop(0, nf, body, 0)

    def mix_copy(m, k, seq, source):
        return remote(
            mine.at[m, seq],
            got.at[m, :, block(source, cols)],
            m_send.at[m, k],
            m_recv.at[m, k],
            (sp, beside[k], tp),
        )

    def hand_out(m):
        for k in (2, 0, 1):
            mix_copy(m, k, beside[k], fs).start()
        got[m, :, block(fs, cols)] = mine[m, fs]

    def state_copies(d, source):
        here = (local_stat, passed) if d == 0 else (stats.at[source], states.at[source])
        return (
            remote(here[0], stats.at[source], s_send.at[0, d], s_recv.at[0, d], up),
            remote(here[1], states.at[source], s_send.at[1, d], s_recv.at[1, d], up),
        )

    def state_send(d):
        @pl.when(has_up & (sp - d >= 0))
        def _():
            for copy in state_copies(d, sp - d):
                copy.start()

    def state_step(d):
        @pl.when(sp - d >= 0)
        def _():
            for copy in state_copies(d - 1, sp - d):
                copy.wait_recv()
            if d < ns - 1:
                state_send(d)

    def join_states():
        carry[...] = jnp.zeros_like(carry)
        carry_m[...] = jnp.zeros_like(carry_m)
        for source in range(ns - 1):

            @pl.when(source < sp)
            def _():
                for s in range(nf):
                    before = stats[source, s : s + 1, :] + carry_m[s : s + 1, :]
                    peak = stats[source, nf + s : nf + s + 1, :]
                    top = jnp.maximum(before, peak)
                    carry[s] = jnp.exp(before - top) * carry[s] + jnp.exp(peak - top) * states[
                        source, s
                    ].astype(F32)
                    carry_m[s : s + 1, :] = top

    def rim_copy():
        return remote(
            padded.at[:, pl.ds(tokens, RIM), :],
            padded.at[:, pl.ds(0, RIM), :],
            r_send,
            r_recv,
            up,
        )

    inner = hosts & (sp + 2 < ns)
    outer = hosts & (sp > 1)

    def products(source, seq, held):
        three = jnp.dot(
            source[tile(seq), :],
            wbuf[:, SPANS[MIX][0] * cols :],
            preferred_element_type=F32,
        ).astype(BF16)
        both = three[:, : 2 * cols].astype(F32)
        held[seq, RIM:, :] = (both[:, :cols] * both[:, cols:]).astype(BF16).astype(F32)
        return three[:, 2 * cols :]

    def convolve(held, seq, gate):
        tap = taps[:, block(g, cols)]
        total = jnp.zeros((tokens, cols), F32)
        for j in range(TAPS):
            at = RIM - (TAPS - 1) + j
            total = total + tap[j : j + 1, :] * held[seq, at : at + tokens, :]
        return (gate.astype(F32) * total).astype(BF16)

    def c_copy(k, seq, source):
        return remote(
            guest_mine.at[seq],
            got.at[0, :, block(source, cols)],
            c_send.at[k],
            c_recv.at[k],
            (pair, around[k], tp),
        )

    def own_products():
        @pl.when(hosts)
        def _():
            def body(i, carried):
                gated[tile(i), :] = products(normed, i, padded)
                return carried

            lax.fori_loop(0, nf, body, 0)

        @pl.when(inner)
        def _():
            rim_copy().start()

    def guest_part(k):
        seq = around[k]
        v_copy(k, 1 - tp).wait_recv()
        gate = products(guest, seq, guest_padded)
        guest_padded[seq, 0:RIM, :] = jnp.where(inner, 0.0, padded[seq, tokens : tokens + RIM, :])
        guest_mine[seq] = convolve(guest_padded, seq, gate)

    def own_part(seq):
        @pl.when(inner)
        def _():
            padded[seq, 0:RIM, :] = guest_padded[seq, tokens : tokens + RIM, :]

        return convolve(padded, seq, gated[tile(seq), :])

    loads[2].wait()
    loads[3].wait()
    pl.semaphore_wait(
        barrier, 2 * nf - 1 + has_up.astype(jnp.int32) + has_down.astype(jnp.int32)
    )
    own(KV)
    loads[0].wait()
    loads[1].wait()
    step = 32

    def norm_rows(i, carried):
        x = raw[pl.ds(pl.multiple_of(i * step, step), step), :].astype(F32)
        scale = lax.rsqrt(jnp.mean(x * x, axis=-1, keepdims=True) + EPSILON)
        rows = pl.ds(pl.multiple_of(fs * tokens + tp * half + i * step, step), step)
        normed[rows, :] = (x * scale * gain[...]).astype(BF16)
        return carried

    lax.fori_loop(0, half // step, norm_rows, 0)
    for way in range(2):
        x_copy(way, fs).start()
    d_copy(0, fs, tp).start()
    loads[8].wait()
    loads[9].wait()
    own(OUT)
    z_step(KV, 1)
    spread(sp)
    loads[5].wait()
    loads[6].wait()
    own(MIX)
    for way in range(2):
        activations_in(way)
    guest_to_pair(1)
    z_step(OUT, 1)
    z_step(KV, 2)
    for way in range(2, 4):
        x_copy(way, beside[2]).wait_recv()
    d_copy(3, beside[2], tp).start()
    loads[7].wait()
    own(GATE)
    loads[4].wait()
    own(QUERY)
    z_step(OUT, 2)
    z_step(KV, 3)
    for j in range(10, 16):
        loads[j].wait()
    for k, seq in enumerate(around):
        d_copy(k, seq, 1 - tp).wait_recv()

    row_at = lax.broadcasted_iota(jnp.int32, (tokens, tokens), 0)
    col_at = lax.broadcasted_iota(jnp.int32, (tokens, tokens), 1)
    gates = jnp.concatenate([wi[...].astype(F32), wf[...].astype(F32)], axis=0).astype(BF16)
    heads = wi.shape[0]
    own_gate = lax.broadcasted_iota(jnp.int32, (2 * heads, tokens), 0)
    own_bias = lax.broadcasted_iota(jnp.int32, (1, heads), 1)
    bias_in = jnp.sum(jnp.where(own_bias == g, bias[0:1, :], 0.0), axis=1, keepdims=True)
    bias_out = jnp.sum(jnp.where(own_bias == g, bias[1:2, :], 0.0), axis=1, keepdims=True)
    line = lax.broadcasted_iota(jnp.int32, (128, tokens), 0)
    packed = jnp.zeros((128, tokens), F32)
    for s in range(nf):
        raw_gates = lax.dot_general(
            gates,
            normed[s * tokens : (s + 1) * tokens, :],
            (((1,), (1,)), ((), ())),
            preferred_element_type=F32,
        )
        entry = jnp.sum(jnp.where(own_gate == g, raw_gates, 0.0), axis=0, keepdims=True) + bias_in
        forget = (
            jnp.sum(jnp.where(own_gate == heads + g, raw_gates, 0.0), axis=0, keepdims=True)
            + bias_out
        )
        shift = jnp.sum(jnp.where(own_gate[:heads] == g, decay[s], 0.0), axis=0, keepdims=True)
        forget = jnp.minimum(forget, 0.0) - jnp.log1p(jnp.exp(-jnp.abs(forget))) + shift
        packed = jnp.where(line == s, forget, packed)
        packed = jnp.where(line == nf + s, entry, packed)
    ones = jnp.where(row_at <= col_at, 1.0, 0.0).astype(F32)
    sums = jnp.dot(packed, ones, precision=HIGHEST_PRECISION, preferred_element_type=F32)
    sums = jnp.where(line < nf, sums, packed)
    logs_t[...] = sums
    logs[...] = sums.T
    project(KV, kv)
    for s in range(nf):
        rows = pl.ds(s * tokens, tokens)
        total = logs_t[s : s + 1, tokens - 1 : tokens]
        reach = total - logs[:, s : s + 1] + logs[:, nf + s : nf + s + 1]
        peak = jnp.max(reach, axis=0, keepdims=True)
        weighted = (kv[rows, cols:].astype(F32) * jnp.exp(reach - peak)).astype(BF16)
        passed[s] = lax.dot_general(
            kv[rows, :cols], weighted, (((0,), (0,)), ((), ())), preferred_element_type=F32
        ).astype(BF16)
        local_stat[s : s + 1, :] = jnp.broadcast_to(total, (1, 128))
        local_stat[nf + s : nf + s + 1, :] = jnp.broadcast_to(peak, (1, 128))

    guest_from_pair(1)
    state_send(0)
    guest_to_pair(2)
    z_step(QUERY, 1)
    z_step(OUT, 3)
    pass_step(0)
    guest_to_pair(0)
    state_step(1)
    z_step(MIX, 1)
    z_step(GATE, 1)
    pass_step(1)
    state_step(2)
    z_step(QUERY, 2)
    state_step(3)
    pass_step(2)
    pass_step(3)
    z_step(QUERY, 3)
    guest_from_pair(2)
    join_states()
    project(QUERY, query)

    scale = HEAD_DIM ** (-0.5)
    head_gain = head[:, block(g, cols)]
    causal = row_at >= col_at
    for s in range(nf):
        rows = pl.ds(s * tokens, tokens)
        scores = lax.dot_general(
            query[rows, :], kv[rows, :cols], (((1,), (1,)), ((), ())), preferred_element_type=F32
        )
        sums = logs[:, s : s + 1]
        pairs = jnp.where(
            causal,
            sums - logs_t[s : s + 1, :] + logs_t[nf + s : nf + s + 1, :],
            FAR_BELOW,
        )
        carried = sums + carry_m[s : s + 1, 0:1]
        top = jnp.maximum(carried, jnp.max(pairs, axis=1, keepdims=True))
        weights = (jnp.exp(pairs - top) * scores).astype(BF16)
        cell = jnp.dot(weights, kv[rows, cols:], preferred_element_type=F32)
        cell = cell + jnp.exp(carried - top) * jnp.dot(
            query[rows, :], carry[s].astype(BF16), preferred_element_type=F32
        )
        cell = cell * scale
        cell = cell * lax.rsqrt(jnp.mean(cell * cell, axis=-1, keepdims=True) + EPSILON)
        mine[1, s] = (cell * head_gain).astype(BF16)

    hand_out(1)
    z_step(MIX, 2)
    z_step(GATE, 2)
    guest_from_beside()
    own_products()

    @pl.when(outer)
    def _():
        rim_copy().wait_recv()

    @pl.when(hosts)
    def _():
        guest_part(1)
        mine[0, beside[0]] = own_part(beside[0])
        c_copy(1, around[1], fs).start()
        guest_part(3)
        mix_copy(0, 0, beside[0], fs).start()
        mine[0, beside[2]] = own_part(beside[2])
        c_copy(3, around[3], fs).start()
        guest_part(2)
        mix_copy(0, 2, beside[2], fs).start()
        mine[0, beside[1]] = own_part(beside[1])
        c_copy(2, around[2], fs).start()

    guest_from_pair(0)

    @pl.when(hosts)
    def _():
        guest_part(0)
        mix_copy(0, 1, beside[1], fs).start()
        got[0, :, block(fs, cols)] = own_part(fs)
        c_copy(0, around[0], fs).start()

    for d in range(ns):
        rest_step(d)
    for k in range(nf - 1):
        mix_copy(1, k, beside[k], beside[k]).wait_recv()

    def memory_share(i, carried):
        acc[:, block(i, ocols)] = jnp.dot(
            got[1], wo[1, :, block(i, ocols)], preferred_element_type=F32
        )
        return carried

    lax.fori_loop(0, ns, memory_share, 0)

    def e_copy(i):
        return remote(
            share.at[:, block(i, ocols)],
            other.at[:, block(i, ocols)],
            e_send.at[i],
            e_recv.at[i],
            partner,
        )

    def add_pair(i, pair):
        acc[:, block(i, ocols)] = acc[:, block(i, ocols)] + jnp.dot(
            got[0, :, block(pair, 2 * cols)],
            wo[0, block(pair, 2 * cols), block(i, ocols)],
            preferred_element_type=F32,
        )

    def conv_in(hosted, guested):
        @pl.when(hosts)
        def _():
            for k in hosted:
                mix_copy(0, k, beside[k], beside[k]).wait_recv()

        @pl.when(guests)
        def _():
            for k in guested:
                c_copy(k, around[k], around[k]).wait_recv()

    conv_in((1, 2), (2, 3))
    for i in range(ns):
        add_pair(i, 1 - fy)
    conv_in((0,), (0, 1))
    for i in range(ns):
        add_pair(i, fy)
        share[:, block(i, ocols)] = acc[block(1 - tp, half), block(i, ocols)].astype(BF16)
        if i > 0:
            e_copy(i - 1).start()
    e_copy(ns - 1).start()
    for i in range(ns):
        e_copy(i).wait_recv()
        out_ref[:, block(i, ocols)] = (
            acc[block(tp, half), block(i, ocols)] + other[:, block(i, ocols)].astype(F32)
        ).astype(BF16)

    def sent(i, carried):
        e_copy(i).wait_send()
        return carried

    lax.fori_loop(0, ns, sent, 0)
    for d in range(ns):
        drain_step(d)
    for way in range(4):
        x_copy(way, (fs, fs, beside[0], beside[1])[way]).wait_send()
    for k, seq in enumerate(around):
        d_copy(k, seq, tp).wait_send()
    for k in range(nf - 1):
        mix_copy(1, k, beside[k], fs).wait_send()

    @pl.when(hosts)
    def _():
        for k in range(nf - 1):
            mix_copy(0, k, beside[k], fs).wait_send()
        for k in range(nf):
            v_copy(k, tp).wait_send()
            c_copy(k, around[k], fs).wait_send()
        u_copy(around[1]).wait_send()

    @pl.when(guests)
    def _():
        for j in range(nf - 1):
            t_copy(j).wait_send()

    @pl.when(inner)
    def _():
        rim_copy().wait_send()

    for side in range(2):
        for d in range(ns - 1):
            for parts in ((KV, QUERY, OUT), (MIX, GATE)):

                @pl.when(sends(parts[0], side, d))
                def _():
                    for part in parts:
                        z_copy(part, side, d, owner_of(side, d)).wait_send()

    for d in range(ns - 1):

        @pl.when(has_up & (sp - d >= 0))
        def _():
            for copy in state_copies(d, sp - d):
                copy.wait_send()


def whole_layer(act, gain, weights, wi, wf, bias, decay, taps, head, w_out_conv, w_out_mem):
    ns, nf = (lax.axis_size("sp"), lax.axis_size("fs"))
    tokens, model = act.shape
    half = tokens // 2
    depth, cols = weights[0].shape
    ocols = w_out_conv.shape[1]
    count = nf * tokens
    anywhere = pl.BlockSpec(memory_space=pl.ANY)
    dma = pltpu.SemaphoreType.DMA
    vmem = pltpu.VMEM
    return pl.pallas_call(
        functools.partial(layer_kernel, ns, nf),
        out_shape=pltpu.VMEM((half, ns * ocols), BF16),
        in_specs=[anywhere] * 16,
        out_specs=pl.BlockSpec(memory_space=pltpu.VMEM),
        scratch_shapes=[
            vmem((half, model), BF16),
            vmem(gain.shape, F32),
            vmem((count, model), BF16),
            vmem((ns * depth, 6 * cols), BF16),
            vmem(wi.shape, BF16),
            vmem(wf.shape, BF16),
            vmem(bias.shape, F32),
            vmem(decay.shape, F32),
            vmem(taps.shape, F32),
            vmem(head.shape, F32),
            vmem((2, nf * cols, ns * ocols), BF16),
            vmem((count, 2 * cols), BF16),
            vmem((count, cols), BF16),
            vmem((tokens, 128), F32),
            vmem((128, tokens), F32),
            vmem((2 * nf, 128), F32),
            vmem((nf, cols, cols), BF16),
            vmem((ns - 1, nf, cols, cols), BF16),
            vmem((ns - 1, 2 * nf, 128), F32),
            vmem((nf, cols, cols), F32),
            vmem((nf, 128), F32),
            vmem((nf, RIM + tokens, cols), F32),
            vmem((count, cols), BF16),
            vmem((2, nf, tokens, cols), BF16),
            vmem((2, tokens, nf * cols), BF16),
            vmem((count, model), BF16),
            vmem((nf, RIM + tokens, cols), F32),
            vmem((nf, tokens, cols), BF16),
            vmem((tokens, ns * ocols), F32),
            vmem((half, ns * ocols), BF16),
            vmem((half, ns * ocols), BF16),
            dma((16,)),
            dma((4,)),
            dma((4,)),
            dma((nf,)),
            dma((nf,)),
            dma((2, ns - 1, PARTS)),
            dma((2, ns - 1, PARTS)),
            dma((ns, 4)),
            dma((ns, 4)),
            dma((2, ns - 1)),
            dma((2, ns - 1)),
            dma,
            dma,
            dma((2, nf - 1)),
            dma((2, nf - 1)),
            dma((ns,)),
            dma((ns,)),
            dma((nf - 1,)),
            dma((nf - 1,)),
            dma,
            dma,
            dma((nf,)),
            dma((nf,)),
            dma((nf,)),
            dma((nf,)),
        ],
        compiler_params=pltpu.CompilerParams(
            collective_id=0, has_side_effects=True, vmem_limit_bytes=54 * 1024 * 1024
        ),
    )(act, gain, *weights, wi, wf, bias, decay, taps, head, w_out_conv, w_out_mem)


def shards(
    activations,
    norm_gain,
    w_conv_gate,
    w_conv_mult,
    w_conv_in,
    conv_taps,
    w_query,
    w_key,
    w_value,
    w_input_gate,
    w_forget_gate,
    gate_bias,
    decay_shift,
    head_gain,
    w_out_conv,
    w_out_mem,
):
    group_index = lax.axis_index(("fs", "tp"))
    heads_here = MEMORY_HEADS // (lax.axis_size("fs") * lax.axis_size("tp"))
    channels = w_conv_gate.shape[1]
    ns, nf, nt = (lax.axis_size("sp"), lax.axis_size("fs"), lax.axis_size("tp"))
    if ns == 4 and nf == 4 and nt == 2 and heads_here == 1 and channels == HEAD_DIM:
        return whole_layer(
            activations[0],
            norm_gain[None, :],
            (w_key, w_value, w_query, w_conv_mult, w_conv_in, w_conv_gate),
            w_input_gate.T,
            w_forget_gate.T,
            gate_bias,
            decay_shift.transpose(0, 2, 1),
            conv_taps,
            head_gain[None, :],
            w_out_conv,
            w_out_mem,
        )[None]
    sequences = lax.all_gather(activations, "fs", axis=0, tiled=True)
    seq_count = sequences.shape[0]
    tokens = sequences.shape[1]
    model_width = sequences.shape[2]
    row_count = seq_count * tokens
    flat_rows = sequences.reshape(row_count, model_width).astype(jnp.float32)
    normed = (
        flat_rows
        * lax.rsqrt(jnp.mean(flat_rows * flat_rows, axis=-1, keepdims=True) + EPSILON)
        * norm_gain
    ).astype(jnp.bfloat16)
    pieces = (
        lax.all_gather(w_conv_gate, "sp", axis=0, tiled=True),
        lax.all_gather(w_conv_mult, "sp", axis=0, tiled=True),
        lax.all_gather(w_conv_in, "sp", axis=0, tiled=True),
        lax.all_gather(w_query, "sp", axis=0, tiled=True),
        lax.all_gather(w_key, "sp", axis=0, tiled=True),
        lax.all_gather(w_value, "sp", axis=0, tiled=True),
    )
    projected = tuple(
        (jnp.dot(normed, shard_piece, preferred_element_type=jnp.float32) for shard_piece in pieces)
    )
    conv_gate, conv_mult, conv_in, query, keys_proj, value = [
        tensor.astype(jnp.bfloat16).reshape(seq_count, tokens, -1) for tensor in projected
    ]
    entry_cols = lax.dynamic_slice_in_dim(w_input_gate, group_index * heads_here, heads_here, 1)
    forget_cols = lax.dynamic_slice_in_dim(w_forget_gate, group_index * heads_here, heads_here, 1)
    gate_values = jnp.dot(
        normed,
        jnp.concatenate([entry_cols, forget_cols], axis=1),
        preferred_element_type=jnp.float32,
    ).reshape(seq_count, tokens, 2 * heads_here)
    product = (conv_mult.astype(jnp.float32) * conv_in.astype(jnp.float32)).astype(jnp.bfloat16)
    ntaps = conv_taps.shape[0]
    rim_rows = from_behind(product[:, tokens - (ntaps - 1) :, :], "sp", 1)
    padded = jnp.concatenate([rim_rows, product], axis=1).astype(jnp.float32)
    tap_weights = lax.dynamic_slice_in_dim(conv_taps, group_index * channels, channels, 1)
    mixed_sum = jnp.zeros((seq_count, tokens, channels), jnp.float32)
    for tap_index in range(ntaps):
        mixed_sum = (
            mixed_sum + tap_weights[tap_index] * padded[:, tap_index : tap_index + tokens, :]
        )
    conv_out = (conv_gate.astype(jnp.float32) * mixed_sum).astype(jnp.bfloat16)
    bias_rows = lax.dynamic_slice_in_dim(gate_bias, group_index * heads_here, heads_here, 1)
    decay_rows = lax.dynamic_slice_in_dim(decay_shift, group_index * heads_here, heads_here, 2)
    entry = gate_values[..., :heads_here] + bias_rows[0]
    log_forget = jax.nn.log_sigmoid(gate_values[..., heads_here:] + bias_rows[1]) + decay_rows
    cell = memory_cell(
        head_rows(query, seq_count, heads_here),
        head_rows(keys_proj, seq_count, heads_here),
        head_rows(value, seq_count, heads_here),
        gate_rows(entry, seq_count, heads_here),
        gate_rows(log_forget, seq_count, heads_here),
    )
    cell = cell * lax.rsqrt(jnp.mean(cell * cell, axis=-1, keepdims=True) + EPSILON)
    gain_rows = lax.dynamic_slice_in_dim(
        head_gain, group_index * heads_here * HEAD_DIM, heads_here * HEAD_DIM, 0
    ).reshape(1, heads_here, 1, HEAD_DIM)
    scaled = cell.reshape(seq_count, heads_here, tokens, HEAD_DIM) * gain_rows
    mem_out = (
        scaled.transpose(0, 2, 1, 3)
        .reshape(seq_count, tokens, heads_here * HEAD_DIM)
        .astype(jnp.bfloat16)
    )
    conv_seq, mem_seq = (
        lax.all_to_all(conv_out, "fs", split_axis=0, concat_axis=2, tiled=True),
        lax.all_to_all(mem_out, "fs", split_axis=0, concat_axis=2, tiled=True),
    )
    rows_conv, rows_mem = (
        lax.all_gather(w_out_conv, "fs", axis=0, tiled=True),
        lax.all_gather(w_out_mem, "fs", axis=0, tiled=True),
    )
    full_conv, full_mem = (
        lax.all_gather(rows_conv, "sp", axis=1, tiled=True),
        lax.all_gather(rows_mem, "sp", axis=1, tiled=True),
    )
    conv_flat = conv_seq[0]
    mem_flat = mem_seq[0]
    output = lax.psum_scatter(
        (
            jnp.dot(conv_flat, full_conv, preferred_element_type=jnp.float32)
            + jnp.dot(mem_flat, full_mem, preferred_element_type=jnp.float32)
        ).astype(jnp.bfloat16),
        "tp",
        scatter_dimension=0,
        tiled=True,
    ).astype(jnp.float32)
    return output.astype(jnp.bfloat16).reshape(1, output.shape[0], -1)


def solution(mesh):
    return jax.shard_map(
        shards,
        mesh=mesh,
        in_specs=(
            P("fs", "sp", None),
            P(),
            P("sp", ("fs", "tp")),
            P("sp", ("fs", "tp")),
            P("sp", ("fs", "tp")),
            P(),
            P("sp", ("fs", "tp")),
            P("sp", ("fs", "tp")),
            P("sp", ("fs", "tp")),
            P(),
            P(),
            P(),
            P(None, "sp", None),
            P(),
            P(("fs", "tp"), "sp"),
            P(("fs", "tp"), "sp"),
        ),
        out_specs=P("fs", ("sp", "tp"), None),
        check_vma=False,
    )
```

```python
import functools

import jax
import jax.numpy as jnp
from jax import lax
from jax.experimental import pallas as pl
from jax.experimental.pallas import tpu as pltpu
from jax.sharding import PartitionSpec as P

MEMORY_HEADS = 8
HEAD_DIM = 128
BLOCK = 64


EPSILON = 1e-06
FAR_BELOW = -1e30
HIGHEST_PRECISION = lax.Precision.HIGHEST


def prefix(value, axis, join, neutral):
    count, mine = (lax.axis_size(axis), lax.axis_index(axis))
    total, peak, state = value
    stats = jnp.stack([total, peak], axis=1)[..., None]
    stats = jnp.broadcast_to(stats, stats.shape[:2] + state.shape[-1:])
    packed = lax.all_gather(jnp.concatenate([state, stats], axis=1), axis)
    height = state.shape[1]
    pieces = (packed[:, :, height, 0], packed[:, :, height + 1, 0], packed[:, :, :height])
    subtotal = jax.tree.map(
        lambda part, zero: jnp.full_like(part, 0) + jnp.asarray(zero, part.dtype), value, neutral
    )

    def lap(position, subtotal):
        longer = join(subtotal, jax.tree.map(lambda part: part[position], pieces))
        return jax.tree.map(lambda new, old: jnp.where(position < mine, new, old), longer, subtotal)

    return lax.fori_loop(0, count - 1, lap, subtotal)


def from_behind(array, axis, by):
    peers = lax.axis_size(axis)
    pairs = [(i, i + by) for i in range(peers) if 0 <= i + by < peers]
    return lax.ppermute(array, axis, pairs)


def combine_states(earlier, later):
    total_one, peak_one, state_one = earlier
    total_two, peak_two, state_two = later
    peak_new = jnp.maximum(total_two + peak_one, peak_two)
    scale_old = jnp.exp(total_two + peak_one - peak_new)
    scale_new = jnp.exp(peak_two - peak_new)
    return (
        total_one + total_two,
        peak_new,
        scale_old[..., None, None] * state_one + scale_new[..., None, None] * state_two,
    )


def head_rows(values, seq_count, heads_here):
    tokens = values.shape[1]
    split_heads = values.reshape(seq_count, tokens, heads_here, HEAD_DIM).transpose(0, 2, 1, 3)
    return split_heads.reshape(seq_count * heads_here, tokens, HEAD_DIM).astype(jnp.float32)


def gate_rows(values, seq_count, heads_here):
    tokens = values.shape[1]
    return values.transpose(0, 2, 1).reshape(seq_count * heads_here, tokens)


def memory_cell(query_rows, key_rows, value_rows, entry_gate, log_forget):
    members = query_rows.shape[0]
    tokens = query_rows.shape[1]
    head_width = query_rows.shape[2]
    nblocks = tokens // BLOCK
    block_shape = (members, nblocks, BLOCK, head_width)
    query_blocks = query_rows.reshape(block_shape)
    key_blocks = key_rows.reshape(block_shape) * head_width ** (-0.5)
    value_blocks = value_rows.reshape(block_shape)
    entry_blocks = entry_gate.reshape(members, nblocks, BLOCK)
    forget_sums = jnp.cumsum(log_forget.reshape(members, nblocks, BLOCK), axis=-1)
    block_total = forget_sums[..., -1]
    local_logs = block_total[..., None] - forget_sums + entry_blocks
    local_peak = jnp.max(local_logs, axis=-1)
    local_weights = jnp.exp(local_logs - local_peak[..., None])
    local_state = jnp.einsum(
        "bclv,bclk->bcvk",
        local_weights[..., None] * value_blocks,
        key_blocks,
        precision=HIGHEST_PRECISION,
    )

    def advance(running, block_item):
        return (combine_states(running, block_item), running)

    zero_sums = jnp.zeros((members,), jnp.float32)
    low_peaks = jnp.full((members,), FAR_BELOW, jnp.float32)
    zero_states = jnp.zeros((members, head_width, head_width), jnp.float32)
    block_items = (
        jnp.moveaxis(block_total, 1, 0),
        jnp.moveaxis(local_peak, 1, 0),
        jnp.moveaxis(local_state, 1, 0),
    )
    device_total, inner_states = lax.scan(advance, (zero_sums, low_peaks, zero_states), block_items)
    inner_states = tuple((jnp.moveaxis(tensor, 0, 1) for tensor in inner_states))
    total_sum, total_peak, total_state = device_total
    before = prefix(
        (total_sum, total_peak, total_state),
        "sp",
        combine_states,
        (zero_sums, low_peaks, zero_states),
    )
    opening = combine_states((zero_sums, zero_sums, zero_states), before)
    opening = tuple((tensor[:, None] for tensor in opening))
    _, prior_peak, prior_state = combine_states(opening, inner_states)
    positions = jnp.arange(BLOCK)
    causal_mask = positions[:, None] >= positions[None, :]
    pair_logs = jnp.where(
        causal_mask,
        forget_sums[..., :, None] - forget_sums[..., None, :] + entry_blocks[..., None, :],
        -jnp.inf,
    )
    carried_logs = forget_sums + prior_peak[..., None]
    row_peak = jnp.maximum(carried_logs, jnp.max(pair_logs, axis=-1))
    inner_weights = jnp.exp(pair_logs - row_peak[..., None])
    carried_weights = jnp.exp(carried_logs - row_peak)
    scores = inner_weights * jnp.einsum(
        "bcld,bcsd->bcls", query_blocks, key_blocks, precision=HIGHEST_PRECISION
    )
    numerator = carried_weights[..., None] * jnp.einsum(
        "bcvk,bclk->bclv", prior_state, query_blocks, precision=HIGHEST_PRECISION
    ) + jnp.einsum("bcls,bcsv->bclv", scores, value_blocks, precision=HIGHEST_PRECISION)
    return numerator.reshape(members, tokens, head_width)


MESH = pl.DeviceIdType.MESH
F32 = jnp.float32
BF16 = jnp.bfloat16
TAPS = 3
RIM = 8
KV, QUERY, OUT, MIX, GATE = range(5)
SPANS = {KV: (0, 2), QUERY: (2, 1), MIX: (3, 2), GATE: (5, 1)}
PARTS = 5


def layer_kernel(
    ns,
    nf,
    act_ref,
    gain_ref,
    w0_ref,
    w1_ref,
    w2_ref,
    w3_ref,
    w4_ref,
    w5_ref,
    wi_ref,
    wf_ref,
    bias_ref,
    decay_ref,
    taps_ref,
    head_ref,
    wc_ref,
    wm_ref,
    out_ref,
    raw,
    gain,
    normed,
    wbuf,
    wi,
    wf,
    bias,
    decay,
    taps,
    head,
    wo,
    kv,
    query,
    logs,
    logs_t,
    local_stat,
    passed,
    states,
    stats,
    carry,
    carry_m,
    padded,
    gated,
    mine,
    got,
    guest,
    guest_padded,
    guest_mine,
    last,
    wo_last,
    acc,
    share,
    other,
    load_sem,
    x_send,
    x_recv,
    d_send,
    d_recv,
    w_send,
    w_recv,
    p_send,
    p_recv,
    s_send,
    s_recv,
    r_send,
    r_recv,
    m_send,
    m_recv,
    e_send,
    e_recv,
    t_send,
    t_recv,
    u_send,
    u_recv,
    v_send,
    v_recv,
    c_send,
    c_recv,
    l_send,
    l_recv,
):
    sp, fs, tp = (lax.axis_index("sp"), lax.axis_index("fs"), lax.axis_index("tp"))
    g = fs * 2 + tp
    depth, cols = w0_ref.shape
    half, model = raw.shape
    tokens = 2 * half
    ocols = wc_ref.shape[1]
    partner = (sp, fs, 1 - tp)
    has_up, has_down = (sp + 1 < ns, sp > 0)
    up, down = ((sp + 1, fs, tp), (sp - 1, fs, tp))
    fy, fx = (fs // 2, lax.rem(fs, 2))
    beside = (fy * 2 + 1 - fx, (1 - fy) * 2 + fx, (1 - fy) * 2 + 1 - fx)

    pair = sp + 1 - 2 * lax.rem(sp, 2)
    hosts = has_up & has_down
    guests = jnp.logical_not(hosts)
    around = (fs,) + beside

    def block(index, size):
        return pl.ds(pl.multiple_of(index * size, size), size)

    def remote(src, dst, send, recv, to):
        return pltpu.make_async_remote_copy(
            src, dst, send, recv, device_id=to, device_id_type=MESH
        )

    loads = [pltpu.make_async_copy(act_ref.at[block(tp, half)], raw, load_sem.at[0])]
    loads.append(pltpu.make_async_copy(gain_ref, gain, load_sem.at[1]))
    for j, ref in enumerate((w0_ref, w1_ref, w2_ref, w3_ref, w4_ref, w5_ref)):
        loads.append(
            pltpu.make_async_copy(
                ref, wbuf.at[block(sp, depth), pl.ds(j * cols, cols)], load_sem.at[2 + j]
            )
        )
    for m, ref in enumerate((wc_ref, wm_ref)):
        loads.append(
            pltpu.make_async_copy(
                ref, wo.at[m, block(fs, cols), block(sp, ocols)], load_sem.at[8 + m]
            )
        )
    smalls = (
        (wi_ref, wi),
        (wf_ref, wf),
        (bias_ref, bias),
        (decay_ref, decay),
        (taps_ref, taps),
        (head_ref, head),
    )
    for j, (ref, held) in enumerate(smalls):
        loads.append(pltpu.make_async_copy(ref, held, load_sem.at[10 + j]))
    for j in (0, 1, 2, 3, 8, 9, 5, 6, 7, 4, 10, 11, 12, 13, 14, 15):
        loads[j].start()

    barrier = pltpu.get_barrier_semaphore()
    for peer in beside:
        pl.semaphore_signal(barrier, inc=1, device_id=(sp, peer, tp), device_id_type=MESH)
        pl.semaphore_signal(barrier, inc=1, device_id=(pair, peer, tp), device_id_type=MESH)
    for there in (partner, (pair, fs, 1 - tp)):
        pl.semaphore_signal(barrier, inc=1, device_id=there, device_id_type=MESH)

    @pl.when(has_up)
    def _():
        pl.semaphore_signal(barrier, inc=1, device_id=up, device_id_type=MESH)

    @pl.when(has_down)
    def _():
        pl.semaphore_signal(barrier, inc=1, device_id=down, device_id_type=MESH)

    def place(part, owner):
        if part == OUT:
            return wo.at[:, block(fs, cols), block(owner, ocols)]
        first, count = SPANS[part]
        return wbuf.at[block(owner, depth), pl.ds(first * cols, count * cols)]

    def z_copy(part, side, d, owner):
        there = place(part, owner)
        return remote(
            there,
            there,
            w_send.at[side, d, part],
            w_recv.at[side, d, part],
            (up, down)[side],
        )

    def owner_of(side, d):
        return sp - d if side == 0 else sp + d

    def arrives(part, side, d):
        there = (sp - d >= 0) if side == 0 else (sp + d < ns)
        return there & hosts if part in (MIX, GATE) else there

    def sends(part, side, d):
        there = (sp - d >= 0) if side == 0 else (sp + d < ns)
        if part in (MIX, GATE):
            return there & ((sp + 2 < ns) if side == 0 else (sp > 1))
        return there & (has_up if side == 0 else has_down)

    def z_send(part, side, d):
        @pl.when(sends(part, side, d))
        def _():
            z_copy(part, side, d, owner_of(side, d)).start()

    def own(part):
        for side in range(2):
            z_send(part, side, 0)

    def p_copy(owner, way, row):
        there = wo.at[:, block(row, cols), block(owner, ocols)]
        return remote(
            there,
            there,
            p_send.at[owner, way],
            p_recv.at[owner, way],
            (sp, beside[(0, 1, 0, 1)[way]], tp),
        )

    def spread(owner):
        for way in range(2):
            p_copy(owner, way, fs).start()

    def side_of(d):
        return 1 if 0 < d < ns - 1 else 0

    def each_block(d, use):
        if d == 0:
            use(sp)
            return
        for side in range(2):

            @pl.when(arrives(OUT, side, d))
            def _():
                use(owner_of(side, d))

    def pass_step(d):
        side = side_of(d)

        def use(owner):
            p_copy(owner, side, beside[side]).wait_recv()
            p_copy(owner, 3 - side, beside[side]).start()

        each_block(d, use)

    def rest_step(d):
        side = side_of(d)

        def use(owner):
            p_copy(owner, 1 - side, beside[1 - side]).wait_recv()
            p_copy(owner, 3 - side, beside[2]).wait_recv()

        each_block(d, use)

    def drain_step(d):
        side = side_of(d)

        def use(owner):
            for way in range(2):
                p_copy(owner, way, fs).wait_send()
            p_copy(owner, 3 - side, beside[side]).wait_send()

        each_block(d, use)

    def z_step(part, d):
        for side in range(2):

            @pl.when(arrives(part, side, d))
            def _():
                owner = owner_of(side, d)
                z_copy(part, side, d - 1, owner).wait_recv()
                if d < ns - 1:
                    z_send(part, side, d)
                if part == OUT:
                    spread(owner)

    def x_copy(way, seq):
        first, rows = ((0, half), (0, half), (0, half // 2), (half // 2, half // 2))[way]
        there = normed.at[pl.ds(pl.multiple_of(seq * tokens + tp * half + first, rows), rows)]
        return remote(
            there, there, x_send.at[way], x_recv.at[way], (sp, beside[(0, 1, 1, 0)[way]], tp)
        )

    def d_copy(k, seq, part):
        there = normed.at[pl.ds(pl.multiple_of(seq * tokens + part * half, half), half)]
        return remote(there, there, d_send.at[k], d_recv.at[k], partner)

    def guest_rows(ref, seq, part):
        return ref.at[pl.ds(pl.multiple_of(seq * tokens + part * half, half), half)]

    quarter = half // 2

    def piece(ref, j, part):
        if j in (0, nf - 1):
            first = fs * tokens + part * half + (0 if j == 0 else quarter)
            return ref.at[pl.ds(pl.multiple_of(first, quarter), quarter)]
        return guest_rows(ref, around[j], part)

    def t_copy(j):
        return remote(
            piece(normed, j, tp),
            piece(guest, j, tp),
            t_send.at[j],
            t_recv.at[j],
            (pair, fs, tp),
        )

    def u_copy(seq):
        there = guest_rows(guest, seq, tp)
        return remote(there, there, u_send, u_recv, (sp, beside[1], tp))

    def v_copy(k, part):
        there = guest_rows(guest, around[k], part)
        return remote(there, there, v_send.at[k], v_recv.at[k], partner)

    def v_piece(j, part):
        at = 0 if j == 0 else nf
        there = piece(guest, j, part)
        return remote(there, there, v_send.at[at], v_recv.at[at], partner)

    def guest_from_pair(j):
        @pl.when(hosts)
        def _():
            t_copy(j).wait_recv()
            if j == 1:
                u_copy(around[1]).start()
            if j in (0, nf - 1):
                v_piece(j, tp).start()
            else:
                v_copy(j, tp).start()

    def guest_from_beside():
        @pl.when(hosts)
        def _():
            u_copy(around[3]).wait_recv()
            v_copy(3, tp).start()

    def guest_to_pair(j):
        @pl.when(guests)
        def _():
            t_copy(j).start()

    def activations_in(way):
        x_copy(way, beside[way]).wait_recv()
        x_copy(way + 2, beside[way]).start()
        d_copy(way + 1, beside[way], tp).start()

    def tile(i):
        return pl.ds(pl.multiple_of(i * tokens, tokens), tokens)

    def project(part, into):
        first, count = SPANS[part]

        def body(i, carried):
            into[tile(i), :] = jnp.dot(
                normed[tile(i), :],
                wbuf[:, first * cols : (first + count) * cols],
                preferred_element_type=F32,
            ).astype(BF16)
            return carried

        lax.fori_loop(0, nf, body, 0)

    def mix_copy(m, k, seq, source):
        return remote(
            mine.at[m, seq],
            got.at[m, :, block(source, cols)],
            m_send.at[m, k],
            m_recv.at[m, k],
            (sp, beside[k], tp),
        )

    def hand_out(m):
        for k in (2, 0, 1):
            mix_copy(m, k, beside[k], fs).start()
        got[m, :, block(fs, cols)] = mine[m, fs]

    def state_copies(d, source):
        here = (local_stat, passed) if d == 0 else (stats.at[source], states.at[source])
        return (
            remote(here[0], stats.at[source], s_send.at[0, d], s_recv.at[0, d], up),
            remote(here[1], states.at[source], s_send.at[1, d], s_recv.at[1, d], up),
        )

    def state_send(d):
        @pl.when(has_up & (sp - d >= 0))
        def _():
            for copy in state_copies(d, sp - d):
                copy.start()

    def state_step(d):
        @pl.when(sp - d >= 0)
        def _():
            for copy in state_copies(d - 1, sp - d):
                copy.wait_recv()
            if d < ns - 1:
                state_send(d)

    def join_states():
        carry[...] = jnp.zeros_like(carry)
        carry_m[...] = jnp.zeros_like(carry_m)
        for source in range(ns - 1):

            @pl.when(source < sp)
            def _():
                for s in range(nf):
                    before = stats[source, s : s + 1, :] + carry_m[s : s + 1, :]
                    peak = stats[source, nf + s : nf + s + 1, :]
                    top = jnp.maximum(before, peak)
                    carry[s] = jnp.exp(before - top) * carry[s] + jnp.exp(peak - top) * states[
                        source, s
                    ].astype(F32)
                    carry_m[s : s + 1, :] = top

    def rim_copy():
        return remote(
            padded.at[:, pl.ds(tokens, RIM), :],
            padded.at[:, pl.ds(0, RIM), :],
            r_send,
            r_recv,
            up,
        )

    inner = hosts & (sp + 2 < ns)
    outer = hosts & (sp > 1)

    def products(source, seq, held):
        three = jnp.dot(
            source[tile(seq), :],
            wbuf[:, SPANS[MIX][0] * cols :],
            preferred_element_type=F32,
        ).astype(BF16)
        both = three[:, : 2 * cols].astype(F32)
        held[seq, RIM:, :] = (both[:, :cols] * both[:, cols:]).astype(BF16).astype(F32)
        return three[:, 2 * cols :]

    def convolve(held, seq, gate):
        tap = taps[:, block(g, cols)]
        total = jnp.zeros((tokens, cols), F32)
        for j in range(TAPS):
            at = RIM - (TAPS - 1) + j
            total = total + tap[j : j + 1, :] * held[seq, at : at + tokens, :]
        return (gate.astype(F32) * total).astype(BF16)

    def c_copy(k, seq, source):
        return remote(
            guest_mine.at[seq],
            got.at[0, :, block(source, cols)],
            c_send.at[k],
            c_recv.at[k],
            (pair, around[k], tp),
        )

    def last_copy(k, source):
        core = tp if k == 0 else 1 - tp
        return remote(
            guest_mine.at[fs, block(core, half)],
            last.at[:, block(source, cols)],
            c_send.at[k],
            c_recv.at[k],
            (pair, fs, core),
        )

    def row_copy():
        return remote(wo.at[0, block(fs, cols)], wo_last, l_send, l_recv, partner)

    def own_products():
        @pl.when(hosts)
        def _():
            def body(i, carried):
                gated[tile(i), :] = products(normed, i, padded)
                return carried

            lax.fori_loop(0, nf, body, 0)

        @pl.when(inner)
        def _():
            rim_copy().start()

    def guest_part(k):
        seq = around[k]
        if k == 0:
            v_piece(0, 1 - tp).wait_recv()
            v_piece(nf - 1, 1 - tp).wait_recv()
        else:
            v_copy(k, 1 - tp).wait_recv()
        gate = products(guest, seq, guest_padded)
        guest_padded[seq, 0:RIM, :] = jnp.where(inner, 0.0, padded[seq, tokens : tokens + RIM, :])
        guest_mine[seq] = convolve(guest_padded, seq, gate)

    def own_part(seq):
        @pl.when(inner)
        def _():
            padded[seq, 0:RIM, :] = guest_padded[seq, tokens : tokens + RIM, :]

        return convolve(padded, seq, gated[tile(seq), :])

    loads[0].wait()
    loads[1].wait()
    step = 32

    def norm_rows(i, carried):
        x = raw[pl.ds(pl.multiple_of(i * step, step), step), :].astype(F32)
        scale = lax.rsqrt(jnp.mean(x * x, axis=-1, keepdims=True) + EPSILON)
        rows = pl.ds(pl.multiple_of(fs * tokens + tp * half + i * step, step), step)
        normed[rows, :] = (x * scale * gain[...]).astype(BF16)
        return carried

    lax.fori_loop(0, half // step, norm_rows, 0)
    loads[2].wait()
    loads[3].wait()
    pl.semaphore_wait(
        barrier, 2 * nf + has_up.astype(jnp.int32) + has_down.astype(jnp.int32)
    )
    own(KV)
    for way in range(2):
        x_copy(way, fs).start()
    d_copy(0, fs, tp).start()
    loads[8].wait()
    loads[9].wait()
    own(OUT)
    z_step(KV, 1)
    spread(sp)
    loads[5].wait()
    loads[6].wait()
    own(MIX)
    for way in range(2):
        activations_in(way)
    guest_to_pair(1)
    z_step(OUT, 1)
    z_step(KV, 2)
    for way in range(2, 4):
        x_copy(way, beside[2]).wait_recv()
    d_copy(3, beside[2], tp).start()
    loads[7].wait()
    own(GATE)
    loads[4].wait()
    own(QUERY)
    z_step(OUT, 2)
    for j in range(10, 16):
        loads[j].wait()
    for k, seq in enumerate(around):
        d_copy(k, seq, 1 - tp).wait_recv()

    row_at = lax.broadcasted_iota(jnp.int32, (tokens, tokens), 0)
    col_at = lax.broadcasted_iota(jnp.int32, (tokens, tokens), 1)
    gates = jnp.concatenate([wi[...].astype(F32), wf[...].astype(F32)], axis=0).astype(BF16)
    heads = wi.shape[0]
    own_gate = lax.broadcasted_iota(jnp.int32, (2 * heads, tokens), 0)
    own_bias = lax.broadcasted_iota(jnp.int32, (1, heads), 1)
    bias_in = jnp.sum(jnp.where(own_bias == g, bias[0:1, :], 0.0), axis=1, keepdims=True)
    bias_out = jnp.sum(jnp.where(own_bias == g, bias[1:2, :], 0.0), axis=1, keepdims=True)
    line = lax.broadcasted_iota(jnp.int32, (128, tokens), 0)
    packed = jnp.zeros((128, tokens), F32)
    for s in range(nf):
        raw_gates = lax.dot_general(
            gates,
            normed[s * tokens : (s + 1) * tokens, :],
            (((1,), (1,)), ((), ())),
            preferred_element_type=F32,
        )
        entry = jnp.sum(jnp.where(own_gate == g, raw_gates, 0.0), axis=0, keepdims=True) + bias_in
        forget = (
            jnp.sum(jnp.where(own_gate == heads + g, raw_gates, 0.0), axis=0, keepdims=True)
            + bias_out
        )
        shift = jnp.sum(jnp.where(own_gate[:heads] == g, decay[s], 0.0), axis=0, keepdims=True)
        forget = jnp.minimum(forget, 0.0) - jnp.log1p(jnp.exp(-jnp.abs(forget))) + shift
        packed = jnp.where(line == s, forget, packed)
        packed = jnp.where(line == nf + s, entry, packed)
    ones = jnp.where(row_at <= col_at, 1.0, 0.0).astype(F32)
    sums = jnp.dot(packed, ones, precision=HIGHEST_PRECISION, preferred_element_type=F32)
    sums = jnp.where(line < nf, sums, packed)
    logs_t[...] = sums
    logs[...] = sums.T
    z_step(KV, 3)
    project(KV, kv)
    for s in range(nf):
        rows = pl.ds(s * tokens, tokens)
        total = logs_t[s : s + 1, tokens - 1 : tokens]
        reach = total - logs[:, s : s + 1] + logs[:, nf + s : nf + s + 1]
        peak = jnp.max(reach, axis=0, keepdims=True)
        weighted = (kv[rows, cols:].astype(F32) * jnp.exp(reach - peak)).astype(BF16)
        passed[s] = lax.dot_general(
            kv[rows, :cols], weighted, (((0,), (0,)), ((), ())), preferred_element_type=F32
        ).astype(BF16)
        local_stat[s : s + 1, :] = jnp.broadcast_to(total, (1, 128))
        local_stat[nf + s : nf + s + 1, :] = jnp.broadcast_to(peak, (1, 128))

    guest_from_pair(1)
    state_send(0)
    guest_to_pair(2)
    z_step(QUERY, 1)
    z_step(OUT, 3)

    @pl.when(guests)
    def _():
        row_copy().start()

    pass_step(0)
    guest_to_pair(0)
    guest_to_pair(nf - 1)
    state_step(1)
    z_step(MIX, 1)
    z_step(GATE, 1)
    pass_step(1)
    state_step(2)
    z_step(QUERY, 2)
    state_step(3)
    pass_step(2)
    pass_step(3)
    z_step(QUERY, 3)
    guest_from_pair(2)
    join_states()
    project(QUERY, query)

    scale = HEAD_DIM ** (-0.5)
    head_gain = head[:, block(g, cols)]
    causal = row_at >= col_at
    for s in range(nf):
        rows = pl.ds(s * tokens, tokens)
        scores = lax.dot_general(
            query[rows, :], kv[rows, :cols], (((1,), (1,)), ((), ())), preferred_element_type=F32
        )
        sums = logs[:, s : s + 1]
        pairs = jnp.where(
            causal,
            sums - logs_t[s : s + 1, :] + logs_t[nf + s : nf + s + 1, :],
            FAR_BELOW,
        )
        carried = sums + carry_m[s : s + 1, 0:1]
        top = jnp.maximum(carried, jnp.max(pairs, axis=1, keepdims=True))
        weights = (jnp.exp(pairs - top) * scores).astype(BF16)
        cell = jnp.dot(weights, kv[rows, cols:], preferred_element_type=F32)
        cell = cell + jnp.exp(carried - top) * jnp.dot(
            query[rows, :], carry[s].astype(BF16), preferred_element_type=F32
        )
        cell = cell * scale
        cell = cell * lax.rsqrt(jnp.mean(cell * cell, axis=-1, keepdims=True) + EPSILON)
        mine[1, s] = (cell * head_gain).astype(BF16)

    hand_out(1)
    z_step(MIX, 2)
    z_step(GATE, 2)
    guest_from_beside()
    own_products()

    @pl.when(outer)
    def _():
        rim_copy().wait_recv()

    @pl.when(hosts)
    def _():
        guest_part(1)
        mine[0, beside[0]] = own_part(beside[0])
        c_copy(1, around[1], fs).start()
        guest_part(3)
        mix_copy(0, 0, beside[0], fs).start()
        mine[0, beside[2]] = own_part(beside[2])
        c_copy(3, around[3], fs).start()
        guest_part(2)
        mix_copy(0, 2, beside[2], fs).start()
        mine[0, beside[1]] = own_part(beside[1])
        c_copy(2, around[2], fs).start()
        mix_copy(0, 1, beside[1], fs).start()

    guest_from_pair(0)
    guest_from_pair(nf - 1)

    @pl.when(hosts)
    def _():
        guest_part(0)
        got[0, :, block(fs, cols)] = own_part(fs)
        for k in (0, nf):
            last_copy(k, tp).start()

    for d in range(ns):
        rest_step(d)
    for k in range(nf - 1):
        mix_copy(1, k, beside[k], beside[k]).wait_recv()

    def memory_share(i, carried):
        acc[:, block(i, ocols)] = jnp.dot(
            got[1], wo[1, :, block(i, ocols)], preferred_element_type=F32
        )
        return carried

    lax.fori_loop(0, ns, memory_share, 0)

    def e_copy(i):
        return remote(
            share.at[:, block(i, ocols)],
            other.at[:, block(i, ocols)],
            e_send.at[i],
            e_recv.at[i],
            partner,
        )

    def add_conv(i, first, count):
        acc[:, block(i, ocols)] = acc[:, block(i, ocols)] + jnp.dot(
            got[0, :, pl.ds(first, count)],
            wo[0, pl.ds(first, count), block(i, ocols)],
            preferred_element_type=F32,
        )

    def add_pair(i, pair_at):
        add_conv(i, pl.multiple_of(pair_at * 2 * cols, 2 * cols), 2 * cols)

    def hand_over(i):
        share[:, block(i, ocols)] = acc[block(1 - tp, half), block(i, ocols)].astype(BF16)
        if i > 0:
            e_copy(i - 1).start()
        if i == ns - 1:
            e_copy(i).start()

    @pl.when(hosts)
    def _():
        for k in (1, 2):
            mix_copy(0, k, beside[k], beside[k]).wait_recv()
        for i in range(ns):
            add_pair(i, 1 - fy)
        mix_copy(0, 0, beside[0], beside[0]).wait_recv()
        for i in range(ns):
            add_pair(i, fy)
            hand_over(i)
        for i in range(ns):
            e_copy(i).wait_recv()
            out_ref[:, block(i, ocols)] = (
                acc[block(tp, half), block(i, ocols)] + other[:, block(i, ocols)].astype(F32)
            ).astype(BF16)

    @pl.when(guests)
    def _():
        c_copy(1, around[1], around[1]).wait_recv()
        for i in range(ns):
            add_conv(i, pl.multiple_of(beside[0] * cols, cols), cols)
        for k in range(2, nf):
            c_copy(k, around[k], around[k]).wait_recv()
        for i in range(ns):
            add_pair(i, 1 - fy)
            hand_over(i)
        row_copy().wait_recv()
        for i in range(ns):
            e_copy(i).wait_recv()
            acc[block(tp, half), block(i, ocols)] = acc[
                block(tp, half), block(i, ocols)
            ] + other[:, block(i, ocols)].astype(F32)
        for k in (0, nf):
            last_copy(k, tp if k == 0 else 1 - tp).wait_recv()
        for i in range(ns):
            out_ref[:, block(i, ocols)] = (
                acc[block(tp, half), block(i, ocols)]
                + jnp.dot(
                    last[:, block(tp, cols)],
                    wo[0, block(fs, cols), block(i, ocols)],
                    preferred_element_type=F32,
                )
                + jnp.dot(
                    last[:, block(1 - tp, cols)],
                    wo_last[:, block(i, ocols)],
                    preferred_element_type=F32,
                )
            ).astype(BF16)

    def sent(i, carried):
        e_copy(i).wait_send()
        return carried

    lax.fori_loop(0, ns, sent, 0)
    for d in range(ns):
        drain_step(d)
    for way in range(4):
        x_copy(way, (fs, fs, beside[0], beside[1])[way]).wait_send()
    for k, seq in enumerate(around):
        d_copy(k, seq, tp).wait_send()
    for k in range(nf - 1):
        mix_copy(1, k, beside[k], fs).wait_send()

    @pl.when(hosts)
    def _():
        for k in range(nf - 1):
            mix_copy(0, k, beside[k], fs).wait_send()
        for k in range(1, nf):
            v_copy(k, tp).wait_send()
        for j in (0, nf - 1):
            v_piece(j, tp).wait_send()
        for k in range(1, nf):
            c_copy(k, around[k], fs).wait_send()
        for k in (0, nf):
            last_copy(k, tp).wait_send()
        u_copy(around[1]).wait_send()

    @pl.when(guests)
    def _():
        for j in range(nf):
            t_copy(j).wait_send()
        row_copy().wait_send()

    @pl.when(inner)
    def _():
        rim_copy().wait_send()

    for side in range(2):
        for d in range(ns - 1):
            for parts in ((KV, QUERY, OUT), (MIX, GATE)):

                @pl.when(sends(parts[0], side, d))
                def _():
                    for part in parts:
                        z_copy(part, side, d, owner_of(side, d)).wait_send()

    for d in range(ns - 1):

        @pl.when(has_up & (sp - d >= 0))
        def _():
            for copy in state_copies(d, sp - d):
                copy.wait_send()


def whole_layer(act, gain, weights, wi, wf, bias, decay, taps, head, w_out_conv, w_out_mem):
    ns, nf = (lax.axis_size("sp"), lax.axis_size("fs"))
    tokens, model = act.shape
    half = tokens // 2
    depth, cols = weights[0].shape
    ocols = w_out_conv.shape[1]
    count = nf * tokens
    anywhere = pl.BlockSpec(memory_space=pl.ANY)
    dma = pltpu.SemaphoreType.DMA
    vmem = pltpu.VMEM
    return pl.pallas_call(
        functools.partial(layer_kernel, ns, nf),
        out_shape=pltpu.VMEM((half, ns * ocols), BF16),
        in_specs=[anywhere] * 16,
        out_specs=pl.BlockSpec(memory_space=pltpu.VMEM),
        scratch_shapes=[
            vmem((half, model), BF16),
            vmem(gain.shape, F32),
            vmem((count, model), BF16),
            vmem((ns * depth, 6 * cols), BF16),
            vmem(wi.shape, BF16),
            vmem(wf.shape, BF16),
            vmem(bias.shape, F32),
            vmem(decay.shape, F32),
            vmem(taps.shape, F32),
            vmem(head.shape, F32),
            vmem((2, nf * cols, ns * ocols), BF16),
            vmem((count, 2 * cols), BF16),
            vmem((count, cols), BF16),
            vmem((tokens, 128), F32),
            vmem((128, tokens), F32),
            vmem((2 * nf, 128), F32),
            vmem((nf, cols, cols), BF16),
            vmem((ns - 1, nf, cols, cols), BF16),
            vmem((ns - 1, 2 * nf, 128), F32),
            vmem((nf, cols, cols), F32),
            vmem((nf, 128), F32),
            vmem((nf, RIM + tokens, cols), F32),
            vmem((count, cols), BF16),
            vmem((2, nf, tokens, cols), BF16),
            vmem((2, tokens, nf * cols), BF16),
            vmem((count, model), BF16),
            vmem((nf, RIM + tokens, cols), F32),
            vmem((nf, tokens, cols), BF16),
            vmem((half, 2 * cols), BF16),
            vmem((cols, ns * ocols), BF16),
            vmem((tokens, ns * ocols), F32),
            vmem((half, ns * ocols), BF16),
            vmem((half, ns * ocols), BF16),
            dma((16,)),
            dma((4,)),
            dma((4,)),
            dma((nf,)),
            dma((nf,)),
            dma((2, ns - 1, PARTS)),
            dma((2, ns - 1, PARTS)),
            dma((ns, 4)),
            dma((ns, 4)),
            dma((2, ns - 1)),
            dma((2, ns - 1)),
            dma,
            dma,
            dma((2, nf - 1)),
            dma((2, nf - 1)),
            dma((ns,)),
            dma((ns,)),
            dma((nf,)),
            dma((nf,)),
            dma,
            dma,
            dma((nf + 1,)),
            dma((nf + 1,)),
            dma((nf + 1,)),
            dma((nf + 1,)),
            dma,
            dma,
        ],
        compiler_params=pltpu.CompilerParams(
            collective_id=0, has_side_effects=True, vmem_limit_bytes=54 * 1024 * 1024
        ),
    )(act, gain, *weights, wi, wf, bias, decay, taps, head, w_out_conv, w_out_mem)


def shards(
    activations,
    norm_gain,
    w_conv_gate,
    w_conv_mult,
    w_conv_in,
    conv_taps,
    w_query,
    w_key,
    w_value,
    w_input_gate,
    w_forget_gate,
    gate_bias,
    decay_shift,
    head_gain,
    w_out_conv,
    w_out_mem,
):
    group_index = lax.axis_index(("fs", "tp"))
    heads_here = MEMORY_HEADS // (lax.axis_size("fs") * lax.axis_size("tp"))
    channels = w_conv_gate.shape[1]
    ns, nf, nt = (lax.axis_size("sp"), lax.axis_size("fs"), lax.axis_size("tp"))
    if ns == 4 and nf == 4 and nt == 2 and heads_here == 1 and channels == HEAD_DIM:
        return whole_layer(
            activations[0],
            norm_gain[None, :],
            (w_key, w_value, w_query, w_conv_mult, w_conv_in, w_conv_gate),
            w_input_gate.T,
            w_forget_gate.T,
            gate_bias,
            decay_shift.transpose(0, 2, 1),
            conv_taps,
            head_gain[None, :],
            w_out_conv,
            w_out_mem,
        )[None]
    sequences = lax.all_gather(activations, "fs", axis=0, tiled=True)
    seq_count = sequences.shape[0]
    tokens = sequences.shape[1]
    model_width = sequences.shape[2]
    row_count = seq_count * tokens
    flat_rows = sequences.reshape(row_count, model_width).astype(jnp.float32)
    normed = (
        flat_rows
        * lax.rsqrt(jnp.mean(flat_rows * flat_rows, axis=-1, keepdims=True) + EPSILON)
        * norm_gain
    ).astype(jnp.bfloat16)
    pieces = (
        lax.all_gather(w_conv_gate, "sp", axis=0, tiled=True),
        lax.all_gather(w_conv_mult, "sp", axis=0, tiled=True),
        lax.all_gather(w_conv_in, "sp", axis=0, tiled=True),
        lax.all_gather(w_query, "sp", axis=0, tiled=True),
        lax.all_gather(w_key, "sp", axis=0, tiled=True),
        lax.all_gather(w_value, "sp", axis=0, tiled=True),
    )
    projected = tuple(
        (jnp.dot(normed, shard_piece, preferred_element_type=jnp.float32) for shard_piece in pieces)
    )
    conv_gate, conv_mult, conv_in, query, keys_proj, value = [
        tensor.astype(jnp.bfloat16).reshape(seq_count, tokens, -1) for tensor in projected
    ]
    entry_cols = lax.dynamic_slice_in_dim(w_input_gate, group_index * heads_here, heads_here, 1)
    forget_cols = lax.dynamic_slice_in_dim(w_forget_gate, group_index * heads_here, heads_here, 1)
    gate_values = jnp.dot(
        normed,
        jnp.concatenate([entry_cols, forget_cols], axis=1),
        preferred_element_type=jnp.float32,
    ).reshape(seq_count, tokens, 2 * heads_here)
    product = (conv_mult.astype(jnp.float32) * conv_in.astype(jnp.float32)).astype(jnp.bfloat16)
    ntaps = conv_taps.shape[0]
    rim_rows = from_behind(product[:, tokens - (ntaps - 1) :, :], "sp", 1)
    padded = jnp.concatenate([rim_rows, product], axis=1).astype(jnp.float32)
    tap_weights = lax.dynamic_slice_in_dim(conv_taps, group_index * channels, channels, 1)
    mixed_sum = jnp.zeros((seq_count, tokens, channels), jnp.float32)
    for tap_index in range(ntaps):
        mixed_sum = (
            mixed_sum + tap_weights[tap_index] * padded[:, tap_index : tap_index + tokens, :]
        )
    conv_out = (conv_gate.astype(jnp.float32) * mixed_sum).astype(jnp.bfloat16)
    bias_rows = lax.dynamic_slice_in_dim(gate_bias, group_index * heads_here, heads_here, 1)
    decay_rows = lax.dynamic_slice_in_dim(decay_shift, group_index * heads_here, heads_here, 2)
    entry = gate_values[..., :heads_here] + bias_rows[0]
    log_forget = jax.nn.log_sigmoid(gate_values[..., heads_here:] + bias_rows[1]) + decay_rows
    cell = memory_cell(
        head_rows(query, seq_count, heads_here),
        head_rows(keys_proj, seq_count, heads_here),
        head_rows(value, seq_count, heads_here),
        gate_rows(entry, seq_count, heads_here),
        gate_rows(log_forget, seq_count, heads_here),
    )
    cell = cell * lax.rsqrt(jnp.mean(cell * cell, axis=-1, keepdims=True) + EPSILON)
    gain_rows = lax.dynamic_slice_in_dim(
        head_gain, group_index * heads_here * HEAD_DIM, heads_here * HEAD_DIM, 0
    ).reshape(1, heads_here, 1, HEAD_DIM)
    scaled = cell.reshape(seq_count, heads_here, tokens, HEAD_DIM) * gain_rows
    mem_out = (
        scaled.transpose(0, 2, 1, 3)
        .reshape(seq_count, tokens, heads_here * HEAD_DIM)
        .astype(jnp.bfloat16)
    )
    conv_seq, mem_seq = (
        lax.all_to_all(conv_out, "fs", split_axis=0, concat_axis=2, tiled=True),
        lax.all_to_all(mem_out, "fs", split_axis=0, concat_axis=2, tiled=True),
    )
    rows_conv, rows_mem = (
        lax.all_gather(w_out_conv, "fs", axis=0, tiled=True),
        lax.all_gather(w_out_mem, "fs", axis=0, tiled=True),
    )
    full_conv, full_mem = (
        lax.all_gather(rows_conv, "sp", axis=1, tiled=True),
        lax.all_gather(rows_mem, "sp", axis=1, tiled=True),
    )
    conv_flat = conv_seq[0]
    mem_flat = mem_seq[0]
    output = lax.psum_scatter(
        (
            jnp.dot(conv_flat, full_conv, preferred_element_type=jnp.float32)
            + jnp.dot(mem_flat, full_mem, preferred_element_type=jnp.float32)
        ).astype(jnp.bfloat16),
        "tp",
        scatter_dimension=0,
        tiled=True,
    ).astype(jnp.float32)
    return output.astype(jnp.bfloat16).reshape(1, output.shape[0], -1)


def solution(mesh):
    return jax.shard_map(
        shards,
        mesh=mesh,
        in_specs=(
            P("fs", "sp", None),
            P(),
            P("sp", ("fs", "tp")),
            P("sp", ("fs", "tp")),
            P("sp", ("fs", "tp")),
            P(),
            P("sp", ("fs", "tp")),
            P("sp", ("fs", "tp")),
            P("sp", ("fs", "tp")),
            P(),
            P(),
            P(),
            P(None, "sp", None),
            P(),
            P(("fs", "tp"), "sp"),
            P(("fs", "tp"), "sp"),
        ),
        out_specs=P("fs", ("sp", "tp"), None),
        check_vma=False,
    )
```

```python
import functools

import jax
import jax.numpy as jnp
from jax import lax
from jax.experimental import pallas as pl
from jax.experimental.pallas import tpu as pltpu
from jax.sharding import PartitionSpec as P

MEMORY_HEADS = 8
HEAD_DIM = 128
BLOCK = 64


EPSILON = 1e-06
FAR_BELOW = -1e30
HIGHEST_PRECISION = lax.Precision.HIGHEST


def prefix(value, axis, join, neutral):
    count, mine = (lax.axis_size(axis), lax.axis_index(axis))
    total, peak, state = value
    stats = jnp.stack([total, peak], axis=1)[..., None]
    stats = jnp.broadcast_to(stats, stats.shape[:2] + state.shape[-1:])
    packed = lax.all_gather(jnp.concatenate([state, stats], axis=1), axis)
    height = state.shape[1]
    pieces = (packed[:, :, height, 0], packed[:, :, height + 1, 0], packed[:, :, :height])
    subtotal = jax.tree.map(
        lambda part, zero: jnp.full_like(part, 0) + jnp.asarray(zero, part.dtype), value, neutral
    )

    def lap(position, subtotal):
        longer = join(subtotal, jax.tree.map(lambda part: part[position], pieces))
        return jax.tree.map(lambda new, old: jnp.where(position < mine, new, old), longer, subtotal)

    return lax.fori_loop(0, count - 1, lap, subtotal)


def from_behind(array, axis, by):
    peers = lax.axis_size(axis)
    pairs = [(i, i + by) for i in range(peers) if 0 <= i + by < peers]
    return lax.ppermute(array, axis, pairs)


def combine_states(earlier, later):
    total_one, peak_one, state_one = earlier
    total_two, peak_two, state_two = later
    peak_new = jnp.maximum(total_two + peak_one, peak_two)
    scale_old = jnp.exp(total_two + peak_one - peak_new)
    scale_new = jnp.exp(peak_two - peak_new)
    return (
        total_one + total_two,
        peak_new,
        scale_old[..., None, None] * state_one + scale_new[..., None, None] * state_two,
    )


def head_rows(values, seq_count, heads_here):
    tokens = values.shape[1]
    split_heads = values.reshape(seq_count, tokens, heads_here, HEAD_DIM).transpose(0, 2, 1, 3)
    return split_heads.reshape(seq_count * heads_here, tokens, HEAD_DIM).astype(jnp.float32)


def gate_rows(values, seq_count, heads_here):
    tokens = values.shape[1]
    return values.transpose(0, 2, 1).reshape(seq_count * heads_here, tokens)


def memory_cell(query_rows, key_rows, value_rows, entry_gate, log_forget):
    members = query_rows.shape[0]
    tokens = query_rows.shape[1]
    head_width = query_rows.shape[2]
    nblocks = tokens // BLOCK
    block_shape = (members, nblocks, BLOCK, head_width)
    query_blocks = query_rows.reshape(block_shape)
    key_blocks = key_rows.reshape(block_shape) * head_width ** (-0.5)
    value_blocks = value_rows.reshape(block_shape)
    entry_blocks = entry_gate.reshape(members, nblocks, BLOCK)
    forget_sums = jnp.cumsum(log_forget.reshape(members, nblocks, BLOCK), axis=-1)
    block_total = forget_sums[..., -1]
    local_logs = block_total[..., None] - forget_sums + entry_blocks
    local_peak = jnp.max(local_logs, axis=-1)
    local_weights = jnp.exp(local_logs - local_peak[..., None])
    local_state = jnp.einsum(
        "bclv,bclk->bcvk",
        local_weights[..., None] * value_blocks,
        key_blocks,
        precision=HIGHEST_PRECISION,
    )

    def advance(running, block_item):
        return (combine_states(running, block_item), running)

    zero_sums = jnp.zeros((members,), jnp.float32)
    low_peaks = jnp.full((members,), FAR_BELOW, jnp.float32)
    zero_states = jnp.zeros((members, head_width, head_width), jnp.float32)
    block_items = (
        jnp.moveaxis(block_total, 1, 0),
        jnp.moveaxis(local_peak, 1, 0),
        jnp.moveaxis(local_state, 1, 0),
    )
    device_total, inner_states = lax.scan(advance, (zero_sums, low_peaks, zero_states), block_items)
    inner_states = tuple((jnp.moveaxis(tensor, 0, 1) for tensor in inner_states))
    total_sum, total_peak, total_state = device_total
    before = prefix(
        (total_sum, total_peak, total_state),
        "sp",
        combine_states,
        (zero_sums, low_peaks, zero_states),
    )
    opening = combine_states((zero_sums, zero_sums, zero_states), before)
    opening = tuple((tensor[:, None] for tensor in opening))
    _, prior_peak, prior_state = combine_states(opening, inner_states)
    positions = jnp.arange(BLOCK)
    causal_mask = positions[:, None] >= positions[None, :]
    pair_logs = jnp.where(
        causal_mask,
        forget_sums[..., :, None] - forget_sums[..., None, :] + entry_blocks[..., None, :],
        -jnp.inf,
    )
    carried_logs = forget_sums + prior_peak[..., None]
    row_peak = jnp.maximum(carried_logs, jnp.max(pair_logs, axis=-1))
    inner_weights = jnp.exp(pair_logs - row_peak[..., None])
    carried_weights = jnp.exp(carried_logs - row_peak)
    scores = inner_weights * jnp.einsum(
        "bcld,bcsd->bcls", query_blocks, key_blocks, precision=HIGHEST_PRECISION
    )
    numerator = carried_weights[..., None] * jnp.einsum(
        "bcvk,bclk->bclv", prior_state, query_blocks, precision=HIGHEST_PRECISION
    ) + jnp.einsum("bcls,bcsv->bclv", scores, value_blocks, precision=HIGHEST_PRECISION)
    return numerator.reshape(members, tokens, head_width)


MESH = pl.DeviceIdType.MESH
F32 = jnp.float32
BF16 = jnp.bfloat16
TAPS = 3
RIM = 8
KV, QUERY, OUT, MIX, GATE = range(5)
SPANS = {KV: (0, 2), QUERY: (2, 1), MIX: (3, 2), GATE: (5, 1)}
PARTS = 5


def layer_kernel(
    ns,
    nf,
    act_ref,
    gain_ref,
    w0_ref,
    w1_ref,
    w2_ref,
    w3_ref,
    w4_ref,
    w5_ref,
    wi_ref,
    wf_ref,
    bias_ref,
    decay_ref,
    taps_ref,
    head_ref,
    wc_ref,
    wm_ref,
    out_ref,
    raw,
    gain,
    normed,
    wbuf,
    wi,
    wf,
    bias,
    decay,
    taps,
    head,
    wo,
    kv,
    query,
    logs,
    logs_t,
    local_stat,
    passed,
    states,
    stats,
    carry,
    carry_m,
    padded,
    gated,
    mine,
    got,
    guest,
    guest_padded,
    guest_mine,
    last,
    wo_last,
    acc,
    share,
    other,
    load_sem,
    x_send,
    x_recv,
    d_send,
    d_recv,
    w_send,
    w_recv,
    p_send,
    p_recv,
    s_send,
    s_recv,
    r_send,
    r_recv,
    m_send,
    m_recv,
    e_send,
    e_recv,
    t_send,
    t_recv,
    u_send,
    u_recv,
    v_send,
    v_recv,
    c_send,
    c_recv,
    l_send,
    l_recv,
):
    sp, fs, tp = (lax.axis_index("sp"), lax.axis_index("fs"), lax.axis_index("tp"))
    g = fs * 2 + tp
    depth, cols = w0_ref.shape
    half, model = raw.shape
    tokens = 2 * half
    ocols = wc_ref.shape[1]
    partner = (sp, fs, 1 - tp)
    has_up, has_down = (sp + 1 < ns, sp > 0)
    up, down = ((sp + 1, fs, tp), (sp - 1, fs, tp))
    fy, fx = (fs // 2, lax.rem(fs, 2))
    beside = (fy * 2 + 1 - fx, (1 - fy) * 2 + fx, (1 - fy) * 2 + 1 - fx)

    pair = sp + 1 - 2 * lax.rem(sp, 2)
    hosts = has_up & has_down
    guests = jnp.logical_not(hosts)
    around = (fs,) + beside

    def block(index, size):
        return pl.ds(pl.multiple_of(index * size, size), size)

    def remote(src, dst, send, recv, to):
        return pltpu.make_async_remote_copy(
            src, dst, send, recv, device_id=to, device_id_type=MESH
        )

    loads = [pltpu.make_async_copy(act_ref.at[block(tp, half)], raw, load_sem.at[0])]
    loads.append(pltpu.make_async_copy(gain_ref, gain, load_sem.at[1]))
    for j, ref in enumerate((w0_ref, w1_ref, w2_ref, w3_ref, w4_ref, w5_ref)):
        loads.append(
            pltpu.make_async_copy(
                ref, wbuf.at[block(sp, depth), pl.ds(j * cols, cols)], load_sem.at[2 + j]
            )
        )
    for m, ref in enumerate((wc_ref, wm_ref)):
        loads.append(
            pltpu.make_async_copy(
                ref, wo.at[m, block(fs, cols), block(sp, ocols)], load_sem.at[8 + m]
            )
        )
    smalls = (
        (wi_ref, wi),
        (wf_ref, wf),
        (bias_ref, bias),
        (decay_ref, decay),
        (taps_ref, taps),
        (head_ref, head),
    )
    for j, (ref, held) in enumerate(smalls):
        loads.append(pltpu.make_async_copy(ref, held, load_sem.at[10 + j]))
    for j in (0, 1, 2, 3, 8, 9, 5, 6, 7, 4, 10, 11, 12, 13, 14, 15):
        loads[j].start()

    barrier = pltpu.get_barrier_semaphore()
    for peer in beside:
        pl.semaphore_signal(barrier, inc=1, device_id=(sp, peer, tp), device_id_type=MESH)
        pl.semaphore_signal(barrier, inc=1, device_id=(pair, peer, tp), device_id_type=MESH)
    for there in (partner, (pair, fs, 1 - tp)):
        pl.semaphore_signal(barrier, inc=1, device_id=there, device_id_type=MESH)

    @pl.when(has_up)
    def _():
        pl.semaphore_signal(barrier, inc=1, device_id=up, device_id_type=MESH)

    @pl.when(has_down)
    def _():
        pl.semaphore_signal(barrier, inc=1, device_id=down, device_id_type=MESH)

    def place(part, owner):
        if part == OUT:
            return wo.at[:, block(fs, cols), block(owner, ocols)]
        first, count = SPANS[part]
        return wbuf.at[block(owner, depth), pl.ds(first * cols, count * cols)]

    def z_copy(part, side, d, owner):
        there = place(part, owner)
        return remote(
            there,
            there,
            w_send.at[side, d, part],
            w_recv.at[side, d, part],
            (up, down)[side],
        )

    def owner_of(side, d):
        return sp - d if side == 0 else sp + d

    def arrives(part, side, d):
        there = (sp - d >= 0) if side == 0 else (sp + d < ns)
        return there & hosts if part in (MIX, GATE) else there

    def sends(part, side, d):
        there = (sp - d >= 0) if side == 0 else (sp + d < ns)
        if part in (MIX, GATE):
            return there & ((sp + 2 < ns) if side == 0 else (sp > 1))
        return there & (has_up if side == 0 else has_down)

    def z_send(part, side, d):
        @pl.when(sends(part, side, d))
        def _():
            z_copy(part, side, d, owner_of(side, d)).start()

    def own(part):
        for side in range(2):
            z_send(part, side, 0)

    def p_copy(owner, way, row):
        there = wo.at[:, block(row, cols), block(owner, ocols)]
        return remote(
            there,
            there,
            p_send.at[owner, way],
            p_recv.at[owner, way],
            (sp, beside[(0, 1, 0, 1)[way]], tp),
        )

    def spread(owner):
        for way in range(2):
            p_copy(owner, way, fs).start()

    def side_of(d):
        return 1 if 0 < d < ns - 1 else 0

    def each_block(d, use):
        if d == 0:
            use(sp)
            return
        for side in range(2):

            @pl.when(arrives(OUT, side, d))
            def _():
                use(owner_of(side, d))

    def pass_step(d):
        side = side_of(d)

        def use(owner):
            p_copy(owner, side, beside[side]).wait_recv()
            p_copy(owner, 3 - side, beside[side]).start()

        each_block(d, use)

    def rest_step(d):
        side = side_of(d)

        def use(owner):
            p_copy(owner, 1 - side, beside[1 - side]).wait_recv()
            p_copy(owner, 3 - side, beside[2]).wait_recv()

        each_block(d, use)

    def drain_step(d):
        side = side_of(d)

        def use(owner):
            for way in range(2):
                p_copy(owner, way, fs).wait_send()
            p_copy(owner, 3 - side, beside[side]).wait_send()

        each_block(d, use)

    def z_step(part, d):
        for side in range(2):

            @pl.when(arrives(part, side, d))
            def _():
                owner = owner_of(side, d)
                z_copy(part, side, d - 1, owner).wait_recv()
                if d < ns - 1:
                    z_send(part, side, d)
                if part == OUT:
                    spread(owner)

    def x_copy(way, seq):
        first, rows = ((0, half), (0, half), (0, half // 2), (half // 2, half // 2))[way]
        there = normed.at[pl.ds(pl.multiple_of(seq * tokens + tp * half + first, rows), rows)]
        return remote(
            there, there, x_send.at[way], x_recv.at[way], (sp, beside[(0, 1, 1, 0)[way]], tp)
        )

    def d_copy(k, seq, part):
        there = normed.at[pl.ds(pl.multiple_of(seq * tokens + part * half, half), half)]
        return remote(there, there, d_send.at[k], d_recv.at[k], partner)

    def guest_rows(ref, seq, part):
        return ref.at[pl.ds(pl.multiple_of(seq * tokens + part * half, half), half)]

    quarter = half // 2

    def piece(ref, j, part):
        if j in (0, nf - 1):
            first = fs * tokens + part * half + (0 if j == 0 else quarter)
            return ref.at[pl.ds(pl.multiple_of(first, quarter), quarter)]
        return guest_rows(ref, around[j], part)

    def t_copy(j):
        return remote(
            piece(normed, j, tp),
            piece(guest, j, tp),
            t_send.at[j],
            t_recv.at[j],
            (pair, fs, tp),
        )

    def u_copy(seq):
        there = guest_rows(guest, seq, tp)
        return remote(there, there, u_send, u_recv, (sp, beside[1], tp))

    def v_copy(k, part):
        there = guest_rows(guest, around[k], part)
        return remote(there, there, v_send.at[k], v_recv.at[k], partner)

    def v_piece(j, part):
        at = 0 if j == 0 else nf
        there = piece(guest, j, part)
        return remote(there, there, v_send.at[at], v_recv.at[at], partner)

    def guest_from_pair(j):
        @pl.when(hosts)
        def _():
            t_copy(j).wait_recv()
            if j == 1:
                u_copy(around[1]).start()
            if j in (0, nf - 1):
                v_piece(j, tp).start()
            else:
                v_copy(j, tp).start()

    def guest_from_beside():
        @pl.when(hosts)
        def _():
            u_copy(around[3]).wait_recv()
            v_copy(3, tp).start()

    def guest_to_pair(j):
        @pl.when(guests)
        def _():
            t_copy(j).start()

    def activations_in(way):
        x_copy(way, beside[way]).wait_recv()
        x_copy(way + 2, beside[way]).start()
        d_copy(way + 1, beside[way], tp).start()

    def tile(i):
        return pl.ds(pl.multiple_of(i * tokens, tokens), tokens)

    def project(part, into):
        first, count = SPANS[part]

        def body(i, carried):
            into[tile(i), :] = jnp.dot(
                normed[tile(i), :],
                wbuf[:, first * cols : (first + count) * cols],
                preferred_element_type=F32,
            ).astype(BF16)
            return carried

        lax.fori_loop(0, nf, body, 0)

    def mix_copy(m, k, seq, source):
        return remote(
            mine.at[m, seq],
            got.at[m, :, block(source, cols)],
            m_send.at[m, k],
            m_recv.at[m, k],
            (sp, beside[k], tp),
        )

    def hand_out(m):
        for k in (2, 0, 1):
            mix_copy(m, k, beside[k], fs).start()
        got[m, :, block(fs, cols)] = mine[m, fs]

    def state_copies(d, source):
        here = (local_stat, passed) if d == 0 else (stats.at[source], states.at[source])
        return (
            remote(here[0], stats.at[source], s_send.at[0, d], s_recv.at[0, d], up),
            remote(here[1], states.at[source], s_send.at[1, d], s_recv.at[1, d], up),
        )

    def state_send(d):
        @pl.when(has_up & (sp - d >= 0))
        def _():
            for copy in state_copies(d, sp - d):
                copy.start()

    def state_step(d):
        @pl.when(sp - d >= 0)
        def _():
            for copy in state_copies(d - 1, sp - d):
                copy.wait_recv()
            if d < ns - 1:
                state_send(d)

    def join_states():
        carry[...] = jnp.zeros_like(carry)
        carry_m[...] = jnp.zeros_like(carry_m)
        for source in range(ns - 1):

            @pl.when(source < sp)
            def _():
                for s in range(nf):
                    before = stats[source, s : s + 1, :] + carry_m[s : s + 1, :]
                    peak = stats[source, nf + s : nf + s + 1, :]
                    top = jnp.maximum(before, peak)
                    carry[s] = jnp.exp(before - top) * carry[s] + jnp.exp(peak - top) * states[
                        source, s
                    ].astype(F32)
                    carry_m[s : s + 1, :] = top

    def rim_copy():
        return remote(
            padded.at[:, pl.ds(tokens, RIM), :],
            padded.at[:, pl.ds(0, RIM), :],
            r_send,
            r_recv,
            up,
        )

    inner = hosts & (sp + 2 < ns)
    outer = hosts & (sp > 1)

    def products(source, seq, held):
        three = jnp.dot(
            source[tile(seq), :],
            wbuf[:, SPANS[MIX][0] * cols :],
            preferred_element_type=F32,
        ).astype(BF16)
        both = three[:, : 2 * cols].astype(F32)
        held[seq, RIM:, :] = (both[:, :cols] * both[:, cols:]).astype(BF16).astype(F32)
        return three[:, 2 * cols :]

    def convolve(held, seq, gate):
        tap = taps[:, block(g, cols)]
        total = jnp.zeros((tokens, cols), F32)
        for j in range(TAPS):
            at = RIM - (TAPS - 1) + j
            total = total + tap[j : j + 1, :] * held[seq, at : at + tokens, :]
        return (gate.astype(F32) * total).astype(BF16)

    def c_copy(k, seq, source):
        return remote(
            guest_mine.at[seq],
            got.at[0, :, block(source, cols)],
            c_send.at[k],
            c_recv.at[k],
            (pair, around[k], tp),
        )

    def last_copy(k, source):
        core = tp if k == 0 else 1 - tp
        return remote(
            guest_mine.at[fs, block(core, half)],
            last.at[:, block(source, cols)],
            c_send.at[k],
            c_recv.at[k],
            (pair, fs, core),
        )

    def row_copy():
        return remote(wo.at[0, block(fs, cols)], wo_last, l_send, l_recv, partner)

    def own_products():
        @pl.when(hosts)
        def _():
            def body(i, carried):
                gated[tile(i), :] = products(normed, i, padded)
                return carried

            lax.fori_loop(0, nf, body, 0)

        @pl.when(inner)
        def _():
            rim_copy().start()

    def guest_part(k):
        seq = around[k]
        if k == 0:
            v_piece(0, 1 - tp).wait_recv()
            v_piece(nf - 1, 1 - tp).wait_recv()
        else:
            v_copy(k, 1 - tp).wait_recv()
        gate = products(guest, seq, guest_padded)
        guest_padded[seq, 0:RIM, :] = jnp.where(inner, 0.0, padded[seq, tokens : tokens + RIM, :])
        guest_mine[seq] = convolve(guest_padded, seq, gate)

    def own_part(seq):
        @pl.when(inner)
        def _():
            padded[seq, 0:RIM, :] = guest_padded[seq, tokens : tokens + RIM, :]

        return convolve(padded, seq, gated[tile(seq), :])

    loads[0].wait()
    loads[1].wait()
    step = 32

    def norm_rows(i, carried):
        x = raw[pl.ds(pl.multiple_of(i * step, step), step), :].astype(F32)
        scale = lax.rsqrt(jnp.mean(x * x, axis=-1, keepdims=True) + EPSILON)
        rows = pl.ds(pl.multiple_of(fs * tokens + tp * half + i * step, step), step)
        normed[rows, :] = (x * scale * gain[...]).astype(BF16)
        return carried

    lax.fori_loop(0, half // step, norm_rows, 0)
    loads[2].wait()
    loads[3].wait()
    pl.semaphore_wait(
        barrier, 2 * nf + has_up.astype(jnp.int32) + has_down.astype(jnp.int32)
    )
    own(KV)
    for way in range(2):
        x_copy(way, fs).start()
    d_copy(0, fs, tp).start()
    loads[8].wait()
    loads[9].wait()
    own(OUT)
    z_step(KV, 1)
    spread(sp)
    loads[5].wait()
    loads[6].wait()
    own(MIX)
    for way in range(2):
        activations_in(way)
    guest_to_pair(1)
    z_step(OUT, 1)
    z_step(KV, 2)
    for way in range(2, 4):
        x_copy(way, beside[2]).wait_recv()
    d_copy(3, beside[2], tp).start()
    loads[7].wait()
    own(GATE)
    loads[4].wait()
    own(QUERY)
    z_step(OUT, 2)
    for j in range(10, 16):
        loads[j].wait()
    for k, seq in enumerate(around):
        d_copy(k, seq, 1 - tp).wait_recv()

    row_at = lax.broadcasted_iota(jnp.int32, (tokens, tokens), 0)
    col_at = lax.broadcasted_iota(jnp.int32, (tokens, tokens), 1)
    gates = jnp.concatenate([wi[...].astype(F32), wf[...].astype(F32)], axis=0).astype(BF16)
    heads = wi.shape[0]
    own_gate = lax.broadcasted_iota(jnp.int32, (2 * heads, tokens), 0)
    own_bias = lax.broadcasted_iota(jnp.int32, (1, heads), 1)
    bias_in = jnp.sum(jnp.where(own_bias == g, bias[0:1, :], 0.0), axis=1, keepdims=True)
    bias_out = jnp.sum(jnp.where(own_bias == g, bias[1:2, :], 0.0), axis=1, keepdims=True)
    line = lax.broadcasted_iota(jnp.int32, (128, tokens), 0)
    packed = jnp.zeros((128, tokens), F32)
    for s in range(nf):
        raw_gates = lax.dot_general(
            gates,
            normed[s * tokens : (s + 1) * tokens, :],
            (((1,), (1,)), ((), ())),
            preferred_element_type=F32,
        )
        entry = jnp.sum(jnp.where(own_gate == g, raw_gates, 0.0), axis=0, keepdims=True) + bias_in
        forget = (
            jnp.sum(jnp.where(own_gate == heads + g, raw_gates, 0.0), axis=0, keepdims=True)
            + bias_out
        )
        shift = jnp.sum(jnp.where(own_gate[:heads] == g, decay[s], 0.0), axis=0, keepdims=True)
        forget = jnp.minimum(forget, 0.0) - jnp.log1p(jnp.exp(-jnp.abs(forget))) + shift
        packed = jnp.where(line == s, forget, packed)
        packed = jnp.where(line == nf + s, entry, packed)
    ones = jnp.where(row_at <= col_at, 1.0, 0.0).astype(F32)
    sums = jnp.dot(packed, ones, precision=HIGHEST_PRECISION, preferred_element_type=F32)
    sums = jnp.where(line < nf, sums, packed)
    logs_t[...] = sums
    logs[...] = sums.T
    z_step(KV, 3)
    project(KV, kv)
    for s in range(nf):
        rows = pl.ds(s * tokens, tokens)
        total = logs_t[s : s + 1, tokens - 1 : tokens]
        reach = total - logs[:, s : s + 1] + logs[:, nf + s : nf + s + 1]
        peak = jnp.max(reach, axis=0, keepdims=True)
        weighted = (kv[rows, cols:].astype(F32) * jnp.exp(reach - peak)).astype(BF16)
        passed[s] = lax.dot_general(
            kv[rows, :cols], weighted, (((0,), (0,)), ((), ())), preferred_element_type=F32
        ).astype(BF16)
        local_stat[s : s + 1, :] = jnp.broadcast_to(total, (1, 128))
        local_stat[nf + s : nf + s + 1, :] = jnp.broadcast_to(peak, (1, 128))

    guest_from_pair(1)
    state_send(0)
    guest_to_pair(2)
    z_step(QUERY, 1)
    z_step(OUT, 3)

    @pl.when(guests)
    def _():
        row_copy().start()

    pass_step(0)
    guest_to_pair(0)
    guest_to_pair(nf - 1)
    state_step(1)
    z_step(MIX, 1)
    z_step(GATE, 1)
    pass_step(1)
    state_step(2)
    z_step(QUERY, 2)
    pass_step(2)
    pass_step(3)
    z_step(QUERY, 3)
    project(QUERY, query)
    state_step(3)
    join_states()

    scale = HEAD_DIM ** (-0.5)
    head_gain = head[:, block(g, cols)]
    causal = row_at >= col_at
    for s in range(nf):
        rows = pl.ds(s * tokens, tokens)
        scores = lax.dot_general(
            query[rows, :], kv[rows, :cols], (((1,), (1,)), ((), ())), preferred_element_type=F32
        )
        sums = logs[:, s : s + 1]
        pairs = jnp.where(
            causal,
            sums - logs_t[s : s + 1, :] + logs_t[nf + s : nf + s + 1, :],
            FAR_BELOW,
        )
        carried = sums + carry_m[s : s + 1, 0:1]
        top = jnp.maximum(carried, jnp.max(pairs, axis=1, keepdims=True))
        weights = (jnp.exp(pairs - top) * scores).astype(BF16)
        cell = jnp.dot(weights, kv[rows, cols:], preferred_element_type=F32)
        cell = cell + jnp.exp(carried - top) * jnp.dot(
            query[rows, :], carry[s].astype(BF16), preferred_element_type=F32
        )
        cell = cell * scale
        cell = cell * lax.rsqrt(jnp.mean(cell * cell, axis=-1, keepdims=True) + EPSILON)
        mine[1, s] = (cell * head_gain).astype(BF16)

    hand_out(1)
    guest_from_pair(2)
    z_step(MIX, 2)
    z_step(GATE, 2)
    guest_from_beside()
    own_products()

    @pl.when(outer)
    def _():
        rim_copy().wait_recv()

    @pl.when(hosts)
    def _():
        guest_part(1)
        mine[0, beside[0]] = own_part(beside[0])
        c_copy(1, around[1], fs).start()
        guest_part(3)
        mix_copy(0, 0, beside[0], fs).start()
        mine[0, beside[2]] = own_part(beside[2])
        c_copy(3, around[3], fs).start()
        guest_part(2)
        mix_copy(0, 2, beside[2], fs).start()
        mine[0, beside[1]] = own_part(beside[1])
        c_copy(2, around[2], fs).start()
        mix_copy(0, 1, beside[1], fs).start()

    guest_from_pair(0)
    guest_from_pair(nf - 1)

    @pl.when(hosts)
    def _():
        guest_part(0)
        got[0, :, block(fs, cols)] = own_part(fs)
        for k in (0, nf):
            last_copy(k, tp).start()

    for d in range(ns):
        rest_step(d)
    for k in range(nf - 1):
        mix_copy(1, k, beside[k], beside[k]).wait_recv()

    def memory_share(i, carried):
        acc[:, block(i, ocols)] = jnp.dot(
            got[1], wo[1, :, block(i, ocols)], preferred_element_type=F32
        )
        return carried

    lax.fori_loop(0, ns, memory_share, 0)

    def e_copy(i):
        return remote(
            share.at[:, block(i, ocols)],
            other.at[:, block(i, ocols)],
            e_send.at[i],
            e_recv.at[i],
            partner,
        )

    def add_conv(i, first, count):
        acc[:, block(i, ocols)] = acc[:, block(i, ocols)] + jnp.dot(
            got[0, :, pl.ds(first, count)],
            wo[0, pl.ds(first, count), block(i, ocols)],
            preferred_element_type=F32,
        )

    def add_pair(i, pair_at):
        add_conv(i, pl.multiple_of(pair_at * 2 * cols, 2 * cols), 2 * cols)

    def hand_over(i):
        share[:, block(i, ocols)] = acc[block(1 - tp, half), block(i, ocols)].astype(BF16)
        if i > 0:
            e_copy(i - 1).start()
        if i == ns - 1:
            e_copy(i).start()

    @pl.when(hosts)
    def _():
        for k in (1, 2):
            mix_copy(0, k, beside[k], beside[k]).wait_recv()
        for i in range(ns):
            add_pair(i, 1 - fy)
        mix_copy(0, 0, beside[0], beside[0]).wait_recv()
        for i in range(ns):
            add_pair(i, fy)
            hand_over(i)
        for i in range(ns):
            e_copy(i).wait_recv()
            out_ref[:, block(i, ocols)] = (
                acc[block(tp, half), block(i, ocols)] + other[:, block(i, ocols)].astype(F32)
            ).astype(BF16)

    @pl.when(guests)
    def _():
        c_copy(1, around[1], around[1]).wait_recv()
        for i in range(ns):
            add_conv(i, pl.multiple_of(beside[0] * cols, cols), cols)
        for k in range(2, nf):
            c_copy(k, around[k], around[k]).wait_recv()
        for i in range(ns):
            add_pair(i, 1 - fy)
            hand_over(i)
        row_copy().wait_recv()
        for i in range(ns):
            e_copy(i).wait_recv()
            acc[block(tp, half), block(i, ocols)] = acc[
                block(tp, half), block(i, ocols)
            ] + other[:, block(i, ocols)].astype(F32)
        for k in (0, nf):
            last_copy(k, tp if k == 0 else 1 - tp).wait_recv()
        for i in range(ns):
            out_ref[:, block(i, ocols)] = (
                acc[block(tp, half), block(i, ocols)]
                + jnp.dot(
                    last[:, block(tp, cols)],
                    wo[0, block(fs, cols), block(i, ocols)],
                    preferred_element_type=F32,
                )
                + jnp.dot(
                    last[:, block(1 - tp, cols)],
                    wo_last[:, block(i, ocols)],
                    preferred_element_type=F32,
                )
            ).astype(BF16)

    def sent(i, carried):
        e_copy(i).wait_send()
        return carried

    lax.fori_loop(0, ns, sent, 0)
    for d in range(ns):
        drain_step(d)
    for way in range(4):
        x_copy(way, (fs, fs, beside[0], beside[1])[way]).wait_send()
    for k, seq in enumerate(around):
        d_copy(k, seq, tp).wait_send()
    for k in range(nf - 1):
        mix_copy(1, k, beside[k], fs).wait_send()

    @pl.when(hosts)
    def _():
        for k in range(nf - 1):
            mix_copy(0, k, beside[k], fs).wait_send()
        for k in range(1, nf):
            v_copy(k, tp).wait_send()
        for j in (0, nf - 1):
            v_piece(j, tp).wait_send()
        for k in range(1, nf):
            c_copy(k, around[k], fs).wait_send()
        for k in (0, nf):
            last_copy(k, tp).wait_send()
        u_copy(around[1]).wait_send()

    @pl.when(guests)
    def _():
        for j in range(nf):
            t_copy(j).wait_send()
        row_copy().wait_send()

    @pl.when(inner)
    def _():
        rim_copy().wait_send()

    for side in range(2):
        for d in range(ns - 1):
            for parts in ((KV, QUERY, OUT), (MIX, GATE)):

                @pl.when(sends(parts[0], side, d))
                def _():
                    for part in parts:
                        z_copy(part, side, d, owner_of(side, d)).wait_send()

    for d in range(ns - 1):

        @pl.when(has_up & (sp - d >= 0))
        def _():
            for copy in state_copies(d, sp - d):
                copy.wait_send()


def whole_layer(act, gain, weights, wi, wf, bias, decay, taps, head, w_out_conv, w_out_mem):
    ns, nf = (lax.axis_size("sp"), lax.axis_size("fs"))
    tokens, model = act.shape
    half = tokens // 2
    depth, cols = weights[0].shape
    ocols = w_out_conv.shape[1]
    count = nf * tokens
    anywhere = pl.BlockSpec(memory_space=pl.ANY)
    dma = pltpu.SemaphoreType.DMA
    vmem = pltpu.VMEM
    return pl.pallas_call(
        functools.partial(layer_kernel, ns, nf),
        out_shape=pltpu.VMEM((half, ns * ocols), BF16),
        in_specs=[anywhere] * 16,
        out_specs=pl.BlockSpec(memory_space=pltpu.VMEM),
        scratch_shapes=[
            vmem((half, model), BF16),
            vmem(gain.shape, F32),
            vmem((count, model), BF16),
            vmem((ns * depth, 6 * cols), BF16),
            vmem(wi.shape, BF16),
            vmem(wf.shape, BF16),
            vmem(bias.shape, F32),
            vmem(decay.shape, F32),
            vmem(taps.shape, F32),
            vmem(head.shape, F32),
            vmem((2, nf * cols, ns * ocols), BF16),
            vmem((count, 2 * cols), BF16),
            vmem((count, cols), BF16),
            vmem((tokens, 128), F32),
            vmem((128, tokens), F32),
            vmem((2 * nf, 128), F32),
            vmem((nf, cols, cols), BF16),
            vmem((ns - 1, nf, cols, cols), BF16),
            vmem((ns - 1, 2 * nf, 128), F32),
            vmem((nf, cols, cols), F32),
            vmem((nf, 128), F32),
            vmem((nf, RIM + tokens, cols), F32),
            vmem((count, cols), BF16),
            vmem((2, nf, tokens, cols), BF16),
            vmem((2, tokens, nf * cols), BF16),
            vmem((count, model), BF16),
            vmem((nf, RIM + tokens, cols), F32),
            vmem((nf, tokens, cols), BF16),
            vmem((half, 2 * cols), BF16),
            vmem((cols, ns * ocols), BF16),
            vmem((tokens, ns * ocols), F32),
            vmem((half, ns * ocols), BF16),
            vmem((half, ns * ocols), BF16),
            dma((16,)),
            dma((4,)),
            dma((4,)),
            dma((nf,)),
            dma((nf,)),
            dma((2, ns - 1, PARTS)),
            dma((2, ns - 1, PARTS)),
            dma((ns, 4)),
            dma((ns, 4)),
            dma((2, ns - 1)),
            dma((2, ns - 1)),
            dma,
            dma,
            dma((2, nf - 1)),
            dma((2, nf - 1)),
            dma((ns,)),
            dma((ns,)),
            dma((nf,)),
            dma((nf,)),
            dma,
            dma,
            dma((nf + 1,)),
            dma((nf + 1,)),
            dma((nf + 1,)),
            dma((nf + 1,)),
            dma,
            dma,
        ],
        compiler_params=pltpu.CompilerParams(
            collective_id=0, has_side_effects=True, vmem_limit_bytes=54 * 1024 * 1024
        ),
    )(act, gain, *weights, wi, wf, bias, decay, taps, head, w_out_conv, w_out_mem)


def shards(
    activations,
    norm_gain,
    w_conv_gate,
    w_conv_mult,
    w_conv_in,
    conv_taps,
    w_query,
    w_key,
    w_value,
    w_input_gate,
    w_forget_gate,
    gate_bias,
    decay_shift,
    head_gain,
    w_out_conv,
    w_out_mem,
):
    group_index = lax.axis_index(("fs", "tp"))
    heads_here = MEMORY_HEADS // (lax.axis_size("fs") * lax.axis_size("tp"))
    channels = w_conv_gate.shape[1]
    ns, nf, nt = (lax.axis_size("sp"), lax.axis_size("fs"), lax.axis_size("tp"))
    if ns == 4 and nf == 4 and nt == 2 and heads_here == 1 and channels == HEAD_DIM:
        return whole_layer(
            activations[0],
            norm_gain[None, :],
            (w_key, w_value, w_query, w_conv_mult, w_conv_in, w_conv_gate),
            w_input_gate.T,
            w_forget_gate.T,
            gate_bias,
            decay_shift.transpose(0, 2, 1),
            conv_taps,
            head_gain[None, :],
            w_out_conv,
            w_out_mem,
        )[None]
    sequences = lax.all_gather(activations, "fs", axis=0, tiled=True)
    seq_count = sequences.shape[0]
    tokens = sequences.shape[1]
    model_width = sequences.shape[2]
    row_count = seq_count * tokens
    flat_rows = sequences.reshape(row_count, model_width).astype(jnp.float32)
    normed = (
        flat_rows
        * lax.rsqrt(jnp.mean(flat_rows * flat_rows, axis=-1, keepdims=True) + EPSILON)
        * norm_gain
    ).astype(jnp.bfloat16)
    pieces = (
        lax.all_gather(w_conv_gate, "sp", axis=0, tiled=True),
        lax.all_gather(w_conv_mult, "sp", axis=0, tiled=True),
        lax.all_gather(w_conv_in, "sp", axis=0, tiled=True),
        lax.all_gather(w_query, "sp", axis=0, tiled=True),
        lax.all_gather(w_key, "sp", axis=0, tiled=True),
        lax.all_gather(w_value, "sp", axis=0, tiled=True),
    )
    projected = tuple(
        (jnp.dot(normed, shard_piece, preferred_element_type=jnp.float32) for shard_piece in pieces)
    )
    conv_gate, conv_mult, conv_in, query, keys_proj, value = [
        tensor.astype(jnp.bfloat16).reshape(seq_count, tokens, -1) for tensor in projected
    ]
    entry_cols = lax.dynamic_slice_in_dim(w_input_gate, group_index * heads_here, heads_here, 1)
    forget_cols = lax.dynamic_slice_in_dim(w_forget_gate, group_index * heads_here, heads_here, 1)
    gate_values = jnp.dot(
        normed,
        jnp.concatenate([entry_cols, forget_cols], axis=1),
        preferred_element_type=jnp.float32,
    ).reshape(seq_count, tokens, 2 * heads_here)
    product = (conv_mult.astype(jnp.float32) * conv_in.astype(jnp.float32)).astype(jnp.bfloat16)
    ntaps = conv_taps.shape[0]
    rim_rows = from_behind(product[:, tokens - (ntaps - 1) :, :], "sp", 1)
    padded = jnp.concatenate([rim_rows, product], axis=1).astype(jnp.float32)
    tap_weights = lax.dynamic_slice_in_dim(conv_taps, group_index * channels, channels, 1)
    mixed_sum = jnp.zeros((seq_count, tokens, channels), jnp.float32)
    for tap_index in range(ntaps):
        mixed_sum = (
            mixed_sum + tap_weights[tap_index] * padded[:, tap_index : tap_index + tokens, :]
        )
    conv_out = (conv_gate.astype(jnp.float32) * mixed_sum).astype(jnp.bfloat16)
    bias_rows = lax.dynamic_slice_in_dim(gate_bias, group_index * heads_here, heads_here, 1)
    decay_rows = lax.dynamic_slice_in_dim(decay_shift, group_index * heads_here, heads_here, 2)
    entry = gate_values[..., :heads_here] + bias_rows[0]
    log_forget = jax.nn.log_sigmoid(gate_values[..., heads_here:] + bias_rows[1]) + decay_rows
    cell = memory_cell(
        head_rows(query, seq_count, heads_here),
        head_rows(keys_proj, seq_count, heads_here),
        head_rows(value, seq_count, heads_here),
        gate_rows(entry, seq_count, heads_here),
        gate_rows(log_forget, seq_count, heads_here),
    )
    cell = cell * lax.rsqrt(jnp.mean(cell * cell, axis=-1, keepdims=True) + EPSILON)
    gain_rows = lax.dynamic_slice_in_dim(
        head_gain, group_index * heads_here * HEAD_DIM, heads_here * HEAD_DIM, 0
    ).reshape(1, heads_here, 1, HEAD_DIM)
    scaled = cell.reshape(seq_count, heads_here, tokens, HEAD_DIM) * gain_rows
    mem_out = (
        scaled.transpose(0, 2, 1, 3)
        .reshape(seq_count, tokens, heads_here * HEAD_DIM)
        .astype(jnp.bfloat16)
    )
    conv_seq, mem_seq = (
        lax.all_to_all(conv_out, "fs", split_axis=0, concat_axis=2, tiled=True),
        lax.all_to_all(mem_out, "fs", split_axis=0, concat_axis=2, tiled=True),
    )
    rows_conv, rows_mem = (
        lax.all_gather(w_out_conv, "fs", axis=0, tiled=True),
        lax.all_gather(w_out_mem, "fs", axis=0, tiled=True),
    )
    full_conv, full_mem = (
        lax.all_gather(rows_conv, "sp", axis=1, tiled=True),
        lax.all_gather(rows_mem, "sp", axis=1, tiled=True),
    )
    conv_flat = conv_seq[0]
    mem_flat = mem_seq[0]
    output = lax.psum_scatter(
        (
            jnp.dot(conv_flat, full_conv, preferred_element_type=jnp.float32)
            + jnp.dot(mem_flat, full_mem, preferred_element_type=jnp.float32)
        ).astype(jnp.bfloat16),
        "tp",
        scatter_dimension=0,
        tiled=True,
    ).astype(jnp.float32)
    return output.astype(jnp.bfloat16).reshape(1, output.shape[0], -1)


def solution(mesh):
    return jax.shard_map(
        shards,
        mesh=mesh,
        in_specs=(
            P("fs", "sp", None),
            P(),
            P("sp", ("fs", "tp")),
            P("sp", ("fs", "tp")),
            P("sp", ("fs", "tp")),
            P(),
            P("sp", ("fs", "tp")),
            P("sp", ("fs", "tp")),
            P("sp", ("fs", "tp")),
            P(),
            P(),
            P(),
            P(None, "sp", None),
            P(),
            P(("fs", "tp"), "sp"),
            P(("fs", "tp"), "sp"),
        ),
        out_specs=P("fs", ("sp", "tp"), None),
        check_vma=False,
    )
```
